32 devices in a mesh: rep: 2 (over x), fs: 8 (over z, y), tp: 2 (over core).
Axes of the slice: x: 2, y: 2, z: 4, core: 2. Of those that a mesh axis runs over, the one named last changes fastest.
Arguments:
- inputs: bfloat16 [2, 3072, 2048], P('rep', 'fs', 'tp'), may hold values from -6 to 6
- gate_proj: bfloat16 [2048, 2816], P('fs', 'tp'), may hold values from -0.125 to 0.125
- value_proj: bfloat16 [2048, 2816], P('fs', 'tp'), may hold values from -0.125 to 0.125
- gate_taps: float32 [3, 2816], replicated, may hold values from -3 to 3
- value_taps: float32 [3, 2816], replicated, may hold values from -3 to 3
- out_grad: bfloat16 [2, 3072, 2816], P('rep', 'fs', 'tp'), may hold values from -6 to 6
Outputs:
- in_grad: bfloat16 [2, 3072, 2048], P('rep', 'fs', 'tp')
- gate_proj_grad: float32 [2048, 2816], P('fs', 'tp')
- value_proj_grad: float32 [2048, 2816], P('fs', 'tp')
- gate_taps_grad: float32 [3, 2816], replicated
- value_taps_grad: float32 [3, 2816], replicated
The draws below stay inside these ranges and needn't reach their ends.
All inputs are finite; a program needn't handle non-finite values.
Results may differ from the reference program's by a relative error of at most 0.013.
Values may be sent and summed in bfloat16 or wider, within the bound.
A program may use at most 128 MiB of HBM per device.

```python
import jax
import jax.numpy as jnp
from jax import lax

D = 2048
FF = 2816
CONV = 3
HID_DEV = 1408
BATCH = 2
SEQ = 3072
ALL_TOKENS = 6144


def raised(drawn, rng, source, target, shards_of, factor):
    owner, partner = [(jnp.arange(drawn.shape[axis_at]) // (drawn.shape[axis_at] // shards_of)).reshape([-1 if axis == axis_at else 1 for axis in range(drawn.ndim)]) for axis_at in (source, target)]
    chosen = jax.random.permutation(rng, shards_of)[partner]
    strong = (owner == chosen) | (owner == (partner + shards_of // 2) % shards_of)
    return jnp.where(strong, factor * drawn, drawn)


def block_scale(stream_key, extent, shards, least, largest):
    def one(position, blocks):
        draws = jax.random.uniform(jax.random.fold_in(jax.random.fold_in(stream_key, 6), position), (blocks,), jnp.float32, least / len(shards), largest / len(shards))
        return jnp.repeat(jnp.exp(draws), extent[position] // blocks).reshape((-1,) + (1,) * (len(extent) - position - 1))

    factor_of = one(*shards[0])
    for cut in shards[1:]:
        factor_of = factor_of * one(*cut)
    return factor_of


def centred(stream_key, extent, deviation, limit, split=(), kind=jnp.bfloat16):
    level = block_scale(stream_key, extent, split, -0.22, 0.18) if split else 1.0
    result = jax.random.normal(stream_key, extent, jnp.float32) * deviation * level
    return jnp.minimum(jnp.maximum(result, -limit), limit).astype(kind)


def bell_draw_with(key, dims, deviation, bound, split, heavy, kind=jnp.bfloat16):
    array = deviation * jax.random.normal(key, dims, jnp.float32)
    if split:
        array = array * block_scale(key, dims, split, -0.22, 0.18)
    return jnp.clip(raised(array, jax.random.fold_in(key, 3), *heavy), -bound, bound).astype(kind)


def setup_inputs(seed: int = 0) -> dict:
    arg_keys = jax.random.split(jax.random.key(seed), 7)
    inputs = bell_draw_with(arg_keys[0], (BATCH, SEQ, D), 1.0, 6.0, ((0, 2), (1, 8), (2, 2)), (1, 2, 8, 2.0))
    gate_proj = centred(arg_keys[1], (D, FF), D ** -0.5, 0.125, ((0, 8), (1, 2)))
    value_proj = centred(arg_keys[2], (D, FF), D ** -0.5, 0.125, ((0, 8), (1, 2)))
    gate_taps = centred(arg_keys[3], (CONV, FF), 0.577, 3.0, (), jnp.float32)
    value_taps = centred(arg_keys[4], (CONV, FF), 0.577, 3.0, (), jnp.float32)
    out_grad = bell_draw_with(arg_keys[5], (BATCH, SEQ, FF), 1.0, 6.0, ((0, 2), (1, 8), (2, 2)), (1, 2, 8, 2.0))
    return dict(inputs=inputs, gate_proj=gate_proj, value_proj=value_proj, gate_taps=gate_taps, value_taps=value_taps, out_grad=out_grad)


def conv_fwd(pre_acts, taps):
    seq_len = pre_acts.shape[0]
    padded = jnp.pad(pre_acts, ((1, 1), (0, 0)))
    return taps[0] * padded[0:seq_len] + taps[1] * padded[1:seq_len + 1] + taps[2] * padded[2:seq_len + 2]


def conv_back(cot_rows, taps):
    seq_len = cot_rows.shape[0]
    padded = jnp.pad(cot_rows, ((1, 1), (0, 0)))
    return taps[0] * padded[2:seq_len + 2] + taps[1] * padded[1:seq_len + 1] + taps[2] * padded[0:seq_len]


def cotangents(gate_mix, value_mix, cot_in):
    sigmoid_gate = jax.nn.sigmoid(gate_mix)
    gate_cot = cot_in * value_mix * (sigmoid_gate * (1.0 + gate_mix * (1.0 - sigmoid_gate)))
    value_cot = cot_in * (gate_mix * sigmoid_gate)
    return gate_cot, value_cot


def reference(inputs, gate_proj, value_proj, gate_taps, value_taps, out_grad):
    contract_cols = (((1,), (1,)), ((), ()))
    contract_rows = (((0,), (0,)), ((), ()))

    def one_sequence(pair):
        seq_inputs, seq_cot = pair
        seq_len = seq_inputs.shape[0]
        gate_pre = jnp.dot(seq_inputs, gate_proj, preferred_element_type=jnp.float32).astype(jnp.bfloat16)
        value_pre = jnp.dot(seq_inputs, value_proj, preferred_element_type=jnp.float32).astype(jnp.bfloat16)
        gate_mix = conv_fwd(gate_pre.astype(jnp.float32), gate_taps)
        value_mix = conv_fwd(value_pre.astype(jnp.float32), value_taps)
        gate_cot, value_cot = cotangents(gate_mix, value_mix, seq_cot.astype(jnp.float32))
        gate_pre_cot = conv_back(gate_cot, gate_taps).astype(jnp.bfloat16)
        value_pre_cot = conv_back(value_cot, value_taps).astype(jnp.bfloat16)

        def add_block(total, block_index):
            first_col = (block_index * HID_DEV).astype(jnp.int32)
            gate_cols = lax.dynamic_slice_in_dim(gate_pre_cot, first_col, HID_DEV, 1)
            value_cols = lax.dynamic_slice_in_dim(value_pre_cot, first_col, HID_DEV, 1)
            gate_block = lax.dynamic_slice_in_dim(gate_proj, first_col, HID_DEV, 1)
            value_block = lax.dynamic_slice_in_dim(value_proj, first_col, HID_DEV, 1)
            partial_value = lax.dot_general(gate_cols, gate_block, contract_cols, preferred_element_type=jnp.float32)
            partial_value = partial_value + lax.dot_general(value_cols, value_block, contract_cols, preferred_element_type=jnp.float32)
            rounded = lax.optimization_barrier(partial_value.astype(jnp.bfloat16))
            return total + rounded.astype(jnp.float32), None

        in_sum, _ = lax.scan(add_block, jnp.zeros((seq_len, D), jnp.float32), jnp.arange(FF // HID_DEV).astype(jnp.int32))
        in_grad = in_sum.astype(jnp.bfloat16)
        gate_grad = lax.dot_general(seq_inputs, gate_pre_cot, contract_rows, preferred_element_type=jnp.float32)
        value_grad = lax.dot_general(seq_inputs, value_pre_cot, contract_rows, preferred_element_type=jnp.float32)
        gate_padded = jnp.pad(gate_pre.astype(jnp.float32), ((1, 1), (0, 0)))
        value_padded = jnp.pad(value_pre.astype(jnp.float32), ((1, 1), (0, 0)))
        gate_tgrad = jnp.stack([jnp.sum(gate_padded[offset:offset + seq_len] * gate_cot, axis=0) for offset in range(3)])
        value_tgrad = jnp.stack([jnp.sum(value_padded[offset:offset + seq_len] * value_cot, axis=0) for offset in range(3)])
        return in_grad, gate_grad, value_grad, gate_tgrad, value_tgrad

    results = lax.map(one_sequence, (inputs, out_grad))
    factor = float(ALL_TOKENS) ** -0.5
    return (results[0], jnp.sum(results[1], axis=0) * factor, jnp.sum(results[2], axis=0) * factor,
            jnp.sum(results[3], axis=0) * factor, jnp.sum(results[4], axis=0) * factor)
```

```python
import functools

import jax
import jax.numpy as jnp
from jax import lax
from jax.experimental import pallas as pl
from jax.experimental.pallas import tpu as pltpu
from jax.sharding import PartitionSpec as P

HALO = 8


def row_length(mesh):
    axis = mesh.axis_names.index("fs")
    devices = mesh.devices.swapaxes(0, axis)
    line = devices.reshape(devices.shape[0], -1)[:, 0]
    places = [tuple(getattr(d, "coords", (i,))) for i, d in enumerate(line)]
    moved = lambda a, b: [i for i in range(len(a)) if a[i] != b[i]]
    length = 1
    while length < len(places) and moved(places[0], places[length]) == moved(places[0], places[1]):
        length += 1
    return length if len(places) % length == 0 else 1


def remote(src, dst, send, recv, **device):
    return pltpu.make_async_remote_copy(
        src_ref=src, dst_ref=dst, send_sem=send, recv_sem=recv, device_id=device, device_id_type=pl.DeviceIdType.MESH
    )


def gather_kernel(
    sizes, x_ref, g_ref, w_ref, x_all, g_all, w_all,
    w_send, w_recv, xr_send, xt_send, x_recv, xh_send, xh_recv, g_send, g_recv, gh_send, gh_recv, own_sem,
):
    reps, fs_count, tps, across = sizes
    deep = fs_count // across
    rep, fs, tp = (lax.axis_index(a) for a in ("rep", "fs", "tp"))
    z, y = fs // across, fs % across
    tokens, feats = x_ref.shape

    def other(axis_index, step, count):
        return (axis_index + step) % count

    def cols(index):
        return pl.ds(pl.multiple_of(index * feats, feats), feats)

    half_width = w_ref.shape[1] // 2

    def half(c):
        return pl.ds(c * half_width, half_width)

    def send_w(block, c, src, way, target):
        return remote(
            src.at[:, half(c)], w_all.at[block, :, half(c)], w_send.at[block, c, way], w_recv.at[block, c], fs=target
        )

    def along(block, c, src, down, up, sink):
        if down:
            @pl.when(z > 0)
            def _():
                sink(send_w(block, c, src, 0, fs - across))
        if up:
            @pl.when(z < deep - 1)
            def _():
                sink(send_w(block, c, src, 1, fs + across))

    def to_row(block, c, src, sink):
        for step in range(1, across):
            sink(send_w(block, c, src, 1 + step, z * across + other(y, step, across)))

    start = lambda c: c.start()
    sent = lambda c: c.wait_send()

    def x_main(slot, src, sem, **device):
        return remote(src, x_all.at[slot, pl.ds(0, tokens), cols(tp)], sem, x_recv.at[slot, tp], **device)

    def halos(sink):
        for side in range(2):
            near = pl.ds(0, HALO) if side == 0 else pl.ds(tokens - HALO, HALO)
            far = pl.ds(tokens + side * HALO, HALO)
            target = fs - 1 if side == 0 else fs + 1

            @pl.when((fs > 0) if side == 0 else (fs < fs_count - 1))
            def _():
                for slot in range(reps):
                    to_rep = other(rep, slot, reps)
                    for step in range(tps):
                        sink(remote(
                            x_ref.at[near], x_all.at[slot, far, cols(tp)], xh_send.at[side, slot, step],
                            xh_recv.at[side, slot, tp], rep=to_rep, fs=target, tp=other(tp, step, tps),
                        ))
                    sink(remote(
                        g_ref.at[slot, near], g_all.at[slot, far], gh_send.at[side, slot],
                        gh_recv.at[side, slot], rep=to_rep, fs=target,
                    ))

    def to_reps(sink):
        for slot in range(1, reps):
            sink(x_main(slot, x_ref, xr_send.at[slot], rep=other(rep, slot, reps)))
        for slot in range(1, reps):
            sink(remote(
                g_ref.at[slot], g_all.at[slot, pl.ds(0, tokens)], g_send.at[slot], g_recv.at[slot],
                rep=other(rep, slot, reps),
            ))

    def to_tps(slot, src, sink):
        for step in range(1, tps):
            sink(x_main(slot, src, xt_send.at[slot, step], tp=other(tp, step, tps)))

    halos(start)
    for c in range(2):
        along(fs, c, w_ref, True, True, start)
        to_row(fs, c, w_ref, start)
    to_reps(start)
    to_tps(0, x_ref, start)
    own = [
        pltpu.make_async_copy(w_ref, w_all.at[fs], own_sem.at[0]),
        pltpu.make_async_copy(x_ref, x_all.at[0, pl.ds(0, tokens), cols(tp)], own_sem.at[1]),
        pltpu.make_async_copy(g_ref.at[0], g_all.at[0, pl.ds(0, tokens)], own_sem.at[2]),
    ]
    for copy in own:
        copy.start()

    def landed(ref, sem):
        pltpu.make_async_copy(ref, ref, sem).wait()

    def hops(dist, arrive, sink):
        for sign in (-1, 1):
            block = fs + sign * dist * across

            @pl.when((z >= dist) if sign < 0 else (z + dist < deep))
            def _():
                for c in range(2):
                    if arrive:
                        landed(w_all.at[block, :, half(c)], w_recv.at[block, c])
                    along(block, c, w_all.at[block], sign > 0, sign < 0, sink)
                    if c == 0:
                        to_row(block, c, w_all.at[block], sink)
                    else:
                        level = z + sign * dist

                        @pl.when((level > 0) & (level < deep - 1))
                        def _():
                            to_row(block, c, w_all.at[block], sink)

    def across_first(dist, arrive, sink):
        for end in ((0, deep - 1) if deep > 1 else (0,)):
            @pl.when(z == end + dist if end == 0 else z == end - dist)
            def _():
                for step in range(1, across):
                    block = end * across + other(y, step, across)
                    if arrive:
                        landed(w_all.at[block, :, half(1)], w_recv.at[block, 1])
                    along(block, 1, w_all.at[block], end > 0, end == 0 and deep > 1, sink)

    def forward_x(arrive, sink):
        for slot in range(1, reps):
            mine = x_all.at[slot, pl.ds(0, tokens), cols(tp)]
            if arrive:
                landed(mine, x_recv.at[slot, tp])
            to_tps(slot, mine, sink)

    for dist in range(1, deep):
        hops(dist, True, start)
        across_first(dist - 1, True, start)
        if dist == 1:
            forward_x(True, start)
    if deep == 1:
        forward_x(True, start)
    across_first(deep - 1, True, start)

    for slot in range(reps):
        for step in range(1, tps):
            source = other(tp, step, tps)
            landed(x_all.at[slot, pl.ds(0, tokens), cols(source)], x_recv.at[slot, source])
        if slot:
            landed(g_all.at[slot, pl.ds(0, tokens)], g_recv.at[slot])
    for side in range(2):
        far = pl.ds(tokens + side * HALO, HALO)

        @pl.when((fs < fs_count - 1) if side == 0 else (fs > 0))
        def _():
            for slot in range(reps):
                for source in range(tps):
                    landed(x_all.at[slot, far, cols(source)], xh_recv.at[side, slot, source])
                landed(g_all.at[slot, far], gh_recv.at[side, slot])
    for level in range(deep):
        for step in range(1, across):
            block = level * across + other(y, step, across)
            landed(w_all.at[block, :, half(0)], w_recv.at[block, 0])
            if 0 < level < deep - 1:
                landed(w_all.at[block, :, half(1)], w_recv.at[block, 1])
    for copy in own:
        copy.wait()
    halos(sent)
    for c in range(2):
        along(fs, c, w_ref, True, True, sent)
        to_row(fs, c, w_ref, sent)
    to_reps(sent)
    to_tps(0, x_ref, sent)
    for dist in range(1, deep):
        hops(dist, False, sent)
    for dist in range(deep):
        across_first(dist, False, sent)
    forward_x(False, sent)


def gather_all(x_own, g_parts, w_own, across):
    reps, fs_count, tps = (lax.axis_size(a) for a in ("rep", "fs", "tp"))
    tokens, feats = x_own.shape
    width = g_parts.shape[2]
    ext = tokens + 2 * HALO
    sems = [
        (fs_count, 2, 1 + across), (fs_count, 2), (reps,), (reps, tps), (reps, tps), (2, reps, tps), (2, reps, tps),
        (reps,), (reps,), (2, reps), (2, reps), (3,),
    ]
    vmem, hbm = pl.BlockSpec(memory_space=pltpu.VMEM), pl.BlockSpec(memory_space=pl.ANY)
    return pl.pallas_call(
        functools.partial(gather_kernel, (reps, fs_count, tps, across)),
        out_shape=(
            jax.ShapeDtypeStruct((reps, ext, feats * tps), x_own.dtype),
            jax.ShapeDtypeStruct((reps, ext, width), g_parts.dtype),
            jax.ShapeDtypeStruct((fs_count,) + w_own.shape, w_own.dtype),
        ),
        in_specs=[vmem] * 3,
        out_specs=(hbm,) * 3,
        scratch_shapes=[pltpu.SemaphoreType.DMA(s) for s in sems],
        compiler_params=pltpu.CompilerParams(has_side_effects=True),
        name="gather_all",
    )(x_own, g_parts, w_own)


def scatter_kernel(
    sizes, grads, pv, taps, own_all, in_grad, taps_all, y_got, z_got, tp_got, rep_got, taps_got,
    y_send, y_recv, z_send, z_recv, tp_send, tp_recv, rep_send, rep_recv, own_send, own_recv,
    taps_send, taps_recv, all_send, all_recv,
):
    reps, fs_count, tps, across = sizes
    deep = fs_count // across
    rep, fs, tp = (lax.axis_index(a) for a in ("rep", "fs", "tp"))
    z, y = fs // across, fs % across
    rows, width = grads.shape[1], grads.shape[2] // 2
    tokens, feats = in_grad.shape

    def other(axis_index, step, count):
        return (axis_index + step) % count

    def part(c):
        return pl.ds(c * width, width)

    def cols(index):
        return pl.ds(pl.multiple_of(index * feats, feats), feats)

    start = lambda c: c.start()
    sent = lambda c: c.wait_send()

    def landed(ref, sem):
        pltpu.make_async_copy(ref, ref, sem).wait()

    def tap_terms(sink):
        for step in range(1, fs_count):
            sink(remote(taps, taps_got.at[step], taps_send.at[step], taps_recv.at[step], fs=other(fs, step, fs_count)))

    def y_block(c, level, sink):
        for step in range(1, across):
            to = other(y, step, across)
            sink(remote(
                grads.at[level * across + to, :, part(c)], y_got.at[step, level, c],
                y_send.at[step, level, c], y_recv.at[step, level, c], fs=z * across + to,
            ))

    def far_first(visit):
        for dist in range(deep - 1, 0, -1):
            for way in range(2):
                @pl.when((z + dist < deep) if way == 0 else (z >= dist))
                def _():
                    visit(z + dist if way == 0 else z - dist, way)

    def y_sends(sink):
        for c in range(2):
            far_first(lambda level, way: y_block(c, level, sink))
            y_block(c, z, sink)

    def to_tps(sink):
        for slot in list(range(1, reps)) + [0]:
            for step in range(1, tps):
                to = other(tp, step, tps)
                sink(remote(
                    pv.at[slot, :, cols(to)], tp_got.at[slot, step], tp_send.at[slot, step], tp_recv.at[slot, step], tp=to
                ))

    def to_reps(sink):
        for slot in range(1, reps):
            sink(remote(
                rep_got.at[0, slot], rep_got.at[1, slot], rep_send.at[slot], rep_recv.at[slot],
                rep=other(rep, reps - slot, reps),
            ))

    def z_hop(c, level, way, sink):
        sink(remote(
            grads.at[level * across + y, :, part(c)], z_got.at[way, level, c],
            z_send.at[way, level, c], z_recv.at[way, level, c], fs=fs + across if way == 0 else fs - across,
        ))

    def own_rep(c, sink):
        mine = own_all.at[rep, :, part(c)]
        for step in range(1, reps):
            sink(remote(mine, mine, own_send.at[step, c], own_recv.at[step, c], rep=other(rep, step, reps)))

    def taps_out(sink):
        mine = taps_all.at[rep, tp]
        for slot in range(reps):
            for step in range(tps):
                if slot or step:
                    sink(remote(
                        mine, mine, all_send.at[slot, step], all_recv.at[slot, step],
                        rep=other(rep, slot, reps), tp=other(tp, step, tps),
                    ))

    tap_terms(start)
    to_tps(start)
    y_sends(start)

    for way in range(2):
        @pl.when((z == 0) if way == 0 else (z == deep - 1))
        def _():
            @pl.loop(0, deep)
            def _(level):
                for c in range(2):
                    @pl.loop(0, rows // 16)
                    def _(i):
                        z_got[way, level, c, pl.ds(pl.multiple_of(i * 16, 16), 16)] = jnp.zeros((16, width), z_got.dtype)

    def own_tps(slot, at):
        total = pv[slot, at, cols(tp)].astype(jnp.float32)
        for step in range(1, tps):
            total += tp_got[slot, step, at].astype(jnp.float32)
        return total

    for slot in range(1, reps):
        for step in range(1, tps):
            landed(tp_got.at[slot, step], tp_recv.at[slot, step])

        @pl.loop(0, tokens // 16)
        def _(i):
            at = pl.ds(pl.multiple_of(i * 16, 16), 16)
            rep_got[0, slot, at] = own_tps(slot, at).astype(rep_got.dtype)
    to_reps(start)

    def add_up(c, level, ways, store):
        for step in range(1, across):
            landed(y_got.at[step, level, c], y_recv.at[step, level, c])
        for way in ways:
            @pl.when((z > 0) if way == 0 else (z < deep - 1))
            def _():
                landed(z_got.at[way, level, c], z_recv.at[way, level, c])

        @pl.loop(0, rows // 16)
        def _(i):
            at = pl.ds(pl.multiple_of(i * 16, 16), 16)
            total = grads[level * across + y, at, part(c)].astype(jnp.float32)
            for step in range(1, across):
                total += y_got[step, level, c, at].astype(jnp.float32)
            for way in ways:
                total += z_got[way, level, c, at].astype(jnp.float32)
            store(at, total.astype(grads.dtype))

    def pass_on(c, level, way):
        def store(at, value):
            grads[level * across + y, at, part(c)] = value

        add_up(c, level, (way,), store)
        z_hop(c, level, way, start)

    for c in range(2):
        far_first(lambda level, way: pass_on(c, level, way))

        def store(at, value):
            own_all[rep, at, part(c)] = value

        add_up(c, z, (0, 1), store)
        own_rep(c, start)
        if c == 0:
            total = taps[...]
            for step in range(1, fs_count):
                landed(taps_got.at[step], taps_recv.at[step])
                total += taps_got[step]
            taps_all[rep, tp] = total
            taps_out(start)
            for step in range(1, tps):
                landed(tp_got.at[0, step], tp_recv.at[0, step])
            for slot in range(1, reps):
                landed(rep_got.at[1, slot], rep_recv.at[slot])

            @pl.loop(0, tokens // 16)
            def _(i):
                at = pl.ds(pl.multiple_of(i * 16, 16), 16)
                total = own_tps(0, at)
                for slot in range(1, reps):
                    total += rep_got[1, slot, at].astype(jnp.float32)
                in_grad[at] = total.astype(in_grad.dtype)

    for slot in range(reps):
        for step in range(tps):
            if slot or step:
                landed(taps_all.at[other(rep, reps - slot, reps), other(tp, tps - step, tps)], all_recv.at[slot, step])
    for step in range(1, reps):
        for c in range(2):
            landed(own_all.at[other(rep, reps - step, reps), :, part(c)], own_recv.at[step, c])
    tap_terms(sent)
    to_tps(sent)
    y_sends(sent)
    to_reps(sent)
    for c in range(2):
        far_first(lambda level, way: z_hop(c, level, way, sent))
        own_rep(c, sent)
    taps_out(sent)


def scatter_all(grads, pv, taps, across):
    reps, fs_count, tps = (lax.axis_size(a) for a in ("rep", "fs", "tp"))
    deep = fs_count // across
    rows, width = grads.shape[1], grads.shape[2] // 2
    tokens, feats = pv.shape[1], pv.shape[2] // tps
    sem = pltpu.SemaphoreType.DMA
    pairs = [
        (across, deep, 2), (2, deep, 2), (reps, tps), (reps,), (reps, 2), (fs_count,), (reps, tps),
    ]
    vmem = pl.BlockSpec(memory_space=pltpu.VMEM)
    return pl.pallas_call(
        functools.partial(scatter_kernel, (reps, fs_count, tps, across)),
        out_shape=(
            jax.ShapeDtypeStruct((reps, rows, 2 * width), grads.dtype),
            jax.ShapeDtypeStruct((tokens, feats), pv.dtype),
            jax.ShapeDtypeStruct((reps, tps) + taps.shape, taps.dtype),
        ),
        in_specs=[vmem] * 3,
        out_specs=(vmem,) * 3,
        scratch_shapes=[
            pltpu.VMEM((across, deep, 2, rows, width), grads.dtype),
            pltpu.VMEM((2, deep, 2, rows, width), grads.dtype),
            pltpu.VMEM((reps, tps, tokens, feats), pv.dtype),
            pltpu.VMEM((2, reps, tokens, feats), pv.dtype),
            pltpu.VMEM((fs_count,) + taps.shape, taps.dtype),
        ] + [sem(p) for p in pairs for _ in range(2)],
        compiler_params=pltpu.CompilerParams(has_side_effects=True, vmem_limit_bytes=60000 * 1024),
        name="scatter_all",
    )(grads, pv, taps)


def mix_kernel(fs_count, factor, pre, g, taps, pre_cot, terms):
    reps, ext, width = g.shape
    tokens = pre_cot.shape[1]
    fs = lax.axis_index("fs")
    row = lax.broadcasted_iota(jnp.int32, (ext, 128), 0)
    has_next, has_prev = (fs < fs_count - 1).astype(jnp.int32), (fs > 0).astype(jnp.int32)
    inside = (row < tokens) | ((row < tokens + HALO) & (has_next > 0)) | ((row >= tokens + HALO) & (has_prev > 0))

    def before(x):
        return pltpu.roll(x, 1, 0)

    def after(x):
        return pltpu.roll(x, ext - 1, 0)

    terms[...] = jnp.zeros_like(terms)

    @pl.loop(0, width // 128)
    def _(j):
        spots = [pl.ds(pl.multiple_of(branch * width + j * 128, 128), 128) for branch in range(2)]
        weights = [[taps[k : k + 1, at] for k in range(3)] for at in spots]
        for slot in range(reps):
            pres = [jnp.where(inside, pre[slot, :, at].astype(jnp.float32), 0.0) for at in spots]
            around = [(before(p), p, after(p)) for p in pres]
            gate_mix, value_mix = [sum(w * p for w, p in zip(ws, ps)) for ws, ps in zip(weights, around)]
            cot_in = jnp.where(inside, g[slot, :, spots[0]].astype(jnp.float32), 0.0)
            sig = jax.nn.sigmoid(gate_mix)
            cots = (
                cot_in * value_mix * (sig * (1.0 + gate_mix * (1.0 - sig))),
                cot_in * (gate_mix * sig),
            )
            for at, ws, ps, cot in zip(spots, weights, around, cots):
                back = ws[0] * after(cot) + ws[1] * cot + ws[2] * before(cot)
                pre_cot[slot, :, at] = back[:tokens].astype(pre_cot.dtype)
                for k in range(3):
                    total = jnp.sum(ps[k][:tokens] * cot[:tokens], axis=0, keepdims=True)
                    terms[k : k + 1, at] += total * factor


def mix_all(pre, g, taps, tokens, fs_count, factor):
    reps, ext, both = pre.shape
    vmem = pl.BlockSpec(memory_space=pltpu.VMEM)
    return pl.pallas_call(
        functools.partial(mix_kernel, fs_count, factor),
        out_shape=(
            jax.ShapeDtypeStruct((reps, tokens, both), pre.dtype),
            jax.ShapeDtypeStruct((8, both), jnp.float32),
        ),
        in_specs=[vmem] * 3,
        out_specs=(vmem,) * 2,
        compiler_params=pltpu.CompilerParams(vmem_limit_bytes=40000 * 1024),
        name="mix_all",
    )(pre, g, taps)


LANES = 128
EDGE = 16


def part_width(hid, parts):
    return min(hid, -(-hid // parts // LANES) * LANES)


def fused_kernel(
    sizes, factor, x_own, gate_w, value_w, gate_taps, value_taps, g_own,
    in_grad, gate_out, value_out, gate_taps_out, value_taps_out,
    x_all, w_all, g_all, pre, cot, grads, from_z, fin, pv, from_tp, first_got, second_got, terms, terms_z, terms_all,
    own_sem, wy_send, wy_recv, wz_send, wz_recv, x_send, xf_send, xs_send, x_recv, hz_send, hb_send, hx_recv,
    g_send, g_recv, hg_send, hg_recv, sz_send, sz_recv, out_send, out_recv, tp_send, tp_recv,
    s1_send, s1_recv, s2_send, s2_recv, tz_send, tz_recv, ta_send, ta_recv,
):
    deep, across, width = sizes
    rep, fs, tp = (lax.axis_index(a) for a in ("rep", "fs", "tp"))
    z, y = fs // across, fs % across
    nrep, ny, ntp = 1 - rep, 1 - y, 1 - tp
    tokens, feats = x_own.shape
    rows, hid = gate_w.shape
    main = across * tokens
    ext = main + 2 * EDGE
    chunks = width // LANES
    both = 2 * LANES
    blocks = feats // rows
    half_feats = feats // 2
    cut = -(-tokens * 2 // 3 // 16) * 16
    weights = (gate_w, value_w)
    outs = (gate_out, value_out)
    others = [(dr, dy) for dr in range(2) for dy in range(2) if dr or dy]

    start = lambda c: c.start()
    sent = lambda c: c.wait_send()

    def landed(ref, sem):
        pltpu.make_async_copy(ref, ref, sem).wait()

    def moved(index, step):
        return (index + step) % 2

    def part_of(r, yy):
        return r * across + yy

    part = part_of(rep, y)

    def first_col(which):
        return jnp.minimum(which * width, hid - width)

    def live(which, c):
        return c * LANES >= which * width - first_col(which)

    def chunk_cols(which, c):
        return pl.ds(pl.multiple_of(first_col(which) + c * LANES, LANES), LANES)

    def all_cols(which):
        return pl.ds(pl.multiple_of(first_col(which), LANES), width)

    def cols(half):
        return pl.ds(pl.multiple_of(half * feats, feats), feats)

    def token_rows(yy):
        return pl.ds(pl.multiple_of(yy * tokens, 16), tokens)

    def lanes(branch):
        return pl.ds(branch * LANES, LANES)

    def near(side):
        return pl.ds(0, EDGE) if side == 0 else pl.ds(tokens - EDGE, EDGE)

    def far(side):
        return pl.ds(main + side * EDGE, EDGE)

    def gives_edge(side):
        return (y == 0) & (z > 0) if side == 0 else (y == across - 1) & (z < deep - 1)

    def has_edge(side):
        return z < deep - 1 if side == 0 else z > 0

    def takes_edge(side):
        return (y == 0) & (z < deep - 1) if side == 0 else (y == across - 1) & (z > 0)

    def w_across(c, sink):
        for branch, w in enumerate(weights):
            sink(remote(
                w.at[:, chunk_cols(part_of(rep, ny), c)], w_all.at[c, fs, :, lanes(branch)],
                wy_send.at[c, branch], wy_recv.at[c, branch], fs=z * across + ny,
            ))

    def w_along(c, block, up, down, sink):
        ref = w_all.at[c, block]
        if up:
            @pl.when(z < deep - 1)
            def _():
                sink(remote(ref, ref, wz_send.at[c, block, 0], wz_recv.at[c, block], fs=fs + across))
        if down:
            @pl.when(z > 0)
            def _():
                sink(remote(ref, ref, wz_send.at[c, block, 1], wz_recv.at[c, block], fs=fs - across))

    def w_local(c):
        return [
            pltpu.make_async_copy(
                w.at[:, chunk_cols(part, c)], w_all.at[c, fs, :, lanes(branch)], own_sem.at[2 * c + branch]
            ) for branch, w in enumerate(weights)
        ]

    def w_own_along(c, sink):
        w_along(c, fs, True, True, sink)

    def w_near_along(c, arrive, sink):
        block = z * across + ny
        if arrive:
            for branch in range(2):
                landed(w_all.at[c, block, :, lanes(branch)], wy_recv.at[c, branch])
        w_along(c, block, True, True, sink)

    def w_step(c, dist, arrive, sink):
        for sign in (-1, 1):
            @pl.when((z >= dist) if sign < 0 else (z + dist < deep))
            def _():
                for yy in (y, ny):
                    block = (z + sign * dist) * across + yy
                    if arrive:
                        landed(w_all.at[c, block], wz_recv.at[c, block])
                    w_along(c, block, sign < 0, sign > 0, sink)

    def piece(k):
        return (0, cut) if k == 0 else (cut, tokens - cut)

    def x_at(r, yy, k, half):
        offset, size = piece(k)
        return x_all.at[r, pl.ds(pl.multiple_of(yy * tokens + offset, 16), size), cols(half)]

    def x_mine(k):
        return x_own.at[pl.ds(*piece(k))]

    def x_direct(sink):
        for k in range(2):
            sink(remote(x_mine(k), x_at(rep, y, k, tp), x_send.at[1, k], x_recv.at[rep, y, k, tp], fs=z * across + ny))
            other = 1 - k
            sink(remote(x_mine(other), x_at(rep, y, other, tp), x_send.at[0, other], x_recv.at[rep, y, other, tp], rep=nrep))

    def x_to_sibling(sink):
        for k in range(2):
            sink(remote(x_mine(k), x_at(rep, y, k, tp), xs_send.at[rep, y, k], x_recv.at[rep, y, k, tp], tp=ntp))

    def x_forward(way, sink):
        if way == 0:
            ref = x_at(rep, ny, 0, tp)
            sink(remote(ref, ref, xf_send.at[0], x_recv.at[rep, ny, 0, tp], rep=nrep))
        else:
            ref = x_at(nrep, y, 1, tp)
            sink(remote(ref, ref, xf_send.at[1], x_recv.at[nrep, y, 1, tp], fs=z * across + ny))

    def x_share(r, yy, k, sink):
        ref = x_at(r, yy, k, tp)
        sink(remote(ref, ref, xs_send.at[r, yy, k], x_recv.at[r, yy, k, tp], tp=ntp))

    def x_landed(r, yy, k, half):
        landed(x_at(r, yy, k, half), x_recv.at[r, yy, k, half])

    def edge_out(side, sink):
        target = fs - across if side == 0 else fs + across

        @pl.when(gives_edge(side))
        def _():
            sink(remote(
                x_own.at[near(side)], x_all.at[rep, far(side), cols(tp)], hz_send.at[side],
                hx_recv.at[side, rep, tp], fs=target,
            ))
            level = z - 1 if side == 0 else z + 1
            for dr in range(2):
                for dy in range(2):
                    r, yy = moved(rep, dr), moved(y, dy)
                    sink(remote(
                        g_own.at[near(side), all_cols(part_of(r, yy))], g_all.at[rep, far(side)],
                        hg_send.at[side, dr, dy], hg_recv.at[side, rep], rep=r, fs=level * across + yy,
                    ))

    def edge_share(side, arrive, sink):
        @pl.when(takes_edge(side))
        def _():
            ref = x_all.at[rep, far(side), cols(tp)]
            if arrive:
                landed(ref, hx_recv.at[side, rep, tp])
            for dr in range(2):
                for dy in range(2):
                    for dt in range(2):
                        if dr or dy or dt:
                            sink(remote(
                                ref, ref, hb_send.at[side, dr, dy, dt], hx_recv.at[side, rep, tp],
                                rep=moved(rep, dr), fs=z * across + moved(y, dy), tp=moved(tp, dt),
                            ))

    def edge_landed(side):
        @pl.when(has_edge(side))
        def _():
            for dr in range(2):
                r = moved(rep, dr)
                for dt in range(2):
                    half = moved(tp, dt)
                    ref, sem = x_all.at[r, far(side), cols(half)], hx_recv.at[side, r, half]
                    if dr or dt:
                        landed(ref, sem)
                    else:
                        @pl.when(jnp.logical_not(takes_edge(side)))
                        def _():
                            landed(ref, sem)
                landed(g_all.at[r, far(side)], hg_recv.at[side, r])

    def g_direct(c, sink):
        for dr, dy in others:
            r, yy = moved(rep, dr), moved(y, dy)
            sink(remote(
                g_own.at[:, chunk_cols(part_of(r, yy), c)], g_all.at[rep, token_rows(y), pl.ds(c * LANES, LANES)],
                g_send.at[c, dr, dy], g_recv.at[c, rep, y], rep=r, fs=z * across + yy,
            ))

    def g_landed(c):
        for dr, dy in others:
            r, yy = moved(rep, dr), moved(y, dy)
            landed(g_all.at[r, token_rows(yy), pl.ds(c * LANES, LANES)], g_recv.at[c, r, yy])

    x_local = pltpu.make_async_copy(
        x_own, x_all.at[rep, token_rows(y), cols(tp)], own_sem.at[2 * chunks]
    )
    g_local = pltpu.make_async_copy(
        g_own.at[:, all_cols(part)], g_all.at[rep, token_rows(y)], own_sem.at[2 * chunks + 1]
    )

    def chunk_lanes(c):
        return pl.ds(c * both, both)

    def project(c):
        @pl.loop(0, 2)
        def _(slot):
            total = jnp.dot(
                x_all[slot], w_all[c].reshape(-1, both), preferred_element_type=jnp.float32
            )
            pre[slot] = total.astype(pre.dtype)

    def mix(c):
        row = lax.broadcasted_iota(jnp.int32, (ext, LANES), 0)
        has_next, has_prev = (z < deep - 1).astype(jnp.int32), (z > 0).astype(jnp.int32)
        inside = (row < main) | ((row < main + EDGE) & (has_next > 0)) | ((row >= main + EDGE) & (has_prev > 0))
        counted = inside & (live(part, c).astype(jnp.int32) > 0)
        tap_cols = pl.ds(pl.multiple_of(tp * hid + first_col(part) + c * LANES, LANES), LANES)
        taps = [[ref[k : k + 1, tap_cols] for k in range(3)] for ref in (gate_taps, value_taps)]
        terms[:, pl.ds(c * LANES, LANES)] = jnp.zeros((8, LANES), jnp.float32)

        def before(v):
            return pltpu.roll(v, 1, 0)

        def after(v):
            return pltpu.roll(v, ext - 1, 0)

        @pl.loop(0, 2)
        def _(slot):
            pres = [jnp.where(inside, pre[slot, :, lanes(b)].astype(jnp.float32), 0.0) for b in range(2)]
            around = [(before(p), p, after(p)) for p in pres]
            gate_mix, value_mix = [sum(w * p for w, p in zip(ws, ps)) for ws, ps in zip(taps, around)]
            cot_in = jnp.where(counted, g_all[slot, :, pl.ds(c * LANES, LANES)].astype(jnp.float32), 0.0)
            sig = jax.nn.sigmoid(gate_mix)
            cots = (
                cot_in * value_mix * (sig * (1.0 + gate_mix * (1.0 - sig))),
                cot_in * (gate_mix * sig),
            )
            for b in range(2):
                ws, ps, one = taps[b], around[b], cots[b]
                back = ws[0] * after(one) + ws[1] * one + ws[2] * before(one)
                cot[slot, :, pl.ds(c * both + b * LANES, LANES)] = back[:main].astype(cot.dtype)
                for k in range(3):
                    total = jnp.sum(ps[k][:main] * one[:main], axis=0, keepdims=True)
                    terms[2 * k + b : 2 * k + b + 1, pl.ds(c * LANES, LANES)] += total * factor

    def far_first(visit):
        @pl.loop(0, 2 * deep - 1)
        def _(i):
            dist = deep - 1 - i // 2
            level = jnp.where(i % 2 == 0, z + dist, z - dist)

            @pl.when((level >= 0) & (level < deep))
            def _():
                visit(level)

    def sum_hop(c, block, up, sink):
        way = 0 if up else 1
        sink(remote(
            grads.at[c, block], from_z.at[way, c, block], sz_send.at[c, block], sz_recv.at[way, c, block],
            fs=fs + across if up else fs - across,
        ))

    def weight_terms(c):
        def visit(level):
            for yy in range(across):
                block = level * across + yy
                at = pl.ds(pl.multiple_of(block * rows, rows), rows)
                total = sum(
                    lax.dot_general(
                        x_all[slot, :main, at], cot[slot, :, chunk_lanes(c)], (((0,), (0,)), ((), ())),
                        preferred_element_type=jnp.float32,
                    ) for slot in range(2)
                )
                grads[c, block] = (total * factor).astype(grads.dtype)
            for up in (True, False):
                @pl.when((level > z) & (z == 0) if up else (level < z) & (z == deep - 1))
                def _():
                    for yy in range(across):
                        sum_hop(c, level * across + yy, up, start)

        far_first(visit)

    def inner(level, up):
        return (z > 0) & (z < deep - 1) & ((level > z) if up else (level < z))

    def pass_on(c):
        def visit(level):
            for up in (True, False):
                @pl.when(inner(level, up))
                def _():
                    way = 0 if up else 1
                    for yy in range(across):
                        block = level * across + yy
                        landed(from_z.at[way, c, block], sz_recv.at[way, c, block])
                        total = grads[c, block].astype(jnp.float32) + from_z[way, c, block].astype(jnp.float32)
                        grads[c, block] = total.astype(grads.dtype)
                        sum_hop(c, block, up, start)

        far_first(visit)

    def sums_sent(c):
        def visit(level):
            for up in (True, False):
                @pl.when((level > z) if up else (level < z))
                def _():
                    for yy in range(across):
                        sum_hop(c, level * across + yy, up, sent)

        far_first(visit)

    def to_owners(c, same, sink):
        here = chunk_cols(part, c)
        for branch, out in enumerate(outs):
            if same:
                sink(remote(
                    out.at[:, here], out.at[:, here], out_send.at[c, branch, 0], out_recv.at[c, branch, rep, y], rep=nrep
                ))
            else:
                src = fin.at[c, :, lanes(branch)]
                for k, r in ((1, rep), (2, nrep)):
                    sink(remote(
                        src, out.at[:, here], out_send.at[c, branch, k], out_recv.at[c, branch, rep, y],
                        rep=r, fs=z * across + ny,
                    ))

    def finish(c):
        for same in (False, True):
            block = z * across + (y if same else ny)
            for way in range(2):
                @pl.when(z > 0 if way == 0 else z < deep - 1)
                def _():
                    landed(from_z.at[way, c, block], sz_recv.at[way, c, block])
            total = grads[c, block].astype(jnp.float32)
            for way in range(2):
                total += from_z[way, c, block].astype(jnp.float32)
            total = total.astype(grads.dtype)

            @pl.when(live(part, c))
            def _():
                if same:
                    for branch, out in enumerate(outs):
                        out[:, chunk_cols(part, c)] = total[:, branch * LANES : (branch + 1) * LANES]
                else:
                    fin[c] = total
                to_owners(c, same, start)

    def input_terms():
        for dr, dy in ((1, 1), (0, 1), (1, 0), (0, 0)):
            r, yy = moved(rep, dr), moved(y, dy)
            q = part_of(r, yy)

            @pl.loop(0, 2 * blocks)
            def _(i):
                half = jnp.where(i < blocks, ntp, tp)
                j = i % blocks
                total = sum(
                    lax.dot_general(
                        cot[r, token_rows(yy), chunk_lanes(c)], w_all[c, half * blocks + j],
                        (((1,), (1,)), ((), ())), preferred_element_type=jnp.float32,
                    ) for c in range(chunks)
                )
                pv[half, q, :, pl.ds(pl.multiple_of(j * rows, rows), rows)] = total.astype(pv.dtype)

            tp_hop(q, start)

    def tp_hop(q, sink):
        sink(remote(pv.at[ntp, q], from_tp.at[q], tp_send.at[q], tp_recv.at[q], tp=ntp))

    def f_cols(f):
        return pl.ds(f * half_feats, half_feats)

    def first_hop(f, k, sink):
        q = part_of(nrep, ny) if k else part_of(nrep, y) if f == 0 else part_of(rep, ny)
        target = dict(rep=nrep) if f == 0 else dict(fs=z * across + ny)
        sink(remote(pv.at[tp, q, :, f_cols(f)], first_got.at[f, k], s1_send.at[f, k], s1_recv.at[f, k], **target))

    def second_hop(f, sink):
        q = part_of(rep, ny) if f == 0 else part_of(nrep, y)
        target = dict(fs=z * across + ny) if f == 0 else dict(rep=nrep)
        sink(remote(pv.at[tp, q, :, f_cols(f)], second_got.at[f], s2_send.at[f], s2_recv.at[f], **target))

    def row_tiles(body):
        @pl.loop(0, tokens // 16)
        def _(i):
            body(pl.ds(pl.multiple_of(i * 16, 16), 16))

    def add_sibling(q):
        landed(from_tp.at[q], tp_recv.at[q])

        def body(at):
            total = pv[tp, q, at].astype(jnp.float32) + from_tp[q, at].astype(jnp.float32)
            pv[tp, q, at] = total.astype(pv.dtype)

        row_tiles(body)

    def input_first():
        add_sibling(part_of(nrep, ny))
        first_hop(0, 1, start)
        first_hop(1, 1, start)
        add_sibling(part_of(nrep, y))
        first_hop(0, 0, start)
        add_sibling(part_of(rep, ny))
        first_hop(1, 0, start)

    def input_second():
        for f in range(2):
            q = part_of(rep, ny) if f == 0 else part_of(nrep, y)
            landed(first_got.at[f, 1], s1_recv.at[f, 1])

            def body(at):
                total = pv[tp, q, at, f_cols(f)].astype(jnp.float32) + first_got[f, 1, at].astype(jnp.float32)
                pv[tp, q, at, f_cols(f)] = total.astype(pv.dtype)

            row_tiles(body)
            second_hop(f, start)

    def input_last():
        landed(from_tp.at[part], tp_recv.at[part])
        for f in range(2):
            landed(first_got.at[f, 0], s1_recv.at[f, 0])
            landed(second_got.at[f], s2_recv.at[f])

        def body(at):
            for f in range(2):
                total = pv[tp, part, at, f_cols(f)].astype(jnp.float32) + from_tp[part, at, f_cols(f)].astype(jnp.float32)
                total += first_got[f, 0, at].astype(jnp.float32) + second_got[f, at].astype(jnp.float32)
                in_grad[at, f_cols(f)] = total.astype(in_grad.dtype)

        row_tiles(body)

    def taps_along(sink):
        for step in range(1, deep):
            to = (z + step) % deep
            sink(remote(
                terms_z.at[z], terms_z.at[z], tz_send.at[step], tz_recv.at[z], fs=to * across + y
            ))

    def taps_start():
        terms_z[z] = terms[...]
        taps_along(start)

    def taps_out(sink):
        ref = terms_all.at[rep, y, tp]
        for dr in range(2):
            for dy in range(2):
                for dt in range(2):
                    if dr or dy or dt:
                        sink(remote(
                            ref, ref, ta_send.at[dr, dy, dt], ta_recv.at[rep, y, tp],
                            rep=moved(rep, dr), fs=z * across + moved(y, dy), tp=moved(tp, dt),
                        ))

    def taps_sum():
        for step in range(1, deep):
            source = (z + step) % deep
            landed(terms_z.at[source], tz_recv.at[source])
        terms_all[rep, y, tp] = sum(terms_z[level] for level in range(deep))
        taps_out(start)

    def taps_last():
        for dr in range(2):
            for dy in range(2):
                for dt in range(2):
                    if dr or dy or dt:
                        at = (moved(rep, dr), moved(y, dy), moved(tp, dt))
                        landed(terms_all.at[at], ta_recv.at[at])
        for r in range(2):
            for yy in range(across):
                which = r * across + yy
                first = min(which * width, hid - width)
                skip = which * width - first
                for half in range(2):
                    for branch, out in enumerate((gate_taps_out, value_taps_out)):
                        for k in range(3):
                            if skip < width:
                                begin = half * hid + first + skip
                                out[k : k + 1, begin : begin + width - skip] = terms_all[
                                    r, yy, half, 2 * k + branch : 2 * k + branch + 1, skip:
                                ]

    for c in range(chunks):
        for copy in w_local(c):
            copy.start()
    x_local.start()
    g_local.start()
    w_across(0, start)
    for side in range(2):
        edge_out(side, start)
    for c in range(chunks):
        for copy in w_local(c):
            copy.wait()
        w_own_along(c, start)
        if c == 0:
            for later in range(1, min(2, chunks)):
                w_across(later, start)
            x_direct(start)
            x_to_sibling(start)
            g_direct(0, start)
            for later in range(2, chunks):
                w_across(later, start)
            for later in range(1, chunks):
                g_direct(later, start)

    for way in range(2):
        @pl.when((z == 0) if way == 0 else (z == deep - 1))
        def _():
            for c in range(chunks):
                for yy in range(across):
                    from_z[way, c, z * across + yy] = jnp.zeros((rows, both), from_z.dtype)

    for side in range(2):
        edge_share(side, True, start)
    w_near_along(0, True, start)
    w_step(0, 1, True, start)
    x_landed(nrep, y, 1, tp)
    x_forward(1, start)
    x_share(nrep, y, 1, start)
    if chunks > 1:
        w_near_along(1, True, start)
    for dist in range(2, deep):
        w_step(0, dist, True, start)
    x_landed(rep, ny, 0, tp)
    x_forward(0, start)
    x_share(rep, ny, 0, start)
    x_landed(nrep, y, 0, tp)
    x_share(nrep, y, 0, start)
    if chunks > 1:
        w_step(1, 1, True, start)
    x_landed(rep, ny, 1, tp)
    x_share(rep, ny, 1, start)
    for k in (1, 0):
        x_landed(nrep, ny, k, tp)
        x_share(nrep, ny, k, start)
    x_local.wait()
    for r in range(2):
        for yy in range(across):
            for k in range(2):
                x_landed(r, yy, k, ntp)
    for side in range(2):
        edge_landed(side)
    g_local.wait()

    for c in range(chunks):
        project(c)
        if c + 1 < chunks:
            for dist in range(2, deep):
                w_step(c + 1, dist, True, start)
        g_landed(c)
        mix(c)
        if c + 2 < chunks:
            w_near_along(c + 2, True, start)
            w_step(c + 2, 1, True, start)
        weight_terms(c)
        if c > 0:
            pass_on(c - 1)
    taps_start()
    input_terms()
    for c in range(chunks - 1):
        finish(c)
        if c == 0:
            input_first()
    if chunks == 1:
        input_first()
    taps_sum()
    pass_on(chunks - 1)
    input_second()
    finish(chunks - 1)
    input_last()
    taps_last()
    for dr, dy in others:
        r, yy = moved(rep, dr), moved(y, dy)
        for c in range(chunks):
            @pl.when(live(part_of(r, yy), c))
            def _():
                at = chunk_cols(part_of(r, yy), c)
                for branch, out in enumerate(outs):
                    landed(out.at[:, at], out_recv.at[c, branch, r, yy])

    for side in range(2):
        edge_out(side, sent)
        edge_share(side, False, sent)
    x_direct(sent)
    x_to_sibling(sent)
    for way in range(2):
        x_forward(way, sent)
    for k in range(2):
        for dr, dy in others:
            x_share(moved(rep, dr), moved(y, dy), k, sent)
    for c in range(chunks):
        w_across(c, sent)
        w_own_along(c, sent)
        w_near_along(c, False, sent)
        for dist in range(1, deep):
            w_step(c, dist, False, sent)
        g_direct(c, sent)
        sums_sent(c)

        @pl.when(live(part, c))
        def _():
            for same in (False, True):
                to_owners(c, same, sent)
    for dr in range(2):
        for dy in range(2):
            tp_hop(part_of(moved(rep, dr), moved(y, dy)), sent)
    for f in range(2):
        for k in range(2):
            first_hop(f, k, sent)
        second_hop(f, sent)
    taps_along(sent)
    taps_out(sent)


def fused_all(across, x_own, gate_w, value_w, gate_taps, value_taps, g_own):
    reps, fs_count, tps = (lax.axis_size(a) for a in ("rep", "fs", "tp"))
    deep = fs_count // across
    tokens, feats = x_own.shape
    rows, hid = gate_w.shape
    width = part_width(hid, reps * across)
    chunks = width // LANES
    both = 2 * LANES
    main = across * tokens
    ext = main + 2 * EDGE
    half = feats // 2
    parts = reps * across
    factor = float(tokens * fs_count * reps) ** (-0.5)
    dtype = x_own.dtype
    f32 = jnp.float32
    sem = pltpu.SemaphoreType.DMA
    sems = [
        (2 * chunks + 2,), (chunks, 2), (chunks, 2), (chunks, fs_count, 2), (chunks, fs_count), (2, 2), (2,),
        (reps, across, 2), (reps, across, 2, tps), (2,), (2, 2, 2, 2), (2, reps, tps),
        (chunks, 2, 2), (chunks, reps, across), (2, 2, 2), (2, reps), (chunks, fs_count), (2, chunks, fs_count),
        (chunks, 2, 3), (chunks, 2, reps, across), (parts,), (parts,),
        (2, 2), (2, 2), (2,), (2,), (deep,), (deep,), (2, 2, 2), (reps, across, tps),
    ]
    buffers = [
        ((reps, ext, tps * feats), dtype), ((chunks, fs_count, rows, both), dtype), ((reps, ext, width), dtype),
        ((reps, ext, both), dtype), ((reps, main, 2 * width), dtype), ((chunks, fs_count, rows, both), dtype),
        ((2, chunks, fs_count, rows, both), dtype), ((chunks, rows, both), dtype),
        ((tps, parts, tokens, feats), dtype), ((parts, tokens, feats), dtype),
        ((2, 2, tokens, half), dtype), ((2, tokens, half), dtype),
        ((8, width), f32), ((deep, 8, width), f32), ((reps, across, tps, 8, width), f32),
    ]
    vmem = pl.BlockSpec(memory_space=pltpu.VMEM)
    return pl.pallas_call(
        functools.partial(fused_kernel, (deep, across, width), factor),
        out_shape=(
            jax.ShapeDtypeStruct((tokens, feats), dtype),
            jax.ShapeDtypeStruct((rows, hid), dtype),
            jax.ShapeDtypeStruct((rows, hid), dtype),
            jax.ShapeDtypeStruct(gate_taps.shape, f32),
            jax.ShapeDtypeStruct(value_taps.shape, f32),
        ),
        in_specs=[vmem] * 6,
        out_specs=(vmem,) * 5,
        scratch_shapes=[pltpu.VMEM(*b) for b in buffers] + [sem(s) for s in sems],
        compiler_params=pltpu.CompilerParams(has_side_effects=True, vmem_limit_bytes=60000 * 1024),
        name="fused_all",
    )(x_own, gate_w, value_w, gate_taps, value_taps, g_own)


def fits_plane(across, inputs, gate_proj):
    reps, fs_count, tps = (lax.axis_size(a) for a in ("rep", "fs", "tp"))
    tokens, feats = inputs.shape[1:]
    rows, hid = gate_proj.shape
    parts = reps * across
    width = part_width(hid, parts)
    return (
        reps == across == tps == 2 and fs_count > across and tokens % 16 == 0 and tokens >= 48
        and hid % LANES == 0 and rows % LANES == 0 and feats % rows == 0 and feats % (2 * LANES) == 0
        and 4 * parts * width <= 5 * hid
    )


def shards(across, inputs, gate_proj, value_proj, gate_taps, value_taps, out_grad):
    if fits_plane(across, inputs, gate_proj):
        in_grad, gate_grad, value_grad, gate_terms, value_terms = fused_all(
            across, inputs[0], gate_proj, value_proj, gate_taps, value_taps, out_grad[0]
        )
        return in_grad[None], gate_grad.astype(jnp.float32), value_grad.astype(jnp.float32), gate_terms, value_terms

    contract_cols = (((1,), (1,)), ((), ()))
    contract_rows = (((0,), (0,)), ((), ()))
    reps, fs_count = lax.axis_size("rep"), lax.axis_size("fs")
    rep = lax.axis_index("rep")
    tokens, feats = inputs.shape[1:]
    hid = gate_proj.shape[1]
    width = min(hid, -(-hid // reps // 128) * 128)
    last = hid - width

    def start_of(part):
        return jnp.minimum(part * width, last)

    first = start_of(rep)
    dead = rep * width - first
    live = jnp.arange(width) >= dead

    def part_cols(x, part):
        return lax.dynamic_slice_in_dim(x, start_of(part), width, x.ndim - 1)

    w_own = jnp.concatenate(
        [jnp.where(live, part_cols(w, rep), jnp.zeros((), w.dtype)) for w in (gate_proj, value_proj)], axis=1
    )
    g_parts = jnp.stack([part_cols(out_grad[0], (rep + step) % reps) for step in range(reps)])
    x_all, g_all, w_all = gather_all(inputs[0], g_parts, w_own, across)
    w_all = w_all.reshape(-1, 2 * width)

    ext = tokens + 2 * HALO
    pre = jnp.dot(x_all.reshape(reps * ext, -1), w_all, preferred_element_type=jnp.float32)
    pre = pre.astype(jnp.bfloat16).reshape(reps, ext, 2 * width)
    tap_start = lax.axis_index("tp") * hid + first
    taps = jnp.concatenate(
        [lax.dynamic_slice_in_dim(t, tap_start, width, 1) for t in (gate_taps, value_taps)], axis=1
    )
    factor = float(tokens * fs_count * reps) ** (-0.5)
    pre_cot, tap_terms = mix_all(pre, g_all, taps, tokens, fs_count, factor)
    pre_cot = pre_cot.reshape(reps * tokens, 2 * width)
    tap_terms = tap_terms[:3]

    grads = lax.dot_general(
        x_all[:, :tokens].reshape(reps * tokens, -1), pre_cot, contract_rows, preferred_element_type=jnp.float32
    )
    grads = (grads * factor).astype(jnp.bfloat16).reshape(fs_count, -1, 2 * width)
    partial_value = lax.dot_general(pre_cot, w_all, contract_cols, preferred_element_type=jnp.float32)
    partial_value = partial_value.astype(jnp.bfloat16).reshape(reps, tokens, -1)
    lanes = -(-tap_terms.size // 1024) * 128
    tap_terms = jnp.pad(tap_terms.reshape(-1), (0, 8 * lanes - tap_terms.size)).reshape(8, lanes)
    own, in_grad, tap_all = scatter_all(grads, partial_value, tap_terms, across)

    skips = [max(0, p * width - last) for p in range(reps)]
    proj_grads = [
        jnp.concatenate(
            [own[p, :, branch * width + skips[p] : (branch + 1) * width] for p in range(reps)], axis=1
        ).astype(jnp.float32)
        for branch in range(2)
    ]
    tap_all = tap_all.reshape(reps, -1, 8 * lanes)[:, :, : 6 * width].reshape(reps, -1, 3, 2, width)
    taps_out = jnp.concatenate(
        [tap_all[p, half, :, :, skips[p] :] for half in range(tap_all.shape[1]) for p in range(reps)], axis=2
    )
    return in_grad[None], proj_grads[0], proj_grads[1], taps_out[:, 0], taps_out[:, 1]


def solution(mesh):
    placed = (P("rep", "fs", "tp"), P("fs", "tp"), P("fs", "tp"), P(), P(), P("rep", "fs", "tp"))
    return jax.shard_map(
        functools.partial(shards, row_length(mesh)),
        mesh=mesh,
        in_specs=placed,
        out_specs=(P("rep", "fs", "tp"), P("fs", "tp"), P("fs", "tp"), P(), P()),
        check_vma=False,
    )
```

```python
import functools

import jax
import jax.numpy as jnp
from jax import lax
from jax.experimental import pallas as pl
from jax.experimental.pallas import tpu as pltpu
from jax.sharding import PartitionSpec as P

HALO = 8


def row_length(mesh):
    axis = mesh.axis_names.index("fs")
    devices = mesh.devices.swapaxes(0, axis)
    line = devices.reshape(devices.shape[0], -1)[:, 0]
    places = [tuple(getattr(d, "coords", (i,))) for i, d in enumerate(line)]
    moved = lambda a, b: [i for i in range(len(a)) if a[i] != b[i]]
    length = 1
    while length < len(places) and moved(places[0], places[length]) == moved(places[0], places[1]):
        length += 1
    return length if len(places) % length == 0 else 1


def remote(src, dst, send, recv, **device):
    return pltpu.make_async_remote_copy(
        src_ref=src, dst_ref=dst, send_sem=send, recv_sem=recv, device_id=device, device_id_type=pl.DeviceIdType.MESH
    )


def gather_kernel(
    sizes, x_ref, g_ref, w_ref, x_all, g_all, w_all,
    w_send, w_recv, xr_send, xt_send, x_recv, xh_send, xh_recv, g_send, g_recv, gh_send, gh_recv, own_sem,
):
    reps, fs_count, tps, across = sizes
    deep = fs_count // across
    rep, fs, tp = (lax.axis_index(a) for a in ("rep", "fs", "tp"))
    z, y = fs // across, fs % across
    tokens, feats = x_ref.shape

    def other(axis_index, step, count):
        return (axis_index + step) % count

    def cols(index):
        return pl.ds(pl.multiple_of(index * feats, feats), feats)

    half_width = w_ref.shape[1] // 2

    def half(c):
        return pl.ds(c * half_width, half_width)

    def send_w(block, c, src, way, target):
        return remote(
            src.at[:, half(c)], w_all.at[block, :, half(c)], w_send.at[block, c, way], w_recv.at[block, c], fs=target
        )

    def along(block, c, src, down, up, sink):
        if down:
            @pl.when(z > 0)
            def _():
                sink(send_w(block, c, src, 0, fs - across))
        if up:
            @pl.when(z < deep - 1)
            def _():
                sink(send_w(block, c, src, 1, fs + across))

    def to_row(block, c, src, sink):
        for step in range(1, across):
            sink(send_w(block, c, src, 1 + step, z * across + other(y, step, across)))

    start = lambda c: c.start()
    sent = lambda c: c.wait_send()

    def x_main(slot, src, sem, **device):
        return remote(src, x_all.at[slot, pl.ds(0, tokens), cols(tp)], sem, x_recv.at[slot, tp], **device)

    def halos(sink):
        for side in range(2):
            near = pl.ds(0, HALO) if side == 0 else pl.ds(tokens - HALO, HALO)
            far = pl.ds(tokens + side * HALO, HALO)
            target = fs - 1 if side == 0 else fs + 1

            @pl.when((fs > 0) if side == 0 else (fs < fs_count - 1))
            def _():
                for slot in range(reps):
                    to_rep = other(rep, slot, reps)
                    for step in range(tps):
                        sink(remote(
                            x_ref.at[near], x_all.at[slot, far, cols(tp)], xh_send.at[side, slot, step],
                            xh_recv.at[side, slot, tp], rep=to_rep, fs=target, tp=other(tp, step, tps),
                        ))
                    sink(remote(
                        g_ref.at[slot, near], g_all.at[slot, far], gh_send.at[side, slot],
                        gh_recv.at[side, slot], rep=to_rep, fs=target,
                    ))

    def to_reps(sink):
        for slot in range(1, reps):
            sink(x_main(slot, x_ref, xr_send.at[slot], rep=other(rep, slot, reps)))
        for slot in range(1, reps):
            sink(remote(
                g_ref.at[slot], g_all.at[slot, pl.ds(0, tokens)], g_send.at[slot], g_recv.at[slot],
                rep=other(rep, slot, reps),
            ))

    def to_tps(slot, src, sink):
        for step in range(1, tps):
            sink(x_main(slot, src, xt_send.at[slot, step], tp=other(tp, step, tps)))

    halos(start)
    for c in range(2):
        along(fs, c, w_ref, True, True, start)
        to_row(fs, c, w_ref, start)
    to_reps(start)
    to_tps(0, x_ref, start)
    own = [
        pltpu.make_async_copy(w_ref, w_all.at[fs], own_sem.at[0]),
        pltpu.make_async_copy(x_ref, x_all.at[0, pl.ds(0, tokens), cols(tp)], own_sem.at[1]),
        pltpu.make_async_copy(g_ref.at[0], g_all.at[0, pl.ds(0, tokens)], own_sem.at[2]),
    ]
    for copy in own:
        copy.start()

    def landed(ref, sem):
        pltpu.make_async_copy(ref, ref, sem).wait()

    def hops(dist, arrive, sink):
        for sign in (-1, 1):
            block = fs + sign * dist * across

            @pl.when((z >= dist) if sign < 0 else (z + dist < deep))
            def _():
                for c in range(2):
                    if arrive:
                        landed(w_all.at[block, :, half(c)], w_recv.at[block, c])
                    along(block, c, w_all.at[block], sign > 0, sign < 0, sink)
                    if c == 0:
                        to_row(block, c, w_all.at[block], sink)
                    else:
                        level = z + sign * dist

                        @pl.when((level > 0) & (level < deep - 1))
                        def _():
                            to_row(block, c, w_all.at[block], sink)

    def across_first(dist, arrive, sink):
        for end in ((0, deep - 1) if deep > 1 else (0,)):
            @pl.when(z == end + dist if end == 0 else z == end - dist)
            def _():
                for step in range(1, across):
                    block = end * across + other(y, step, across)
                    if arrive:
                        landed(w_all.at[block, :, half(1)], w_recv.at[block, 1])
                    along(block, 1, w_all.at[block], end > 0, end == 0 and deep > 1, sink)

    def forward_x(arrive, sink):
        for slot in range(1, reps):
            mine = x_all.at[slot, pl.ds(0, tokens), cols(tp)]
            if arrive:
                landed(mine, x_recv.at[slot, tp])
            to_tps(slot, mine, sink)

    for dist in range(1, deep):
        hops(dist, True, start)
        across_first(dist - 1, True, start)
        if dist == 1:
            forward_x(True, start)
    if deep == 1:
        forward_x(True, start)
    across_first(deep - 1, True, start)

    for slot in range(reps):
        for step in range(1, tps):
            source = other(tp, step, tps)
            landed(x_all.at[slot, pl.ds(0, tokens), cols(source)], x_recv.at[slot, source])
        if slot:
            landed(g_all.at[slot, pl.ds(0, tokens)], g_recv.at[slot])
    for side in range(2):
        far = pl.ds(tokens + side * HALO, HALO)

        @pl.when((fs < fs_count - 1) if side == 0 else (fs > 0))
        def _():
            for slot in range(reps):
                for source in range(tps):
                    landed(x_all.at[slot, far, cols(source)], xh_recv.at[side, slot, source])
                landed(g_all.at[slot, far], gh_recv.at[side, slot])
    for level in range(deep):
        for step in range(1, across):
            block = level * across + other(y, step, across)
            landed(w_all.at[block, :, half(0)], w_recv.at[block, 0])
            if 0 < level < deep - 1:
                landed(w_all.at[block, :, half(1)], w_recv.at[block, 1])
    for copy in own:
        copy.wait()
    halos(sent)
    for c in range(2):
        along(fs, c, w_ref, True, True, sent)
        to_row(fs, c, w_ref, sent)
    to_reps(sent)
    to_tps(0, x_ref, sent)
    for dist in range(1, deep):
        hops(dist, False, sent)
    for dist in range(deep):
        across_first(dist, False, sent)
    forward_x(False, sent)


def gather_all(x_own, g_parts, w_own, across):
    reps, fs_count, tps = (lax.axis_size(a) for a in ("rep", "fs", "tp"))
    tokens, feats = x_own.shape
    width = g_parts.shape[2]
    ext = tokens + 2 * HALO
    sems = [
        (fs_count, 2, 1 + across), (fs_count, 2), (reps,), (reps, tps), (reps, tps), (2, reps, tps), (2, reps, tps),
        (reps,), (reps,), (2, reps), (2, reps), (3,),
    ]
    vmem, hbm = pl.BlockSpec(memory_space=pltpu.VMEM), pl.BlockSpec(memory_space=pl.ANY)
    return pl.pallas_call(
        functools.partial(gather_kernel, (reps, fs_count, tps, across)),
        out_shape=(
            jax.ShapeDtypeStruct((reps, ext, feats * tps), x_own.dtype),
            jax.ShapeDtypeStruct((reps, ext, width), g_parts.dtype),
            jax.ShapeDtypeStruct((fs_count,) + w_own.shape, w_own.dtype),
        ),
        in_specs=[vmem] * 3,
        out_specs=(hbm,) * 3,
        scratch_shapes=[pltpu.SemaphoreType.DMA(s) for s in sems],
        compiler_params=pltpu.CompilerParams(has_side_effects=True),
        name="gather_all",
    )(x_own, g_parts, w_own)


def scatter_kernel(
    sizes, grads, pv, taps, own_all, in_grad, taps_all, y_got, z_got, tp_got, rep_got, taps_got,
    y_send, y_recv, z_send, z_recv, tp_send, tp_recv, rep_send, rep_recv, own_send, own_recv,
    taps_send, taps_recv, all_send, all_recv,
):
    reps, fs_count, tps, across = sizes
    deep = fs_count // across
    rep, fs, tp = (lax.axis_index(a) for a in ("rep", "fs", "tp"))
    z, y = fs // across, fs % across
    rows, width = grads.shape[1], grads.shape[2] // 2
    tokens, feats = in_grad.shape

    def other(axis_index, step, count):
        return (axis_index + step) % count

    def part(c):
        return pl.ds(c * width, width)

    def cols(index):
        return pl.ds(pl.multiple_of(index * feats, feats), feats)

    start = lambda c: c.start()
    sent = lambda c: c.wait_send()

    def landed(ref, sem):
        pltpu.make_async_copy(ref, ref, sem).wait()

    def tap_terms(sink):
        for step in range(1, fs_count):
            sink(remote(taps, taps_got.at[step], taps_send.at[step], taps_recv.at[step], fs=other(fs, step, fs_count)))

    def y_block(c, level, sink):
        for step in range(1, across):
            to = other(y, step, across)
            sink(remote(
                grads.at[level * across + to, :, part(c)], y_got.at[step, level, c],
                y_send.at[step, level, c], y_recv.at[step, level, c], fs=z * across + to,
            ))

    def far_first(visit):
        for dist in range(deep - 1, 0, -1):
            for way in range(2):
                @pl.when((z + dist < deep) if way == 0 else (z >= dist))
                def _():
                    visit(z + dist if way == 0 else z - dist, way)

    def y_sends(sink):
        for c in range(2):
            far_first(lambda level, way: y_block(c, level, sink))
            y_block(c, z, sink)

    def to_tps(sink):
        for slot in list(range(1, reps)) + [0]:
            for step in range(1, tps):
                to = other(tp, step, tps)
                sink(remote(
                    pv.at[slot, :, cols(to)], tp_got.at[slot, step], tp_send.at[slot, step], tp_recv.at[slot, step], tp=to
                ))

    def to_reps(sink):
        for slot in range(1, reps):
            sink(remote(
                rep_got.at[0, slot], rep_got.at[1, slot], rep_send.at[slot], rep_recv.at[slot],
                rep=other(rep, reps - slot, reps),
            ))

    def z_hop(c, level, way, sink):
        sink(remote(
            grads.at[level * across + y, :, part(c)], z_got.at[way, level, c],
            z_send.at[way, level, c], z_recv.at[way, level, c], fs=fs + across if way == 0 else fs - across,
        ))

    def own_rep(c, sink):
        mine = own_all.at[rep, :, part(c)]
        for step in range(1, reps):
            sink(remote(mine, mine, own_send.at[step, c], own_recv.at[step, c], rep=other(rep, step, reps)))

    def taps_out(sink):
        mine = taps_all.at[rep, tp]
        for slot in range(reps):
            for step in range(tps):
                if slot or step:
                    sink(remote(
                        mine, mine, all_send.at[slot, step], all_recv.at[slot, step],
                        rep=other(rep, slot, reps), tp=other(tp, step, tps),
                    ))

    tap_terms(start)
    to_tps(start)
    y_sends(start)

    for way in range(2):
        @pl.when((z == 0) if way == 0 else (z == deep - 1))
        def _():
            @pl.loop(0, deep)
            def _(level):
                for c in range(2):
                    @pl.loop(0, rows // 16)
                    def _(i):
                        z_got[way, level, c, pl.ds(pl.multiple_of(i * 16, 16), 16)] = jnp.zeros((16, width), z_got.dtype)

    def own_tps(slot, at):
        total = pv[slot, at, cols(tp)].astype(jnp.float32)
        for step in range(1, tps):
            total += tp_got[slot, step, at].astype(jnp.float32)
        return total

    for slot in range(1, reps):
        for step in range(1, tps):
            landed(tp_got.at[slot, step], tp_recv.at[slot, step])

        @pl.loop(0, tokens // 16)
        def _(i):
            at = pl.ds(pl.multiple_of(i * 16, 16), 16)
            rep_got[0, slot, at] = own_tps(slot, at).astype(rep_got.dtype)
    to_reps(start)

    def add_up(c, level, ways, store):
        for step in range(1, across):
            landed(y_got.at[step, level, c], y_recv.at[step, level, c])
        for way in ways:
            @pl.when((z > 0) if way == 0 else (z < deep - 1))
            def _():
                landed(z_got.at[way, level, c], z_recv.at[way, level, c])

        @pl.loop(0, rows // 16)
        def _(i):
            at = pl.ds(pl.multiple_of(i * 16, 16), 16)
            total = grads[level * across + y, at, part(c)].astype(jnp.float32)
            for step in range(1, across):
                total += y_got[step, level, c, at].astype(jnp.float32)
            for way in ways:
                total += z_got[way, level, c, at].astype(jnp.float32)
            store(at, total.astype(grads.dtype))

    def pass_on(c, level, way):
        def store(at, value):
            grads[level * across + y, at, part(c)] = value

        add_up(c, level, (way,), store)
        z_hop(c, level, way, start)

    for c in range(2):
        far_first(lambda level, way: pass_on(c, level, way))

        def store(at, value):
            own_all[rep, at, part(c)] = value

        add_up(c, z, (0, 1), store)
        own_rep(c, start)
        if c == 0:
            total = taps[...]
            for step in range(1, fs_count):
                landed(taps_got.at[step], taps_recv.at[step])
                total += taps_got[step]
            taps_all[rep, tp] = total
            taps_out(start)
            for step in range(1, tps):
                landed(tp_got.at[0, step], tp_recv.at[0, step])
            for slot in range(1, reps):
                landed(rep_got.at[1, slot], rep_recv.at[slot])

            @pl.loop(0, tokens // 16)
            def _(i):
                at = pl.ds(pl.multiple_of(i * 16, 16), 16)
                total = own_tps(0, at)
                for slot in range(1, reps):
                    total += rep_got[1, slot, at].astype(jnp.float32)
                in_grad[at] = total.astype(in_grad.dtype)

    for slot in range(reps):
        for step in range(tps):
            if slot or step:
                landed(taps_all.at[other(rep, reps - slot, reps), other(tp, tps - step, tps)], all_recv.at[slot, step])
    for step in range(1, reps):
        for c in range(2):
            landed(own_all.at[other(rep, reps - step, reps), :, part(c)], own_recv.at[step, c])
    tap_terms(sent)
    to_tps(sent)
    y_sends(sent)
    to_reps(sent)
    for c in range(2):
        far_first(lambda level, way: z_hop(c, level, way, sent))
        own_rep(c, sent)
    taps_out(sent)


def scatter_all(grads, pv, taps, across):
    reps, fs_count, tps = (lax.axis_size(a) for a in ("rep", "fs", "tp"))
    deep = fs_count // across
    rows, width = grads.shape[1], grads.shape[2] // 2
    tokens, feats = pv.shape[1], pv.shape[2] // tps
    sem = pltpu.SemaphoreType.DMA
    pairs = [
        (across, deep, 2), (2, deep, 2), (reps, tps), (reps,), (reps, 2), (fs_count,), (reps, tps),
    ]
    vmem = pl.BlockSpec(memory_space=pltpu.VMEM)
    return pl.pallas_call(
        functools.partial(scatter_kernel, (reps, fs_count, tps, across)),
        out_shape=(
            jax.ShapeDtypeStruct((reps, rows, 2 * width), grads.dtype),
            jax.ShapeDtypeStruct((tokens, feats), pv.dtype),
            jax.ShapeDtypeStruct((reps, tps) + taps.shape, taps.dtype),
        ),
        in_specs=[vmem] * 3,
        out_specs=(vmem,) * 3,
        scratch_shapes=[
            pltpu.VMEM((across, deep, 2, rows, width), grads.dtype),
            pltpu.VMEM((2, deep, 2, rows, width), grads.dtype),
            pltpu.VMEM((reps, tps, tokens, feats), pv.dtype),
            pltpu.VMEM((2, reps, tokens, feats), pv.dtype),
            pltpu.VMEM((fs_count,) + taps.shape, taps.dtype),
        ] + [sem(p) for p in pairs for _ in range(2)],
        compiler_params=pltpu.CompilerParams(has_side_effects=True, vmem_limit_bytes=60000 * 1024),
        name="scatter_all",
    )(grads, pv, taps)


def mix_kernel(fs_count, factor, pre, g, taps, pre_cot, terms):
    reps, ext, width = g.shape
    tokens = pre_cot.shape[1]
    fs = lax.axis_index("fs")
    row = lax.broadcasted_iota(jnp.int32, (ext, 128), 0)
    has_next, has_prev = (fs < fs_count - 1).astype(jnp.int32), (fs > 0).astype(jnp.int32)
    inside = (row < tokens) | ((row < tokens + HALO) & (has_next > 0)) | ((row >= tokens + HALO) & (has_prev > 0))

    def before(x):
        return pltpu.roll(x, 1, 0)

    def after(x):
        return pltpu.roll(x, ext - 1, 0)

    terms[...] = jnp.zeros_like(terms)

    @pl.loop(0, width // 128)
    def _(j):
        spots = [pl.ds(pl.multiple_of(branch * width + j * 128, 128), 128) for branch in range(2)]
        weights = [[taps[k : k + 1, at] for k in range(3)] for at in spots]
        for slot in range(reps):
            pres = [jnp.where(inside, pre[slot, :, at].astype(jnp.float32), 0.0) for at in spots]
            around = [(before(p), p, after(p)) for p in pres]
            gate_mix, value_mix = [sum(w * p for w, p in zip(ws, ps)) for ws, ps in zip(weights, around)]
            cot_in = jnp.where(inside, g[slot, :, spots[0]].astype(jnp.float32), 0.0)
            sig = jax.nn.sigmoid(gate_mix)
            cots = (
                cot_in * value_mix * (sig * (1.0 + gate_mix * (1.0 - sig))),
                cot_in * (gate_mix * sig),
            )
            for at, ws, ps, cot in zip(spots, weights, around, cots):
                back = ws[0] * after(cot) + ws[1] * cot + ws[2] * before(cot)
                pre_cot[slot, :, at] = back[:tokens].astype(pre_cot.dtype)
                for k in range(3):
                    total = jnp.sum(ps[k][:tokens] * cot[:tokens], axis=0, keepdims=True)
                    terms[k : k + 1, at] += total * factor


def mix_all(pre, g, taps, tokens, fs_count, factor):
    reps, ext, both = pre.shape
    vmem = pl.BlockSpec(memory_space=pltpu.VMEM)
    return pl.pallas_call(
        functools.partial(mix_kernel, fs_count, factor),
        out_shape=(
            jax.ShapeDtypeStruct((reps, tokens, both), pre.dtype),
            jax.ShapeDtypeStruct((8, both), jnp.float32),
        ),
        in_specs=[vmem] * 3,
        out_specs=(vmem,) * 2,
        compiler_params=pltpu.CompilerParams(vmem_limit_bytes=40000 * 1024),
        name="mix_all",
    )(pre, g, taps)


LANES = 128
EDGE = 16


def part_width(hid, parts):
    return min(hid, -(-hid // parts // LANES) * LANES)


def fused_kernel(
    sizes, factor, x_own, gate_w, value_w, gate_taps, value_taps, g_own,
    in_grad, gate_out, value_out, gate_taps_out, value_taps_out,
    x_all, w_all, g_all, pre, cot, grads, from_z, fin, pv, from_tp, first_got, second_got, terms, terms_z, terms_all,
    own_sem, wy_send, wy_recv, wz_send, wz_recv, x_send, xf_send, xs_send, x_recv, hz_send, hb_send, hx_recv,
    g_send, g_recv, hg_send, hg_recv, sz_send, sz_recv, out_send, out_recv, tp_send, tp_recv,
    s1_send, s1_recv, s2_send, s2_recv, tz_send, tz_recv, ta_send, ta_recv,
):
    deep, across, width = sizes
    rep, fs, tp = (lax.axis_index(a) for a in ("rep", "fs", "tp"))
    z, y = fs // across, fs % across
    nrep, ny, ntp = 1 - rep, 1 - y, 1 - tp
    tokens, feats = x_own.shape
    rows, hid = gate_w.shape
    main = across * tokens
    ext = main + 2 * EDGE
    chunks = width // LANES
    both = 2 * LANES
    blocks = feats // rows
    half_feats = feats // 2
    step = tokens * 3 // 8 // 16 * 16
    pieces = ((0, step), (step, step), (2 * step, tokens - 2 * step))
    last = len(pieces) - 1
    weights = (gate_w, value_w)
    outs = (gate_out, value_out)
    others = [(dr, dy) for dr in range(2) for dy in range(2) if dr or dy]

    start = lambda c: c.start()
    sent = lambda c: c.wait_send()

    def landed(ref, sem):
        pltpu.make_async_copy(ref, ref, sem).wait()

    def moved(index, step):
        return (index + step) % 2

    def part_of(r, yy):
        return r * across + yy

    part = part_of(rep, y)

    def first_col(which):
        return jnp.minimum(which * width, hid - width)

    def live(which, c):
        return c * LANES >= which * width - first_col(which)

    def chunk_cols(which, c):
        return pl.ds(pl.multiple_of(first_col(which) + c * LANES, LANES), LANES)

    def all_cols(which):
        return pl.ds(pl.multiple_of(first_col(which), LANES), width)

    def cols(half):
        return pl.ds(pl.multiple_of(half * feats, feats), feats)

    def token_rows(yy):
        return pl.ds(pl.multiple_of(yy * tokens, 16), tokens)

    def lanes(branch):
        return pl.ds(branch * LANES, LANES)

    def near(side):
        return pl.ds(0, EDGE) if side == 0 else pl.ds(tokens - EDGE, EDGE)

    def far(side):
        return pl.ds(main + side * EDGE, EDGE)

    def gives_edge(side):
        return (y == 0) & (z > 0) if side == 0 else (y == across - 1) & (z < deep - 1)

    def has_edge(side):
        return z < deep - 1 if side == 0 else z > 0

    def takes_edge(side):
        return (y == 0) & (z < deep - 1) if side == 0 else (y == across - 1) & (z > 0)

    def greet():
        barrier = pltpu.get_barrier_semaphore()

        def hello(**device):
            pl.semaphore_signal(barrier, 1, device_id=device, device_id_type=pl.DeviceIdType.MESH)

        for dr in range(2):
            for dy in range(2):
                for dt in range(2):
                    if dr or dy or dt:
                        hello(rep=moved(rep, dr), fs=z * across + moved(y, dy), tp=moved(tp, dt))
        for step_z in range(1, deep):
            hello(fs=(z + step_z) % deep * across + y)
        for up in (True, False):
            @pl.when(z < deep - 1 if up else z > 0)
            def _():
                for dr, dy in others:
                    hello(rep=moved(rep, dr), fs=(z + 1 if up else z - 1) * across + moved(y, dy))
        next_levels = (z > 0).astype(jnp.int32) + (z < deep - 1).astype(jnp.int32)
        pl.semaphore_wait(barrier, 6 + deep + len(others) * next_levels)

    def w_across(c, sink):
        if c >= chunks:
            return
        for branch, w in enumerate(weights):
            sink(remote(
                w.at[:, chunk_cols(part_of(rep, ny), c)], w_all.at[c, fs, :, lanes(branch)],
                wy_send.at[c, branch], wy_recv.at[c, branch], fs=z * across + ny,
            ))

    def w_along(c, block, up, down, sink):
        ref = w_all.at[c, block]
        if up:
            @pl.when(z < deep - 1)
            def _():
                sink(remote(ref, ref, wz_send.at[c, block, 0], wz_recv.at[c, block], fs=fs + across))
        if down:
            @pl.when(z > 0)
            def _():
                sink(remote(ref, ref, wz_send.at[c, block, 1], wz_recv.at[c, block], fs=fs - across))

    def w_local(c):
        return [
            pltpu.make_async_copy(
                w.at[:, chunk_cols(part, c)], w_all.at[c, fs, :, lanes(branch)], own_sem.at[2 * c + branch]
            ) for branch, w in enumerate(weights)
        ]

    def w_own_along(c, sink):
        w_along(c, fs, True, True, sink)

    def w_near_along(c, arrive, sink):
        if c >= chunks:
            return
        block = z * across + ny
        if arrive:
            for branch in range(2):
                landed(w_all.at[c, block, :, lanes(branch)], wy_recv.at[c, branch])
        w_along(c, block, True, True, sink)

    def w_step(c, dist, near_block, arrive, sink):
        if c >= chunks or dist >= deep:
            return
        for sign in (-1, 1):
            @pl.when((z >= dist) if sign < 0 else (z + dist < deep))
            def _():
                block = (z + sign * dist) * across + (ny if near_block else y)
                if arrive:
                    landed(w_all.at[c, block], wz_recv.at[c, block])
                w_along(c, block, sign < 0, sign > 0, sink)

    def w_relay(c, dist, near_block):
        if dist < deep - 1:
            w_step(c, dist, near_block, True, start)

    def w_last(c):
        for near_block in (False, True):
            w_step(c, deep - 1, near_block, True, start)

    def x_at(r, yy, k, half):
        offset, size = pieces[k]
        return x_all.at[r, pl.ds(pl.multiple_of(yy * tokens + offset, 16), size), cols(half)]

    def x_mine(k):
        return x_own.at[pl.ds(*pieces[k])]

    def x_across(k, sink):
        sink(remote(x_mine(k), x_at(rep, y, k, tp), x_send.at[1, k], x_recv.at[rep, y, k, tp], fs=z * across + ny))

    def x_over(k, sink):
        sink(remote(x_mine(k), x_at(rep, y, k, tp), x_send.at[0, k], x_recv.at[rep, y, k, tp], rep=nrep))

    def x_to_sibling(sink):
        for k in range(len(pieces)):
            sink(remote(x_mine(k), x_at(rep, y, k, tp), xs_send.at[rep, y, k], x_recv.at[rep, y, k, tp], tp=ntp))

    def x_forward(k, sink):
        if k < last:
            ref = x_at(rep, ny, k, tp)
            sink(remote(ref, ref, xf_send.at[k], x_recv.at[rep, ny, k, tp], rep=nrep))
        else:
            ref = x_at(nrep, y, k, tp)
            sink(remote(ref, ref, xf_send.at[k], x_recv.at[nrep, y, k, tp], fs=z * across + ny))

    def x_take(r, yy, k, forward):
        x_landed(r, yy, k, tp)
        if forward:
            x_forward(k, start)
        x_share(r, yy, k, start)

    def x_share(r, yy, k, sink):
        ref = x_at(r, yy, k, tp)
        sink(remote(ref, ref, xs_send.at[r, yy, k], x_recv.at[r, yy, k, tp], tp=ntp))

    def x_landed(r, yy, k, half):
        landed(x_at(r, yy, k, half), x_recv.at[r, yy, k, half])

    def edge_out(side, sink):
        target = fs - across if side == 0 else fs + across

        @pl.when(gives_edge(side))
        def _():
            sink(remote(
                x_own.at[near(side)], x_all.at[rep, far(side), cols(tp)], hz_send.at[side],
                hx_recv.at[side, rep, tp], fs=target,
            ))
            level = z - 1 if side == 0 else z + 1
            for dr in range(2):
                for dy in range(2):
                    r, yy = moved(rep, dr), moved(y, dy)
                    sink(remote(
                        g_own.at[near(side), all_cols(part_of(r, yy))], g_all.at[rep, far(side)],
                        hg_send.at[side, dr, dy], hg_recv.at[side, rep], rep=r, fs=level * across + yy,
                    ))

    def edge_share(side, arrive, sink):
        @pl.when(takes_edge(side))
        def _():
            ref = x_all.at[rep, far(side), cols(tp)]
            if arrive:
                landed(ref, hx_recv.at[side, rep, tp])
            for dr in range(2):
                for dy in range(2):
                    for dt in range(2):
                        if dr or dy or dt:
                            sink(remote(
                                ref, ref, hb_send.at[side, dr, dy, dt], hx_recv.at[side, rep, tp],
                                rep=moved(rep, dr), fs=z * across + moved(y, dy), tp=moved(tp, dt),
                            ))

    def edge_landed(side):
        @pl.when(has_edge(side))
        def _():
            for dr in range(2):
                r = moved(rep, dr)
                for dt in range(2):
                    half = moved(tp, dt)
                    ref, sem = x_all.at[r, far(side), cols(half)], hx_recv.at[side, r, half]
                    if dr or dt:
                        landed(ref, sem)
                    else:
                        @pl.when(jnp.logical_not(takes_edge(side)))
                        def _():
                            landed(ref, sem)
                landed(g_all.at[r, far(side)], hg_recv.at[side, r])

    def g_direct(c, sink):
        for dr, dy in others:
            r, yy = moved(rep, dr), moved(y, dy)
            sink(remote(
                g_own.at[:, chunk_cols(part_of(r, yy), c)], g_all.at[rep, token_rows(y), pl.ds(c * LANES, LANES)],
                g_send.at[c, dr, dy], g_recv.at[c, rep, y], rep=r, fs=z * across + yy,
            ))

    def g_landed(c):
        for dr, dy in others:
            r, yy = moved(rep, dr), moved(y, dy)
            landed(g_all.at[r, token_rows(yy), pl.ds(c * LANES, LANES)], g_recv.at[c, r, yy])

    x_local = pltpu.make_async_copy(
        x_own, x_all.at[rep, token_rows(y), cols(tp)], own_sem.at[2 * chunks]
    )
    g_local = pltpu.make_async_copy(
        g_own.at[:, all_cols(part)], g_all.at[rep, token_rows(y)], own_sem.at[2 * chunks + 1]
    )

    def chunk_lanes(c):
        return pl.ds(c * both, both)

    def project(c):
        @pl.loop(0, 2)
        def _(slot):
            total = jnp.dot(
                x_all[slot], w_all[c].reshape(-1, both), preferred_element_type=jnp.float32
            )
            pre[slot] = total.astype(pre.dtype)

    def mix(c):
        row = lax.broadcasted_iota(jnp.int32, (ext, LANES), 0)
        has_next, has_prev = (z < deep - 1).astype(jnp.int32), (z > 0).astype(jnp.int32)
        inside = (row < main) | ((row < main + EDGE) & (has_next > 0)) | ((row >= main + EDGE) & (has_prev > 0))
        counted = inside & (live(part, c).astype(jnp.int32) > 0)
        tap_cols = pl.ds(pl.multiple_of(tp * hid + first_col(part) + c * LANES, LANES), LANES)
        taps = [[ref[k : k + 1, tap_cols] for k in range(3)] for ref in (gate_taps, value_taps)]
        terms[:, pl.ds(c * LANES, LANES)] = jnp.zeros((8, LANES), jnp.float32)

        def before(v):
            return pltpu.roll(v, 1, 0)

        def after(v):
            return pltpu.roll(v, ext - 1, 0)

        @pl.loop(0, 2)
        def _(slot):
            pres = [jnp.where(inside, pre[slot, :, lanes(b)].astype(jnp.float32), 0.0) for b in range(2)]
            around = [(before(p), p, after(p)) for p in pres]
            gate_mix, value_mix = [sum(w * p for w, p in zip(ws, ps)) for ws, ps in zip(taps, around)]
            cot_in = jnp.where(counted, g_all[slot, :, pl.ds(c * LANES, LANES)].astype(jnp.float32), 0.0)
            sig = jax.nn.sigmoid(gate_mix)
            cots = (
                cot_in * value_mix * (sig * (1.0 + gate_mix * (1.0 - sig))),
                cot_in * (gate_mix * sig),
            )
            for b in range(2):
                ws, ps, one = taps[b], around[b], cots[b]
                back = ws[0] * after(one) + ws[1] * one + ws[2] * before(one)
                cot[slot, :, pl.ds(c * both + b * LANES, LANES)] = back[:main].astype(cot.dtype)
                for k in range(3):
                    total = jnp.sum(ps[k][:main] * one[:main], axis=0, keepdims=True)
                    terms[2 * k + b : 2 * k + b + 1, pl.ds(c * LANES, LANES)] += total * factor

    def far_first(visit):
        @pl.loop(0, 2 * deep - 1)
        def _(i):
            dist = deep - 1 - i // 2
            level = jnp.where(i % 2 == 0, z + dist, z - dist)

            @pl.when((level >= 0) & (level < deep))
            def _():
                visit(level)

    def sum_hop(c, block, up, sink):
        way = 0 if up else 1
        sink(remote(
            grads.at[c, block], from_z.at[way, c, block], sz_send.at[c, block], sz_recv.at[way, c, block],
            fs=fs + across if up else fs - across,
        ))

    def weight_terms(c):
        def visit(level):
            for yy in range(across):
                block = level * across + yy
                at = pl.ds(pl.multiple_of(block * rows, rows), rows)
                total = sum(
                    lax.dot_general(
                        x_all[slot, :main, at], cot[slot, :, chunk_lanes(c)], (((0,), (0,)), ((), ())),
                        preferred_element_type=jnp.float32,
                    ) for slot in range(2)
                )
                grads[c, block] = (total * factor).astype(grads.dtype)
            for up in (True, False):
                @pl.when((level > z) & (z == 0) if up else (level < z) & (z == deep - 1))
                def _():
                    for yy in range(across):
                        sum_hop(c, level * across + yy, up, start)

        far_first(visit)

    def inner(level, up):
        return (z > 0) & (z < deep - 1) & ((level > z) if up else (level < z))

    def pass_on(c):
        def visit(level):
            for up in (True, False):
                @pl.when(inner(level, up))
                def _():
                    way = 0 if up else 1
                    for yy in range(across):
                        block = level * across + yy
                        landed(from_z.at[way, c, block], sz_recv.at[way, c, block])
                        total = grads[c, block].astype(jnp.float32) + from_z[way, c, block].astype(jnp.float32)
                        grads[c, block] = total.astype(grads.dtype)
                        sum_hop(c, block, up, start)

        far_first(visit)

    def sums_sent(c):
        def visit(level):
            for up in (True, False):
                @pl.when((level > z) if up else (level < z))
                def _():
                    for yy in range(across):
                        sum_hop(c, level * across + yy, up, sent)

        far_first(visit)

    def to_owners(c, same, sink):
        here = chunk_cols(part, c)
        for branch, out in enumerate(outs):
            if same:
                sink(remote(
                    out.at[:, here], out.at[:, here], out_send.at[c, branch, 0], out_recv.at[c, branch, rep, y], rep=nrep
                ))
            else:
                src = fin.at[c, :, lanes(branch)]
                for k, r in ((1, rep), (2, nrep)):
                    sink(remote(
                        src, out.at[:, here], out_send.at[c, branch, k], out_recv.at[c, branch, rep, y],
                        rep=r, fs=z * across + ny,
                    ))

    def finish(c):
        for same in (False, True):
            block = z * across + (y if same else ny)
            for way in range(2):
                @pl.when(z > 0 if way == 0 else z < deep - 1)
                def _():
                    landed(from_z.at[way, c, block], sz_recv.at[way, c, block])
            total = grads[c, block].astype(jnp.float32)
            for way in range(2):
                total += from_z[way, c, block].astype(jnp.float32)
            total = total.astype(grads.dtype)

            @pl.when(live(part, c))
            def _():
                if same:
                    for branch, out in enumerate(outs):
                        out[:, chunk_cols(part, c)] = total[:, branch * LANES : (branch + 1) * LANES]
                else:
                    fin[c] = total
                to_owners(c, same, start)

    def input_terms(dr, dy):
        r, yy = moved(rep, dr), moved(y, dy)
        q = part_of(r, yy)

        @pl.loop(0, 2 * blocks)
        def _(i):
            half = jnp.where(i < blocks, ntp, tp)
            j = i % blocks
            total = sum(
                lax.dot_general(
                    cot[r, token_rows(yy), chunk_lanes(c)], w_all[c, half * blocks + j],
                    (((1,), (1,)), ((), ())), preferred_element_type=jnp.float32,
                ) for c in range(chunks)
            )
            pv[half, q, :, pl.ds(pl.multiple_of(j * rows, rows), rows)] = total.astype(pv.dtype)

        tp_hop(q, start)

    def tp_hop(q, sink):
        sink(remote(pv.at[ntp, q], from_tp.at[q], tp_send.at[q], tp_recv.at[q], tp=ntp))

    def f_cols(f):
        return pl.ds(f * half_feats, half_feats)

    def first_hop(f, k, sink):
        q = part_of(nrep, ny) if k else part_of(nrep, y) if f == 0 else part_of(rep, ny)
        target = dict(rep=nrep) if f == 0 else dict(fs=z * across + ny)
        sink(remote(pv.at[tp, q, :, f_cols(f)], first_got.at[f, k], s1_send.at[f, k], s1_recv.at[f, k], **target))

    def second_hop(f, sink):
        q = part_of(rep, ny) if f == 0 else part_of(nrep, y)
        target = dict(fs=z * across + ny) if f == 0 else dict(rep=nrep)
        sink(remote(pv.at[tp, q, :, f_cols(f)], second_got.at[f], s2_send.at[f], s2_recv.at[f], **target))

    def row_tiles(body):
        @pl.loop(0, tokens // 16)
        def _(i):
            body(pl.ds(pl.multiple_of(i * 16, 16), 16))

    def add_sibling(q):
        landed(from_tp.at[q], tp_recv.at[q])

        def body(at):
            total = pv[tp, q, at].astype(jnp.float32) + from_tp[q, at].astype(jnp.float32)
            pv[tp, q, at] = total.astype(pv.dtype)

        row_tiles(body)

    def input_first(dr, dy):
        add_sibling(part_of(moved(rep, dr), moved(y, dy)))
        if dr:
            first_hop(0, dy, start)
        if dy:
            first_hop(1, dr, start)

    def input_second():
        for f in range(2):
            q = part_of(rep, ny) if f == 0 else part_of(nrep, y)
            landed(first_got.at[f, 1], s1_recv.at[f, 1])

            def body(at):
                total = pv[tp, q, at, f_cols(f)].astype(jnp.float32) + first_got[f, 1, at].astype(jnp.float32)
                pv[tp, q, at, f_cols(f)] = total.astype(pv.dtype)

            row_tiles(body)
            second_hop(f, start)

    def input_last():
        landed(from_tp.at[part], tp_recv.at[part])
        for f in range(2):
            landed(first_got.at[f, 0], s1_recv.at[f, 0])
            landed(second_got.at[f], s2_recv.at[f])

        def body(at):
            for f in range(2):
                total = pv[tp, part, at, f_cols(f)].astype(jnp.float32) + from_tp[part, at, f_cols(f)].astype(jnp.float32)
                total += first_got[f, 0, at].astype(jnp.float32) + second_got[f, at].astype(jnp.float32)
                in_grad[at, f_cols(f)] = total.astype(in_grad.dtype)

        row_tiles(body)

    def taps_along(sink):
        for step in range(1, deep):
            to = (z + step) % deep
            sink(remote(
                terms_z.at[z], terms_z.at[z], tz_send.at[step], tz_recv.at[z], fs=to * across + y
            ))

    def taps_start():
        terms_z[z] = terms[...]
        taps_along(start)

    def taps_out(sink):
        ref = terms_all.at[rep, y, tp]
        for dr in range(2):
            for dy in range(2):
                for dt in range(2):
                    if dr or dy or dt:
                        sink(remote(
                            ref, ref, ta_send.at[dr, dy, dt], ta_recv.at[rep, y, tp],
                            rep=moved(rep, dr), fs=z * across + moved(y, dy), tp=moved(tp, dt),
                        ))

    def taps_sum():
        for step in range(1, deep):
            source = (z + step) % deep
            landed(terms_z.at[source], tz_recv.at[source])
        terms_all[rep, y, tp] = sum(terms_z[level] for level in range(deep))
        taps_out(start)

    def taps_last():
        for dr in range(2):
            for dy in range(2):
                for dt in range(2):
                    if dr or dy or dt:
                        at = (moved(rep, dr), moved(y, dy), moved(tp, dt))
                        landed(terms_all.at[at], ta_recv.at[at])
        for r in range(2):
            for yy in range(across):
                which = r * across + yy
                first = min(which * width, hid - width)
                skip = which * width - first
                for half in range(2):
                    for branch, out in enumerate((gate_taps_out, value_taps_out)):
                        for k in range(3):
                            if skip < width:
                                begin = half * hid + first + skip
                                out[k : k + 1, begin : begin + width - skip] = terms_all[
                                    r, yy, half, 2 * k + branch : 2 * k + branch + 1, skip:
                                ]

    for c in range(chunks):
        for copy in w_local(c):
            copy.start()
    x_local.start()
    g_local.start()
    for way in range(2):
        @pl.when((z == 0) if way == 0 else (z == deep - 1))
        def _():
            for c in range(chunks):
                for yy in range(across):
                    from_z[way, c, z * across + yy] = jnp.zeros((rows, both), from_z.dtype)
    greet()

    w_across(0, start)
    x_across(0, start)
    w_across(1, start)
    x_across(1, start)
    w_across(2, start)
    x_across(2, start)
    for k in (2, 0, 1):
        x_over(k, start)
    for side in range(2):
        edge_out(side, start)
    x_to_sibling(start)
    for c in range(chunks):
        for copy in w_local(c):
            copy.wait()
        w_own_along(c, start)
    for c in range(3, chunks):
        w_across(c, start)

    w_near_along(0, True, start)
    for side in range(2):
        edge_share(side, True, start)
    w_relay(0, 1, False)
    x_take(nrep, y, 2, True)
    w_relay(1, 1, False)
    x_take(rep, ny, 0, True)
    w_relay(0, 1, True)
    w_near_along(1, True, start)
    w_relay(2, 1, False)
    for dist in range(2, deep):
        w_relay(0, dist, False)
        w_relay(0, dist, True)
    x_take(rep, ny, 1, True)
    for c in range(chunks):
        g_direct(c, start)
    for k in (0, 1):
        x_take(nrep, y, k, False)
    w_near_along(2, True, start)
    w_relay(1, 1, True)
    for dist in range(2, deep):
        w_relay(1, dist, False)
    x_take(nrep, ny, 0, False)
    x_take(rep, ny, 2, False)
    for dist in range(2, deep):
        w_relay(1, dist, True)
    w_relay(2, 1, True)
    for k in (1, 2):
        x_take(nrep, ny, k, False)
    x_local.wait()
    for r in range(2):
        for yy in range(across):
            for k in range(len(pieces)):
                x_landed(r, yy, k, ntp)
    for side in range(2):
        edge_landed(side)
    g_local.wait()

    order = ((1, 1), (0, 1), (1, 0), (0, 0))
    for c in range(chunks):
        w_last(c)
        project(c)
        if c == 0:
            for dist in range(2, deep):
                w_relay(2, dist, False)
        g_landed(c)
        mix(c)
        if c == 0:
            for dist in range(2, deep):
                w_relay(2, dist, True)
        for later in range(c + 3, c + 4):
            w_near_along(later, True, start)
            for dist in range(1, deep):
                w_relay(later, dist, False)
                w_relay(later, dist, True)
        if c < chunks - 1 or c == 0:
            weight_terms(c)
        if c == chunks - 2:
            for early in range(chunks - 2):
                pass_on(early)
    taps_start()
    input_terms(*order[0])
    input_terms(*order[1])
    input_first(*order[0])
    if chunks > 2:
        finish(0)
    input_terms(*order[2])
    input_first(*order[1])
    input_terms(*order[3])
    input_first(*order[2])
    if chunks > 1:
        weight_terms(chunks - 1)
    for c in range(1, chunks - 2):
        finish(c)
    if chunks > 1:
        pass_on(chunks - 2)
    input_second()
    if chunks > 1:
        finish(chunks - 2)
    taps_sum()
    pass_on(chunks - 1)
    finish(chunks - 1)
    input_last()
    taps_last()
    for dr, dy in others:
        r, yy = moved(rep, dr), moved(y, dy)
        for c in range(chunks):
            @pl.when(live(part_of(r, yy), c))
            def _():
                at = chunk_cols(part_of(r, yy), c)
                for branch, out in enumerate(outs):
                    landed(out.at[:, at], out_recv.at[c, branch, r, yy])

    for side in range(2):
        edge_out(side, sent)
        edge_share(side, False, sent)
    x_to_sibling(sent)
    for k in range(len(pieces)):
        x_across(k, sent)
        x_over(k, sent)
        x_forward(k, sent)
        for dr, dy in others:
            x_share(moved(rep, dr), moved(y, dy), k, sent)
    for c in range(chunks):
        w_across(c, sent)
        w_own_along(c, sent)
        w_near_along(c, False, sent)
        for dist in range(1, deep):
            for near_block in (False, True):
                w_step(c, dist, near_block, False, sent)
        g_direct(c, sent)
        sums_sent(c)

        @pl.when(live(part, c))
        def _():
            for same in (False, True):
                to_owners(c, same, sent)
    for dr in range(2):
        for dy in range(2):
            tp_hop(part_of(moved(rep, dr), moved(y, dy)), sent)
    for f in range(2):
        for k in range(2):
            first_hop(f, k, sent)
        second_hop(f, sent)
    taps_along(sent)
    taps_out(sent)


def fused_all(across, x_own, gate_w, value_w, gate_taps, value_taps, g_own):
    reps, fs_count, tps = (lax.axis_size(a) for a in ("rep", "fs", "tp"))
    deep = fs_count // across
    tokens, feats = x_own.shape
    rows, hid = gate_w.shape
    width = part_width(hid, reps * across)
    chunks = width // LANES
    both = 2 * LANES
    main = across * tokens
    ext = main + 2 * EDGE
    half = feats // 2
    parts = reps * across
    factor = float(tokens * fs_count * reps) ** (-0.5)
    dtype = x_own.dtype
    f32 = jnp.float32
    sem = pltpu.SemaphoreType.DMA
    sems = [
        (2 * chunks + 2,), (chunks, 2), (chunks, 2), (chunks, fs_count, 2), (chunks, fs_count), (2, 3), (3,),
        (reps, across, 3), (reps, across, 3, tps), (2,), (2, 2, 2, 2), (2, reps, tps),
        (chunks, 2, 2), (chunks, reps, across), (2, 2, 2), (2, reps), (chunks, fs_count), (2, chunks, fs_count),
        (chunks, 2, 3), (chunks, 2, reps, across), (parts,), (parts,),
        (2, 2), (2, 2), (2,), (2,), (deep,), (deep,), (2, 2, 2), (reps, across, tps),
    ]
    buffers = [
        ((reps, ext, tps * feats), dtype), ((chunks, fs_count, rows, both), dtype), ((reps, ext, width), dtype),
        ((reps, ext, both), dtype), ((reps, main, 2 * width), dtype), ((chunks, fs_count, rows, both), dtype),
        ((2, chunks, fs_count, rows, both), dtype), ((chunks, rows, both), dtype),
        ((tps, parts, tokens, feats), dtype), ((parts, tokens, feats), dtype),
        ((2, 2, tokens, half), dtype), ((2, tokens, half), dtype),
        ((8, width), f32), ((deep, 8, width), f32), ((reps, across, tps, 8, width), f32),
    ]
    vmem = pl.BlockSpec(memory_space=pltpu.VMEM)
    return pl.pallas_call(
        functools.partial(fused_kernel, (deep, across, width), factor),
        out_shape=(
            jax.ShapeDtypeStruct((tokens, feats), dtype),
            jax.ShapeDtypeStruct((rows, hid), dtype),
            jax.ShapeDtypeStruct((rows, hid), dtype),
            jax.ShapeDtypeStruct(gate_taps.shape, f32),
            jax.ShapeDtypeStruct(value_taps.shape, f32),
        ),
        in_specs=[vmem] * 6,
        out_specs=(vmem,) * 5,
        scratch_shapes=[pltpu.VMEM(*b) for b in buffers] + [sem(s) for s in sems],
        compiler_params=pltpu.CompilerParams(has_side_effects=True, collective_id=0, vmem_limit_bytes=60000 * 1024),
        name="fused_all",
    )(x_own, gate_w, value_w, gate_taps, value_taps, g_own)


def fits_plane(across, inputs, gate_proj):
    reps, fs_count, tps = (lax.axis_size(a) for a in ("rep", "fs", "tp"))
    tokens, feats = inputs.shape[1:]
    rows, hid = gate_proj.shape
    parts = reps * across
    width = part_width(hid, parts)
    return (
        reps == across == tps == 2 and fs_count > across and tokens % 16 == 0 and tokens >= 48
        and hid % LANES == 0 and rows % LANES == 0 and feats % rows == 0 and feats % (2 * LANES) == 0
        and 4 * parts * width <= 5 * hid
    )


def shards(across, inputs, gate_proj, value_proj, gate_taps, value_taps, out_grad):
    if fits_plane(across, inputs, gate_proj):
        in_grad, gate_grad, value_grad, gate_terms, value_terms = fused_all(
            across, inputs[0], gate_proj, value_proj, gate_taps, value_taps, out_grad[0]
        )
        return in_grad[None], gate_grad.astype(jnp.float32), value_grad.astype(jnp.float32), gate_terms, value_terms

    contract_cols = (((1,), (1,)), ((), ()))
    contract_rows = (((0,), (0,)), ((), ()))
    reps, fs_count = lax.axis_size("rep"), lax.axis_size("fs")
    rep = lax.axis_index("rep")
    tokens, feats = inputs.shape[1:]
    hid = gate_proj.shape[1]
    width = min(hid, -(-hid // reps // 128) * 128)
    last = hid - width

    def start_of(part):
        return jnp.minimum(part * width, last)

    first = start_of(rep)
    dead = rep * width - first
    live = jnp.arange(width) >= dead

    def part_cols(x, part):
        return lax.dynamic_slice_in_dim(x, start_of(part), width, x.ndim - 1)

    w_own = jnp.concatenate(
        [jnp.where(live, part_cols(w, rep), jnp.zeros((), w.dtype)) for w in (gate_proj, value_proj)], axis=1
    )
    g_parts = jnp.stack([part_cols(out_grad[0], (rep + step) % reps) for step in range(reps)])
    x_all, g_all, w_all = gather_all(inputs[0], g_parts, w_own, across)
    w_all = w_all.reshape(-1, 2 * width)

    ext = tokens + 2 * HALO
    pre = jnp.dot(x_all.reshape(reps * ext, -1), w_all, preferred_element_type=jnp.float32)
    pre = pre.astype(jnp.bfloat16).reshape(reps, ext, 2 * width)
    tap_start = lax.axis_index("tp") * hid + first
    taps = jnp.concatenate(
        [lax.dynamic_slice_in_dim(t, tap_start, width, 1) for t in (gate_taps, value_taps)], axis=1
    )
    factor = float(tokens * fs_count * reps) ** (-0.5)
    pre_cot, tap_terms = mix_all(pre, g_all, taps, tokens, fs_count, factor)
    pre_cot = pre_cot.reshape(reps * tokens, 2 * width)
    tap_terms = tap_terms[:3]

    grads = lax.dot_general(
        x_all[:, :tokens].reshape(reps * tokens, -1), pre_cot, contract_rows, preferred_element_type=jnp.float32
    )
    grads = (grads * factor).astype(jnp.bfloat16).reshape(fs_count, -1, 2 * width)
    partial_value = lax.dot_general(pre_cot, w_all, contract_cols, preferred_element_type=jnp.float32)
    partial_value = partial_value.astype(jnp.bfloat16).reshape(reps, tokens, -1)
    lanes = -(-tap_terms.size // 1024) * 128
    tap_terms = jnp.pad(tap_terms.reshape(-1), (0, 8 * lanes - tap_terms.size)).reshape(8, lanes)
    own, in_grad, tap_all = scatter_all(grads, partial_value, tap_terms, across)

    skips = [max(0, p * width - last) for p in range(reps)]
    proj_grads = [
        jnp.concatenate(
            [own[p, :, branch * width + skips[p] : (branch + 1) * width] for p in range(reps)], axis=1
        ).astype(jnp.float32)
        for branch in range(2)
    ]
    tap_all = tap_all.reshape(reps, -1, 8 * lanes)[:, :, : 6 * width].reshape(reps, -1, 3, 2, width)
    taps_out = jnp.concatenate(
        [tap_all[p, half, :, :, skips[p] :] for half in range(tap_all.shape[1]) for p in range(reps)], axis=2
    )
    return in_grad[None], proj_grads[0], proj_grads[1], taps_out[:, 0], taps_out[:, 1]


def solution(mesh):
    placed = (P("rep", "fs", "tp"), P("fs", "tp"), P("fs", "tp"), P(), P(), P("rep", "fs", "tp"))
    return jax.shard_map(
        functools.partial(shards, row_length(mesh)),
        mesh=mesh,
        in_specs=placed,
        out_specs=(P("rep", "fs", "tp"), P("fs", "tp"), P("fs", "tp"), P(), P()),
        check_vma=False,
    )
```

```python
import functools

import jax
import jax.numpy as jnp
from jax import lax
from jax.experimental import pallas as pl
from jax.experimental.pallas import tpu as pltpu
from jax.sharding import PartitionSpec as P

HALO = 8


def row_length(mesh):
    axis = mesh.axis_names.index("fs")
    devices = mesh.devices.swapaxes(0, axis)
    line = devices.reshape(devices.shape[0], -1)[:, 0]
    places = [tuple(getattr(d, "coords", (i,))) for i, d in enumerate(line)]
    moved = lambda a, b: [i for i in range(len(a)) if a[i] != b[i]]
    length = 1
    while length < len(places) and moved(places[0], places[length]) == moved(places[0], places[1]):
        length += 1
    return length if len(places) % length == 0 else 1


def remote(src, dst, send, recv, **device):
    return pltpu.make_async_remote_copy(
        src_ref=src, dst_ref=dst, send_sem=send, recv_sem=recv, device_id=device, device_id_type=pl.DeviceIdType.MESH
    )


def gather_kernel(
    sizes, x_ref, g_ref, w_ref, x_all, g_all, w_all,
    w_send, w_recv, xr_send, xt_send, x_recv, xh_send, xh_recv, g_send, g_recv, gh_send, gh_recv, own_sem,
):
    reps, fs_count, tps, across = sizes
    deep = fs_count // across
    rep, fs, tp = (lax.axis_index(a) for a in ("rep", "fs", "tp"))
    z, y = fs // across, fs % across
    tokens, feats = x_ref.shape

    def other(axis_index, step, count):
        return (axis_index + step) % count

    def cols(index):
        return pl.ds(pl.multiple_of(index * feats, feats), feats)

    half_width = w_ref.shape[1] // 2

    def half(c):
        return pl.ds(c * half_width, half_width)

    def send_w(block, c, src, way, target):
        return remote(
            src.at[:, half(c)], w_all.at[block, :, half(c)], w_send.at[block, c, way], w_recv.at[block, c], fs=target
        )

    def along(block, c, src, down, up, sink):
        if down:
            @pl.when(z > 0)
            def _():
                sink(send_w(block, c, src, 0, fs - across))
        if up:
            @pl.when(z < deep - 1)
            def _():
                sink(send_w(block, c, src, 1, fs + across))

    def to_row(block, c, src, sink):
        for step in range(1, across):
            sink(send_w(block, c, src, 1 + step, z * across + other(y, step, across)))

    start = lambda c: c.start()
    sent = lambda c: c.wait_send()

    def x_main(slot, src, sem, **device):
        return remote(src, x_all.at[slot, pl.ds(0, tokens), cols(tp)], sem, x_recv.at[slot, tp], **device)

    def halos(sink):
        for side in range(2):
            near = pl.ds(0, HALO) if side == 0 else pl.ds(tokens - HALO, HALO)
            far = pl.ds(tokens + side * HALO, HALO)
            target = fs - 1 if side == 0 else fs + 1

            @pl.when((fs > 0) if side == 0 else (fs < fs_count - 1))
            def _():
                for slot in range(reps):
                    to_rep = other(rep, slot, reps)
                    for step in range(tps):
                        sink(remote(
                            x_ref.at[near], x_all.at[slot, far, cols(tp)], xh_send.at[side, slot, step],
                            xh_recv.at[side, slot, tp], rep=to_rep, fs=target, tp=other(tp, step, tps),
                        ))
                    sink(remote(
                        g_ref.at[slot, near], g_all.at[slot, far], gh_send.at[side, slot],
                        gh_recv.at[side, slot], rep=to_rep, fs=target,
                    ))

    def to_reps(sink):
        for slot in range(1, reps):
            sink(x_main(slot, x_ref, xr_send.at[slot], rep=other(rep, slot, reps)))
        for slot in range(1, reps):
            sink(remote(
                g_ref.at[slot], g_all.at[slot, pl.ds(0, tokens)], g_send.at[slot], g_recv.at[slot],
                rep=other(rep, slot, reps),
            ))

    def to_tps(slot, src, sink):
        for step in range(1, tps):
            sink(x_main(slot, src, xt_send.at[slot, step], tp=other(tp, step, tps)))

    halos(start)
    for c in range(2):
        along(fs, c, w_ref, True, True, start)
        to_row(fs, c, w_ref, start)
    to_reps(start)
    to_tps(0, x_ref, start)
    own = [
        pltpu.make_async_copy(w_ref, w_all.at[fs], own_sem.at[0]),
        pltpu.make_async_copy(x_ref, x_all.at[0, pl.ds(0, tokens), cols(tp)], own_sem.at[1]),
        pltpu.make_async_copy(g_ref.at[0], g_all.at[0, pl.ds(0, tokens)], own_sem.at[2]),
    ]
    for copy in own:
        copy.start()

    def landed(ref, sem):
        pltpu.make_async_copy(ref, ref, sem).wait()

    def hops(dist, arrive, sink):
        for sign in (-1, 1):
            block = fs + sign * dist * across

            @pl.when((z >= dist) if sign < 0 else (z + dist < deep))
            def _():
                for c in range(2):
                    if arrive:
                        landed(w_all.at[block, :, half(c)], w_recv.at[block, c])
                    along(block, c, w_all.at[block], sign > 0, sign < 0, sink)
                    if c == 0:
                        to_row(block, c, w_all.at[block], sink)
                    else:
                        level = z + sign * dist

                        @pl.when((level > 0) & (level < deep - 1))
                        def _():
                            to_row(block, c, w_all.at[block], sink)

    def across_first(dist, arrive, sink):
        for end in ((0, deep - 1) if deep > 1 else (0,)):
            @pl.when(z == end + dist if end == 0 else z == end - dist)
            def _():
                for step in range(1, across):
                    block = end * across + other(y, step, across)
                    if arrive:
                        landed(w_all.at[block, :, half(1)], w_recv.at[block, 1])
                    along(block, 1, w_all.at[block], end > 0, end == 0 and deep > 1, sink)

    def forward_x(arrive, sink):
        for slot in range(1, reps):
            mine = x_all.at[slot, pl.ds(0, tokens), cols(tp)]
            if arrive:
                landed(mine, x_recv.at[slot, tp])
            to_tps(slot, mine, sink)

    for dist in range(1, deep):
        hops(dist, True, start)
        across_first(dist - 1, True, start)
        if dist == 1:
            forward_x(True, start)
    if deep == 1:
        forward_x(True, start)
    across_first(deep - 1, True, start)

    for slot in range(reps):
        for step in range(1, tps):
            source = other(tp, step, tps)
            landed(x_all.at[slot, pl.ds(0, tokens), cols(source)], x_recv.at[slot, source])
        if slot:
            landed(g_all.at[slot, pl.ds(0, tokens)], g_recv.at[slot])
    for side in range(2):
        far = pl.ds(tokens + side * HALO, HALO)

        @pl.when((fs < fs_count - 1) if side == 0 else (fs > 0))
        def _():
            for slot in range(reps):
                for source in range(tps):
                    landed(x_all.at[slot, far, cols(source)], xh_recv.at[side, slot, source])
                landed(g_all.at[slot, far], gh_recv.at[side, slot])
    for level in range(deep):
        for step in range(1, across):
            block = level * across + other(y, step, across)
            landed(w_all.at[block, :, half(0)], w_recv.at[block, 0])
            if 0 < level < deep - 1:
                landed(w_all.at[block, :, half(1)], w_recv.at[block, 1])
    for copy in own:
        copy.wait()
    halos(sent)
    for c in range(2):
        along(fs, c, w_ref, True, True, sent)
        to_row(fs, c, w_ref, sent)
    to_reps(sent)
    to_tps(0, x_ref, sent)
    for dist in range(1, deep):
        hops(dist, False, sent)
    for dist in range(deep):
        across_first(dist, False, sent)
    forward_x(False, sent)


def gather_all(x_own, g_parts, w_own, across):
    reps, fs_count, tps = (lax.axis_size(a) for a in ("rep", "fs", "tp"))
    tokens, feats = x_own.shape
    width = g_parts.shape[2]
    ext = tokens + 2 * HALO
    sems = [
        (fs_count, 2, 1 + across), (fs_count, 2), (reps,), (reps, tps), (reps, tps), (2, reps, tps), (2, reps, tps),
        (reps,), (reps,), (2, reps), (2, reps), (3,),
    ]
    vmem, hbm = pl.BlockSpec(memory_space=pltpu.VMEM), pl.BlockSpec(memory_space=pl.ANY)
    return pl.pallas_call(
        functools.partial(gather_kernel, (reps, fs_count, tps, across)),
        out_shape=(
            jax.ShapeDtypeStruct((reps, ext, feats * tps), x_own.dtype),
            jax.ShapeDtypeStruct((reps, ext, width), g_parts.dtype),
            jax.ShapeDtypeStruct((fs_count,) + w_own.shape, w_own.dtype),
        ),
        in_specs=[vmem] * 3,
        out_specs=(hbm,) * 3,
        scratch_shapes=[pltpu.SemaphoreType.DMA(s) for s in sems],
        compiler_params=pltpu.CompilerParams(has_side_effects=True),
        name="gather_all",
    )(x_own, g_parts, w_own)


def scatter_kernel(
    sizes, grads, pv, taps, own_all, in_grad, taps_all, y_got, z_got, tp_got, rep_got, taps_got,
    y_send, y_recv, z_send, z_recv, tp_send, tp_recv, rep_send, rep_recv, own_send, own_recv,
    taps_send, taps_recv, all_send, all_recv,
):
    reps, fs_count, tps, across = sizes
    deep = fs_count // across
    rep, fs, tp = (lax.axis_index(a) for a in ("rep", "fs", "tp"))
    z, y = fs // across, fs % across
    rows, width = grads.shape[1], grads.shape[2] // 2
    tokens, feats = in_grad.shape

    def other(axis_index, step, count):
        return (axis_index + step) % count

    def part(c):
        return pl.ds(c * width, width)

    def cols(index):
        return pl.ds(pl.multiple_of(index * feats, feats), feats)

    start = lambda c: c.start()
    sent = lambda c: c.wait_send()

    def landed(ref, sem):
        pltpu.make_async_copy(ref, ref, sem).wait()

    def tap_terms(sink):
        for step in range(1, fs_count):
            sink(remote(taps, taps_got.at[step], taps_send.at[step], taps_recv.at[step], fs=other(fs, step, fs_count)))

    def y_block(c, level, sink):
        for step in range(1, across):
            to = other(y, step, across)
            sink(remote(
                grads.at[level * across + to, :, part(c)], y_got.at[step, level, c],
                y_send.at[step, level, c], y_recv.at[step, level, c], fs=z * across + to,
            ))

    def far_first(visit):
        for dist in range(deep - 1, 0, -1):
            for way in range(2):
                @pl.when((z + dist < deep) if way == 0 else (z >= dist))
                def _():
                    visit(z + dist if way == 0 else z - dist, way)

    def y_sends(sink):
        for c in range(2):
            far_first(lambda level, way: y_block(c, level, sink))
            y_block(c, z, sink)

    def to_tps(sink):
        for slot in list(range(1, reps)) + [0]:
            for step in range(1, tps):
                to = other(tp, step, tps)
                sink(remote(
                    pv.at[slot, :, cols(to)], tp_got.at[slot, step], tp_send.at[slot, step], tp_recv.at[slot, step], tp=to
                ))

    def to_reps(sink):
        for slot in range(1, reps):
            sink(remote(
                rep_got.at[0, slot], rep_got.at[1, slot], rep_send.at[slot], rep_recv.at[slot],
                rep=other(rep, reps - slot, reps),
            ))

    def z_hop(c, level, way, sink):
        sink(remote(
            grads.at[level * across + y, :, part(c)], z_got.at[way, level, c],
            z_send.at[way, level, c], z_recv.at[way, level, c], fs=fs + across if way == 0 else fs - across,
        ))

    def own_rep(c, sink):
        mine = own_all.at[rep, :, part(c)]
        for step in range(1, reps):
            sink(remote(mine, mine, own_send.at[step, c], own_recv.at[step, c], rep=other(rep, step, reps)))

    def taps_out(sink):
        mine = taps_all.at[rep, tp]
        for slot in range(reps):
            for step in range(tps):
                if slot or step:
                    sink(remote(
                        mine, mine, all_send.at[slot, step], all_recv.at[slot, step],
                        rep=other(rep, slot, reps), tp=other(tp, step, tps),
                    ))

    tap_terms(start)
    to_tps(start)
    y_sends(start)

    for way in range(2):
        @pl.when((z == 0) if way == 0 else (z == deep - 1))
        def _():
            @pl.loop(0, deep)
            def _(level):
                for c in range(2):
                    @pl.loop(0, rows // 16)
                    def _(i):
                        z_got[way, level, c, pl.ds(pl.multiple_of(i * 16, 16), 16)] = jnp.zeros((16, width), z_got.dtype)

    def own_tps(slot, at):
        total = pv[slot, at, cols(tp)].astype(jnp.float32)
        for step in range(1, tps):
            total += tp_got[slot, step, at].astype(jnp.float32)
        return total

    for slot in range(1, reps):
        for step in range(1, tps):
            landed(tp_got.at[slot, step], tp_recv.at[slot, step])

        @pl.loop(0, tokens // 16)
        def _(i):
            at = pl.ds(pl.multiple_of(i * 16, 16), 16)
            rep_got[0, slot, at] = own_tps(slot, at).astype(rep_got.dtype)
    to_reps(start)

    def add_up(c, level, ways, store):
        for step in range(1, across):
            landed(y_got.at[step, level, c], y_recv.at[step, level, c])
        for way in ways:
            @pl.when((z > 0) if way == 0 else (z < deep - 1))
            def _():
                landed(z_got.at[way, level, c], z_recv.at[way, level, c])

        @pl.loop(0, rows // 16)
        def _(i):
            at = pl.ds(pl.multiple_of(i * 16, 16), 16)
            total = grads[level * across + y, at, part(c)].astype(jnp.float32)
            for step in range(1, across):
                total += y_got[step, level, c, at].astype(jnp.float32)
            for way in ways:
                total += z_got[way, level, c, at].astype(jnp.float32)
            store(at, total.astype(grads.dtype))

    def pass_on(c, level, way):
        def store(at, value):
            grads[level * across + y, at, part(c)] = value

        add_up(c, level, (way,), store)
        z_hop(c, level, way, start)

    for c in range(2):
        far_first(lambda level, way: pass_on(c, level, way))

        def store(at, value):
            own_all[rep, at, part(c)] = value

        add_up(c, z, (0, 1), store)
        own_rep(c, start)
        if c == 0:
            total = taps[...]
            for step in range(1, fs_count):
                landed(taps_got.at[step], taps_recv.at[step])
                total += taps_got[step]
            taps_all[rep, tp] = total
            taps_out(start)
            for step in range(1, tps):
                landed(tp_got.at[0, step], tp_recv.at[0, step])
            for slot in range(1, reps):
                landed(rep_got.at[1, slot], rep_recv.at[slot])

            @pl.loop(0, tokens // 16)
            def _(i):
                at = pl.ds(pl.multiple_of(i * 16, 16), 16)
                total = own_tps(0, at)
                for slot in range(1, reps):
                    total += rep_got[1, slot, at].astype(jnp.float32)
                in_grad[at] = total.astype(in_grad.dtype)

    for slot in range(reps):
        for step in range(tps):
            if slot or step:
                landed(taps_all.at[other(rep, reps - slot, reps), other(tp, tps - step, tps)], all_recv.at[slot, step])
    for step in range(1, reps):
        for c in range(2):
            landed(own_all.at[other(rep, reps - step, reps), :, part(c)], own_recv.at[step, c])
    tap_terms(sent)
    to_tps(sent)
    y_sends(sent)
    to_reps(sent)
    for c in range(2):
        far_first(lambda level, way: z_hop(c, level, way, sent))
        own_rep(c, sent)
    taps_out(sent)


def scatter_all(grads, pv, taps, across):
    reps, fs_count, tps = (lax.axis_size(a) for a in ("rep", "fs", "tp"))
    deep = fs_count // across
    rows, width = grads.shape[1], grads.shape[2] // 2
    tokens, feats = pv.shape[1], pv.shape[2] // tps
    sem = pltpu.SemaphoreType.DMA
    pairs = [
        (across, deep, 2), (2, deep, 2), (reps, tps), (reps,), (reps, 2), (fs_count,), (reps, tps),
    ]
    vmem = pl.BlockSpec(memory_space=pltpu.VMEM)
    return pl.pallas_call(
        functools.partial(scatter_kernel, (reps, fs_count, tps, across)),
        out_shape=(
            jax.ShapeDtypeStruct((reps, rows, 2 * width), grads.dtype),
            jax.ShapeDtypeStruct((tokens, feats), pv.dtype),
            jax.ShapeDtypeStruct((reps, tps) + taps.shape, taps.dtype),
        ),
        in_specs=[vmem] * 3,
        out_specs=(vmem,) * 3,
        scratch_shapes=[
            pltpu.VMEM((across, deep, 2, rows, width), grads.dtype),
            pltpu.VMEM((2, deep, 2, rows, width), grads.dtype),
            pltpu.VMEM((reps, tps, tokens, feats), pv.dtype),
            pltpu.VMEM((2, reps, tokens, feats), pv.dtype),
            pltpu.VMEM((fs_count,) + taps.shape, taps.dtype),
        ] + [sem(p) for p in pairs for _ in range(2)],
        compiler_params=pltpu.CompilerParams(has_side_effects=True, vmem_limit_bytes=58 * 1024 * 1024),
        name="scatter_all",
    )(grads, pv, taps)


def mix_kernel(fs_count, factor, pre, g, taps, pre_cot, terms):
    reps, ext, width = g.shape
    tokens = pre_cot.shape[1]
    fs = lax.axis_index("fs")
    row = lax.broadcasted_iota(jnp.int32, (ext, 128), 0)
    has_next, has_prev = (fs < fs_count - 1).astype(jnp.int32), (fs > 0).astype(jnp.int32)
    inside = (row < tokens) | ((row < tokens + HALO) & (has_next > 0)) | ((row >= tokens + HALO) & (has_prev > 0))

    def before(x):
        return pltpu.roll(x, 1, 0)

    def after(x):
        return pltpu.roll(x, ext - 1, 0)

    terms[...] = jnp.zeros_like(terms)

    @pl.loop(0, width // 128)
    def _(j):
        spots = [pl.ds(pl.multiple_of(branch * width + j * 128, 128), 128) for branch in range(2)]
        weights = [[taps[k : k + 1, at] for k in range(3)] for at in spots]
        for slot in range(reps):
            pres = [jnp.where(inside, pre[slot, :, at].astype(jnp.float32), 0.0) for at in spots]
            around = [(before(p), p, after(p)) for p in pres]
            gate_mix, value_mix = [sum(w * p for w, p in zip(ws, ps)) for ws, ps in zip(weights, around)]
            cot_in = jnp.where(inside, g[slot, :, spots[0]].astype(jnp.float32), 0.0)
            sig = jax.nn.sigmoid(gate_mix)
            cots = (
                cot_in * value_mix * (sig * (1.0 + gate_mix * (1.0 - sig))),
                cot_in * (gate_mix * sig),
            )
            for at, ws, ps, cot in zip(spots, weights, around, cots):
                back = ws[0] * after(cot) + ws[1] * cot + ws[2] * before(cot)
                pre_cot[slot, :, at] = back[:tokens].astype(pre_cot.dtype)
                for k in range(3):
                    total = jnp.sum(ps[k][:tokens] * cot[:tokens], axis=0, keepdims=True)
                    terms[k : k + 1, at] += total * factor


def mix_all(pre, g, taps, tokens, fs_count, factor):
    reps, ext, both = pre.shape
    vmem = pl.BlockSpec(memory_space=pltpu.VMEM)
    return pl.pallas_call(
        functools.partial(mix_kernel, fs_count, factor),
        out_shape=(
            jax.ShapeDtypeStruct((reps, tokens, both), pre.dtype),
            jax.ShapeDtypeStruct((8, both), jnp.float32),
        ),
        in_specs=[vmem] * 3,
        out_specs=(vmem,) * 2,
        compiler_params=pltpu.CompilerParams(vmem_limit_bytes=40000 * 1024),
        name="mix_all",
    )(pre, g, taps)


LANES = 128
EDGE = 16


def part_width(hid, parts):
    return min(hid, -(-hid // parts // LANES) * LANES)


TUNED = (
    ("weights_y", 0), ("weights_y", 1), ("tokens_x", 0), ("own", 2), ("own", 0), ("tokens_y", 1), ("near", 0),
    ("tokens_x", 2), ("relay", 0, 1, False), ("relay", 0, 1, True), ("tokens_x", 1), ("relay", 0, 2, False),
    ("tokens_y", 0), ("near", 1), ("weights_y", 2), ("edge_out", 0), ("edge_out", 1), ("take", 1, 0, 2),
    ("take", 0, 1, 1), ("relay", 0, 2, True), ("relay", 2, 1, False), ("own", 1), ("take", 0, 1, 0),
    ("relay", 1, 1, True), ("relay", 1, 1, False), ("edge_share", 0), ("edge_share", 1), ("tokens_y", 2), ("near", 2),
    ("take", 1, 1, 1), ("last", 0), ("take", 1, 0, 0), ("relay", 1, 2, False), ("cots", 0), ("take", 1, 0, 1),
    ("tokens_core",), ("edge_pass", 0), ("edge_pass", 1), ("take", 1, 1, 2), ("take", 1, 1, 0), ("take", 0, 1, 2),
    ("take_rest",), ("project", 0), ("mix", 0), ("relay", 1, 2, True), ("relay", 2, 1, True), ("cots", 1),
    ("weight", 0), ("last", 1), ("relay", 2, 2, False), ("project", 1), ("relay", 2, 2, True), ("pass_on", 0, 2),
    ("cots", 2), ("mix", 1), ("weight", 1), ("pass_on", 0, 1), ("last", 2), ("project", 2), ("mix", 2), ("input", 0),
    ("finish", 0), ("first", 0), ("input", 2), ("pass_on", 1, 2), ("weight", 2), ("owners", 0), ("first", 2),
    ("input", 1), ("taps",), ("pass_on", 1, 1), ("first", 1), ("second", 1), ("pass_on", 2, 2), ("finish", 1),
    ("second", 0), ("pass_on", 2, 1), ("owners", 1), ("input", 3), ("finish", 2), ("taps_sum",), ("owners", 2),
)


def plan(chunks, deep):
    return TUNED if (chunks, deep) == (3, 4) else general_plan(chunks, deep)


def general_plan(chunks, deep):
    yield "weights_y", 0
    yield "tokens_y", 0
    for c in range(1, chunks):
        yield "weights_y", c
        if c < 3:
            yield "tokens_y", c
    for k in range(min(chunks, 3), 3):
        yield "tokens_y", k
    for k in (2, 0, 1):
        yield "tokens_x", k
    for side in range(2):
        yield "edge_out", side
    yield ("tokens_core",)
    for c in range(chunks):
        yield "own", c
    yield "near", 0
    yield "relay", 0, 1, False
    for side in range(2):
        yield "edge_share", side
    yield "take", 1, 0, 2
    for c in range(1, chunks):
        yield "relay", c, 1, False
    yield "take", 0, 1, 0
    yield "relay", 0, 1, True
    for c in range(1, min(chunks, 2)):
        yield "near", c
    for dist in range(2, deep):
        yield "relay", 0, dist, False
        yield "relay", 0, dist, True
    for side in range(2):
        yield "edge_pass", side
    yield "take", 0, 1, 1
    for c in range(chunks):
        yield "cots", c
    for k in (0, 1):
        yield "take", 1, 0, k
    for c in range(2, chunks):
        yield "near", c
    for c in range(1, min(chunks, 2)):
        yield "relay", c, 1, True
        for dist in range(2, deep):
            yield "relay", c, dist, False
    yield "take", 1, 1, 0
    yield "take", 0, 1, 2
    for k in (1, 2):
        yield "take", 1, 1, k
    yield ("take_rest",)
    yield "last", 0
    yield "project", 0
    for c in range(1, chunks):
        for dist in range(1, deep):
            if c > 1 and dist > 1:
                yield "relay", c, dist, False
            if c > 1 or dist > 1:
                yield "relay", c, dist, True
    for c in range(chunks):
        if c:
            yield "last", c
            yield "project", c
        yield "mix", c
        if c < max(chunks - 1, 1):
            yield "weight", c
        if c == chunks - 2:
            for early in range(chunks - 2):
                for dist in range(deep - 1, 0, -1):
                    yield "pass_on", early, dist
    yield ("taps",)
    yield "input", 0
    yield "input", 1
    yield "first", 0
    yield "input", 2
    yield "first", 1
    yield "input", 3
    yield "first", 2
    if chunks > 1:
        yield "weight", chunks - 1
    for c in range(chunks):
        if c >= chunks - 2:
            for dist in range(deep - 1, 0, -1):
                yield "pass_on", c, dist
        if c == max(chunks - 2, 0):
            for f in range(2):
                yield "second", f
            yield ("taps_sum",)
        yield "finish", c
        yield "owners", c


def fused_kernel(
    sizes, factor, x_own, gate_w, value_w, gate_taps, value_taps, g_own,
    in_grad, gate_out, value_out, gate_taps_out, value_taps_out,
    taps_mine, x_all, w_all, g_all, pre, cot, grads, from_z, fin, pv, from_tp, first_got, second_got, terms, terms_z, terms_all,
    own_sem, wy_send, wy_recv, wz_send, wz_recv, x_send, xf_send, xs_send, x_recv, hz_send, hb_send, hs_send, hx_recv,
    g_send, g_recv, hg_send, hg_recv, sz_send, sz_recv, out_send, out_recv, tp_send, tp_recv,
    s1_send, s1_recv, s2_send, s2_recv, tz_send, tz_recv, ta_send, ta_recv,
):
    deep, across, width = sizes
    rep, fs, tp = (lax.axis_index(a) for a in ("rep", "fs", "tp"))
    z, y = fs // across, fs % across
    nrep, ny, ntp = 1 - rep, 1 - y, 1 - tp
    tokens, feats = x_own.shape
    rows, hid = gate_w.shape
    main = across * tokens
    ext = main + 2 * EDGE
    chunks = width // LANES
    both = 2 * LANES
    blocks = feats // rows
    first_feats = feats * 3 // 8 // LANES * LANES
    spans = ((0, first_feats), (first_feats, feats - first_feats))
    step = tokens * 3 // 8 // 16 * 16
    pieces = ((0, step), (step, step), (2 * step, tokens - 2 * step))
    last = len(pieces) - 1
    weights = (gate_w, value_w)
    outs = (gate_out, value_out)
    others = [(dr, dy) for dr in range(2) for dy in range(2) if dr or dy]

    start = lambda c: c.start()
    sent = lambda c: c.wait_send()

    def landed(ref, sem):
        pltpu.make_async_copy(ref, ref, sem).wait()

    def moved(index, step):
        return (index + step) % 2

    def part_of(r, yy):
        return r * across + yy

    part = part_of(rep, y)

    def first_col(which):
        return jnp.minimum(which * width, hid - width)

    def live(which, c):
        return c * LANES >= which * width - first_col(which)

    def chunk_cols(which, c):
        return pl.ds(pl.multiple_of(first_col(which) + c * LANES, LANES), LANES)

    def all_cols(which):
        return pl.ds(pl.multiple_of(first_col(which), LANES), width)

    def cols(half):
        return pl.ds(pl.multiple_of(half * feats, feats), feats)

    def token_rows(yy):
        return pl.ds(pl.multiple_of(yy * tokens, 16), tokens)

    def lanes(branch):
        return pl.ds(branch * LANES, LANES)

    def near(side):
        return pl.ds(0, EDGE) if side == 0 else pl.ds(tokens - EDGE, EDGE)

    def far(side):
        return pl.ds(main + side * EDGE, EDGE)

    def gives_edge(side):
        return (y == 0) & (z > 0) if side == 0 else (y == across - 1) & (z < deep - 1)

    def has_edge(side):
        return z < deep - 1 if side == 0 else z > 0

    def takes_edge(side):
        return (y == 0) & (z < deep - 1) if side == 0 else (y == across - 1) & (z > 0)

    def greet():
        barrier = pltpu.get_barrier_semaphore()

        def hello(**device):
            pl.semaphore_signal(barrier, 1, device_id=device, device_id_type=pl.DeviceIdType.MESH)

        for dr in range(2):
            for dy in range(2):
                for dt in range(2):
                    if dr or dy or dt:
                        hello(rep=moved(rep, dr), fs=z * across + moved(y, dy), tp=moved(tp, dt))
        for step_z in range(1, deep):
            hello(fs=(z + step_z) % deep * across + y)
        for up in (True, False):
            @pl.when(z < deep - 1 if up else z > 0)
            def _():
                for dr, dy in others:
                    hello(rep=moved(rep, dr), fs=(z + 1 if up else z - 1) * across + moved(y, dy))
        next_levels = (z > 0).astype(jnp.int32) + (z < deep - 1).astype(jnp.int32)
        pl.semaphore_wait(barrier, 6 + deep + len(others) * next_levels)

    def w_across(c, sink):
        for branch, w in enumerate(weights):
            sink(remote(
                w.at[:, chunk_cols(part_of(rep, ny), c)], w_all.at[c, fs, :, lanes(branch)],
                wy_send.at[c, branch], wy_recv.at[c, branch], fs=z * across + ny,
            ))

    def w_along(c, block, up, down, sink):
        ref = w_all.at[c, block]
        if up:
            @pl.when(z < deep - 1)
            def _():
                sink(remote(ref, ref, wz_send.at[c, block, 0], wz_recv.at[c, block], fs=fs + across))
        if down:
            @pl.when(z > 0)
            def _():
                sink(remote(ref, ref, wz_send.at[c, block, 1], wz_recv.at[c, block], fs=fs - across))

    def w_local(c):
        return [
            pltpu.make_async_copy(
                w.at[:, chunk_cols(part, c)], w_all.at[c, fs, :, lanes(branch)], own_sem.at[2 * c + branch]
            ) for branch, w in enumerate(weights)
        ]

    def w_own_along(c, sink):
        w_along(c, fs, True, True, sink)

    def w_near_along(c, arrive, sink):
        block = z * across + ny
        if arrive:
            for branch in range(2):
                landed(w_all.at[c, block, :, lanes(branch)], wy_recv.at[c, branch])
        w_along(c, block, True, True, sink)

    def w_step(c, dist, near_block, forward, visit):
        for sign in (-1, 1):
            here = (z >= dist) if sign < 0 else (z + dist < deep)
            goes_on = (z < deep - 1) if sign < 0 else (z > 0)

            @pl.when(here & (goes_on if forward else jnp.logical_not(goes_on)))
            def _():
                visit((z + sign * dist) * across + (ny if near_block else y), sign)

    def w_relay(c, dist, near_block, sink=start):
        def visit(block, sign):
            if sink is start:
                landed(w_all.at[c, block], wz_recv.at[c, block])
            w_along(c, block, sign < 0, sign > 0, sink)

        w_step(c, dist, near_block, True, visit)

    def w_last(c):
        for dist in range(1, deep):
            for near_block in (False, True):
                w_step(
                    c, dist, near_block, False,
                    lambda block, sign: landed(w_all.at[c, block], wz_recv.at[c, block]),
                )

    def x_at(r, yy, k, half):
        offset, size = pieces[k]
        return x_all.at[r, pl.ds(pl.multiple_of(yy * tokens + offset, 16), size), cols(half)]

    def x_mine(k):
        return x_own.at[pl.ds(*pieces[k])]

    def x_across(k, sink):
        sink(remote(x_mine(k), x_at(rep, y, k, tp), x_send.at[1, k], x_recv.at[rep, y, k, tp], fs=z * across + ny))

    def x_over(k, sink):
        sink(remote(x_mine(k), x_at(rep, y, k, tp), x_send.at[0, k], x_recv.at[rep, y, k, tp], rep=nrep))

    def x_to_sibling(sink):
        for k in range(len(pieces)):
            sink(remote(x_mine(k), x_at(rep, y, k, tp), xs_send.at[rep, y, k], x_recv.at[rep, y, k, tp], tp=ntp))

    def x_forward(k, sink):
        if k < last:
            ref = x_at(rep, ny, k, tp)
            sink(remote(ref, ref, xf_send.at[k], x_recv.at[rep, ny, k, tp], rep=nrep))
        else:
            ref = x_at(nrep, y, k, tp)
            sink(remote(ref, ref, xf_send.at[k], x_recv.at[nrep, y, k, tp], fs=z * across + ny))

    def x_take(r, yy, k, forward):
        x_landed(r, yy, k, tp)
        if forward:
            x_forward(k, start)
        x_share(r, yy, k, start)

    def x_share(r, yy, k, sink):
        ref = x_at(r, yy, k, tp)
        sink(remote(ref, ref, xs_send.at[r, yy, k], x_recv.at[r, yy, k, tp], tp=ntp))

    def x_landed(r, yy, k, half):
        landed(x_at(r, yy, k, half), x_recv.at[r, yy, k, half])

    def edge_out(side, sink):
        target = fs - across if side == 0 else fs + across

        @pl.when(gives_edge(side))
        def _():
            sink(remote(
                x_own.at[near(side)], x_all.at[rep, far(side), cols(tp)], hz_send.at[side],
                hx_recv.at[side, rep, tp], fs=target,
            ))
            level = z - 1 if side == 0 else z + 1
            for dr in range(2):
                for dy in range(2):
                    r, yy = moved(rep, dr), moved(y, dy)
                    sink(remote(
                        g_own.at[near(side), all_cols(part_of(r, yy))], g_all.at[rep, far(side)],
                        hg_send.at[side, dr, dy], hg_recv.at[side, rep], rep=r, fs=level * across + yy,
                    ))

    def edge_at(side, r, half):
        return x_all.at[r, far(side), cols(half)]

    def edge_share(side, sink=start):
        @pl.when(takes_edge(side))
        def _():
            ref = edge_at(side, rep, tp)
            if sink is start:
                landed(ref, hx_recv.at[side, rep, tp])
            for dr, dy in others:
                sink(remote(
                    ref, ref, hb_send.at[side, dr, dy], hx_recv.at[side, rep, tp],
                    rep=moved(rep, dr), fs=z * across + moved(y, dy),
                ))
            sink(remote(ref, ref, hs_send.at[side, rep], hx_recv.at[side, rep, tp], tp=ntp))

    def edge_pass(side, sink=start):
        for r in (rep, nrep):
            @pl.when(has_edge(side) & jnp.logical_not(takes_edge(side) & (r == rep)))
            def _():
                ref = edge_at(side, r, tp)
                if sink is start:
                    landed(ref, hx_recv.at[side, r, tp])
                sink(remote(ref, ref, hs_send.at[side, r], hx_recv.at[side, r, tp], tp=ntp))

    def edge_landed(side):
        @pl.when(has_edge(side))
        def _():
            for r in range(2):
                landed(edge_at(side, r, ntp), hx_recv.at[side, r, ntp])
                landed(g_all.at[r, far(side)], hg_recv.at[side, r])

    def g_direct(c, sink):
        for dr, dy in others:
            r, yy = moved(rep, dr), moved(y, dy)
            sink(remote(
                g_own.at[:, chunk_cols(part_of(r, yy), c)], g_all.at[rep, token_rows(y), pl.ds(c * LANES, LANES)],
                g_send.at[c, dr, dy], g_recv.at[c, rep, y], rep=r, fs=z * across + yy,
            ))

    def g_landed(c):
        for dr, dy in others:
            r, yy = moved(rep, dr), moved(y, dy)
            landed(g_all.at[r, token_rows(yy), pl.ds(c * LANES, LANES)], g_recv.at[c, r, yy])

    x_local = pltpu.make_async_copy(
        x_own, x_all.at[rep, token_rows(y), cols(tp)], own_sem.at[2 * chunks]
    )
    g_local = pltpu.make_async_copy(
        g_own.at[:, all_cols(part)], g_all.at[rep, token_rows(y)], own_sem.at[2 * chunks + 1]
    )

    tap_cols = pl.ds(pl.multiple_of(tp * hid + first_col(part), LANES), width)
    taps_local = [
        pltpu.make_async_copy(ref.at[:, tap_cols], taps_mine.at[b], own_sem.at[2 * chunks + 2 + b])
        for b, ref in enumerate((gate_taps, value_taps))
    ]

    def chunk_lanes(c):
        return pl.ds(c * both, both)

    def project(c):
        @pl.loop(0, 2)
        def _(slot):
            total = jnp.dot(
                x_all[slot], w_all[c].reshape(-1, both), preferred_element_type=jnp.float32
            )
            pre[slot] = total.astype(pre.dtype)

    def mix(c):
        row = lax.broadcasted_iota(jnp.int32, (ext, LANES), 0)
        has_next, has_prev = (z < deep - 1).astype(jnp.int32), (z > 0).astype(jnp.int32)
        inside = (row < main) | ((row < main + EDGE) & (has_next > 0)) | ((row >= main + EDGE) & (has_prev > 0))
        counted = inside & (live(part, c).astype(jnp.int32) > 0)
        taps = [[taps_mine[b, k : k + 1, pl.ds(c * LANES, LANES)] for k in range(3)] for b in range(2)]
        terms[:, pl.ds(c * LANES, LANES)] = jnp.zeros((8, LANES), jnp.float32)

        def before(v):
            return pltpu.roll(v, 1, 0)

        def after(v):
            return pltpu.roll(v, ext - 1, 0)

        @pl.loop(0, 2)
        def _(slot):
            pres = [jnp.where(inside, pre[slot, :, lanes(b)].astype(jnp.float32), 0.0) for b in range(2)]
            around = [(before(p), p, after(p)) for p in pres]
            gate_mix, value_mix = [sum(w * p for w, p in zip(ws, ps)) for ws, ps in zip(taps, around)]
            cot_in = jnp.where(counted, g_all[slot, :, pl.ds(c * LANES, LANES)].astype(jnp.float32), 0.0)
            sig = jax.nn.sigmoid(gate_mix)
            cots = (
                cot_in * value_mix * (sig * (1.0 + gate_mix * (1.0 - sig))),
                cot_in * (gate_mix * sig),
            )
            for b in range(2):
                ws, ps, one = taps[b], around[b], cots[b]
                back = ws[0] * after(one) + ws[1] * one + ws[2] * before(one)
                cot[slot, :, pl.ds(c * both + b * LANES, LANES)] = back[:main].astype(cot.dtype)
                for k in range(3):
                    total = jnp.sum(ps[k][:main] * one[:main], axis=0, keepdims=True)
                    terms[2 * k + b : 2 * k + b + 1, pl.ds(c * LANES, LANES)] += total * factor

    def far_first(visit):
        @pl.loop(0, 2 * deep - 1)
        def _(i):
            dist = deep - 1 - i // 2
            level = jnp.where(i % 2 == 0, z + dist, z - dist)

            @pl.when((level >= 0) & (level < deep))
            def _():
                visit(level)

    def sum_hop(c, block, up, sink):
        way = 0 if up else 1
        sink(remote(
            grads.at[c, block], from_z.at[way, c, block], sz_send.at[c, block], sz_recv.at[way, c, block],
            fs=fs + across if up else fs - across,
        ))

    def weight_terms(c):
        def visit(level):
            for yy in range(across):
                block = level * across + yy
                at = pl.ds(pl.multiple_of(block * rows, rows), rows)
                total = sum(
                    lax.dot_general(
                        x_all[slot, :main, at], cot[slot, :, chunk_lanes(c)], (((0,), (0,)), ((), ())),
                        preferred_element_type=jnp.float32,
                    ) for slot in range(2)
                )
                grads[c, block] = (total * factor).astype(grads.dtype)
            for up in (True, False):
                @pl.when((level > z) & (z == 0) if up else (level < z) & (z == deep - 1))
                def _():
                    for yy in range(across):
                        sum_hop(c, level * across + yy, up, start)

        far_first(visit)

    def pass_on(c, dist):
        for up in (True, False):
            level = z + dist if up else z - dist

            @pl.when((z > 0) & (z < deep - 1) & ((level < deep) if up else (level >= 0)))
            def _():
                way = 0 if up else 1
                for yy in range(across):
                    block = level * across + yy
                    landed(from_z.at[way, c, block], sz_recv.at[way, c, block])
                    total = grads[c, block].astype(jnp.float32) + from_z[way, c, block].astype(jnp.float32)
                    grads[c, block] = total.astype(grads.dtype)
                    sum_hop(c, block, up, start)

    def sums_sent(c):
        def visit(level):
            for up in (True, False):
                @pl.when((level > z) if up else (level < z))
                def _():
                    for yy in range(across):
                        sum_hop(c, level * across + yy, up, sent)

        far_first(visit)

    def to_owners(c, same, sink):
        here = chunk_cols(part, c)
        for branch, out in enumerate(outs):
            sems = out_send.at[c, branch, 0 if same else 1], out_recv.at[c, branch, rep, y]
            if same:
                sink(remote(out.at[:, here], out.at[:, here], *sems, rep=nrep))
            else:
                sink(remote(fin.at[c, :, lanes(branch)], out.at[:, here], *sems, fs=z * across + ny))

    def owners_pass(c, sink=start):
        source = part_of(rep, ny)

        @pl.when(live(source, c))
        def _():
            for branch, out in enumerate(outs):
                ref, sem = out.at[:, chunk_cols(source, c)], out_recv.at[c, branch, rep, ny]
                if sink is start:
                    landed(ref, sem)
                sink(remote(ref, ref, out_send.at[c, branch, 2], sem, rep=nrep))

    def owners_last(c):
        for yy in (y, ny):
            source = part_of(nrep, yy)

            @pl.when(live(source, c))
            def _():
                for branch, out in enumerate(outs):
                    landed(out.at[:, chunk_cols(source, c)], out_recv.at[c, branch, nrep, yy])

    def finish(c):
        for same in (False, True):
            block = z * across + (y if same else ny)
            for way in range(2):
                @pl.when(z > 0 if way == 0 else z < deep - 1)
                def _():
                    landed(from_z.at[way, c, block], sz_recv.at[way, c, block])
            total = grads[c, block].astype(jnp.float32)
            for way in range(2):
                total += from_z[way, c, block].astype(jnp.float32)
            total = total.astype(grads.dtype)

            @pl.when(live(part, c))
            def _():
                if same:
                    for branch, out in enumerate(outs):
                        out[:, chunk_cols(part, c)] = total[:, branch * LANES : (branch + 1) * LANES]
                else:
                    fin[c] = total
                to_owners(c, same, start)

    def input_terms(dr, dy):
        r, yy = moved(rep, dr), moved(y, dy)
        q = part_of(r, yy)

        @pl.loop(0, 2 * blocks)
        def _(i):
            half = jnp.where(i < blocks, ntp, tp)
            j = i % blocks
            total = sum(
                lax.dot_general(
                    cot[r, token_rows(yy), chunk_lanes(c)], w_all[c, half * blocks + j],
                    (((1,), (1,)), ((), ())), preferred_element_type=jnp.float32,
                ) for c in range(chunks)
            )
            pv[half, q, :, pl.ds(pl.multiple_of(j * rows, rows), rows)] = total.astype(pv.dtype)

        tp_hop(q, start)

    def tp_hop(q, sink):
        sink(remote(pv.at[ntp, q], from_tp.at[q], tp_send.at[q], tp_recv.at[q], tp=ntp))

    def f_cols(f):
        return pl.ds(*spans[f])

    def first_hop(f, k, sink):
        q = part_of(nrep, ny) if k else part_of(nrep, y) if f == 0 else part_of(rep, ny)
        target = dict(rep=nrep) if f == 0 else dict(fs=z * across + ny)
        sink(remote(pv.at[tp, q, :, f_cols(f)], first_got.at[f, k, :, pl.ds(0, spans[f][1])], s1_send.at[f, k], s1_recv.at[f, k], **target))

    def second_hop(f, sink):
        q = part_of(rep, ny) if f == 0 else part_of(nrep, y)
        target = dict(fs=z * across + ny) if f == 0 else dict(rep=nrep)
        sink(remote(pv.at[tp, q, :, f_cols(f)], second_got.at[f, :, pl.ds(0, spans[f][1])], s2_send.at[f], s2_recv.at[f], **target))

    def row_tiles(body):
        @pl.loop(0, tokens // 16)
        def _(i):
            body(pl.ds(pl.multiple_of(i * 16, 16), 16))

    def add_sibling(q):
        landed(from_tp.at[q], tp_recv.at[q])

        def body(at):
            total = pv[tp, q, at].astype(jnp.float32) + from_tp[q, at].astype(jnp.float32)
            pv[tp, q, at] = total.astype(pv.dtype)

        row_tiles(body)

    def input_first(dr, dy):
        add_sibling(part_of(moved(rep, dr), moved(y, dy)))
        if dr:
            first_hop(0, dy, start)
        if dy:
            first_hop(1, dr, start)

    def input_second(f):
        q = part_of(rep, ny) if f == 0 else part_of(nrep, y)
        landed(first_got.at[f, 1, :, pl.ds(0, spans[f][1])], s1_recv.at[f, 1])

        def body(at):
            total = pv[tp, q, at, f_cols(f)].astype(jnp.float32)
            total += first_got[f, 1, at, : spans[f][1]].astype(jnp.float32)
            pv[tp, q, at, f_cols(f)] = total.astype(pv.dtype)

        row_tiles(body)
        second_hop(f, start)

    def input_last():
        landed(from_tp.at[part], tp_recv.at[part])
        for f in range(2):
            landed(first_got.at[f, 0, :, pl.ds(0, spans[f][1])], s1_recv.at[f, 0])
            landed(second_got.at[f, :, pl.ds(0, spans[f][1])], s2_recv.at[f])

        def body(at):
            for f in range(2):
                total = pv[tp, part, at, f_cols(f)].astype(jnp.float32) + from_tp[part, at, f_cols(f)].astype(jnp.float32)
                total += first_got[f, 0, at, : spans[f][1]].astype(jnp.float32) + second_got[f, at, : spans[f][1]].astype(jnp.float32)
                in_grad[at, f_cols(f)] = total.astype(in_grad.dtype)

        row_tiles(body)

    def taps_along(sink):
        for step in range(1, deep):
            to = (z + step) % deep
            sink(remote(
                terms_z.at[z], terms_z.at[z], tz_send.at[step], tz_recv.at[z], fs=to * across + y
            ))

    def taps_start():
        terms_z[z] = terms[...]
        taps_along(start)

    def taps_out(sink):
        ref = terms_all.at[rep, y, tp]
        for dr in range(2):
            for dy in range(2):
                for dt in range(2):
                    if dr or dy or dt:
                        sink(remote(
                            ref, ref, ta_send.at[dr, dy, dt], ta_recv.at[rep, y, tp],
                            rep=moved(rep, dr), fs=z * across + moved(y, dy), tp=moved(tp, dt),
                        ))

    def taps_sum():
        for step in range(1, deep):
            source = (z + step) % deep
            landed(terms_z.at[source], tz_recv.at[source])
        terms_all[rep, y, tp] = sum(terms_z[level] for level in range(deep))
        taps_out(start)

    def taps_last():
        for dr in range(2):
            for dy in range(2):
                for dt in range(2):
                    if dr or dy or dt:
                        at = (moved(rep, dr), moved(y, dy), moved(tp, dt))
                        landed(terms_all.at[at], ta_recv.at[at])
        for r in range(2):
            for yy in range(across):
                which = r * across + yy
                first = min(which * width, hid - width)
                skip = which * width - first
                for half in range(2):
                    for branch, out in enumerate((gate_taps_out, value_taps_out)):
                        for k in range(3):
                            if skip < width:
                                begin = half * hid + first + skip
                                out[k : k + 1, begin : begin + width - skip] = terms_all[
                                    r, yy, half, 2 * k + branch : 2 * k + branch + 1, skip:
                                ]

    for c in range(chunks):
        for copy in w_local(c):
            copy.start()
    x_local.start()
    g_local.start()
    for copy in taps_local:
        copy.start()
    for way in range(2):
        @pl.when((z == 0) if way == 0 else (z == deep - 1))
        def _():
            for c in range(chunks):
                for yy in range(across):
                    from_z[way, c, z * across + yy] = jnp.zeros((rows, both), from_z.dtype)
    greet()

    def w_own(c):
        for copy in w_local(c):
            copy.wait()
        w_own_along(c, start)

    def take(dr, dy, k):
        x_take(moved(rep, dr), moved(y, dy), k, (not dr) if k < last else (not dy))

    def take_rest():
        x_local.wait()
        g_local.wait()
        for copy in taps_local:
            copy.wait()
        for r in range(2):
            for yy in range(across):
                for k in range(len(pieces)):
                    x_landed(r, yy, k, ntp)
        for side in range(2):
            edge_landed(side)

    def mix_chunk(c):
        g_landed(c)
        mix(c)

    offsets = ((1, 1), (0, 1), (1, 0), (0, 0))
    actions = dict(
        weights_y=lambda c: w_across(c, start),
        tokens_y=lambda k: x_across(k, start),
        tokens_x=lambda k: x_over(k, start),
        tokens_core=lambda: x_to_sibling(start),
        edge_out=lambda side: edge_out(side, start),
        own=w_own,
        near=lambda c: w_near_along(c, True, start),
        relay=w_relay,
        edge_share=edge_share,
        edge_pass=edge_pass,
        take=take,
        cots=lambda c: g_direct(c, start),
        take_rest=take_rest,
        last=w_last,
        project=project,
        mix=mix_chunk,
        weight=weight_terms,
        pass_on=pass_on,
        finish=finish,
        owners=owners_pass,
        taps=taps_start,
        taps_sum=taps_sum,
        input=lambda i: input_terms(*offsets[i]),
        first=lambda i: input_first(*offsets[i]),
        second=input_second,
    )
    for name, *args in plan(chunks, deep):
        actions[name](*args)
    input_last()
    taps_last()
    for c in range(chunks):
        owners_last(c)
    for side in range(2):
        edge_out(side, sent)
        edge_share(side, sent)
        edge_pass(side, sent)
    x_to_sibling(sent)
    for k in range(len(pieces)):
        x_across(k, sent)
        x_over(k, sent)
        x_forward(k, sent)
        for dr, dy in others:
            x_share(moved(rep, dr), moved(y, dy), k, sent)
    for c in range(chunks):
        w_across(c, sent)
        w_own_along(c, sent)
        w_near_along(c, False, sent)
        for dist in range(1, deep):
            for near_block in (False, True):
                w_relay(c, dist, near_block, sent)
        g_direct(c, sent)
        sums_sent(c)

        @pl.when(live(part, c))
        def _():
            for same in (False, True):
                to_owners(c, same, sent)

        owners_pass(c, sent)
    for dr in range(2):
        for dy in range(2):
            tp_hop(part_of(moved(rep, dr), moved(y, dy)), sent)
    for f in range(2):
        for k in range(2):
            first_hop(f, k, sent)
        second_hop(f, sent)
    taps_along(sent)
    taps_out(sent)


def fused_all(across, x_own, gate_w, value_w, gate_taps, value_taps, g_own):
    reps, fs_count, tps = (lax.axis_size(a) for a in ("rep", "fs", "tp"))
    deep = fs_count // across
    tokens, feats = x_own.shape
    rows, hid = gate_w.shape
    width = part_width(hid, reps * across)
    chunks = width // LANES
    both = 2 * LANES
    main = across * tokens
    ext = main + 2 * EDGE
    parts = reps * across
    factor = float(tokens * fs_count * reps) ** (-0.5)
    dtype = x_own.dtype
    f32 = jnp.float32
    sem = pltpu.SemaphoreType.DMA
    sems = [
        (2 * chunks + 4,), (chunks, 2), (chunks, 2), (chunks, fs_count, 2), (chunks, fs_count), (2, 3), (3,),
        (reps, across, 3), (reps, across, 3, tps), (2,), (2, 2, 2), (2, reps), (2, reps, tps),
        (chunks, 2, 2), (chunks, reps, across), (2, 2, 2), (2, reps), (chunks, fs_count), (2, chunks, fs_count),
        (chunks, 2, 3), (chunks, 2, reps, across), (parts,), (parts,),
        (2, 2), (2, 2), (2,), (2,), (deep,), (deep,), (2, 2, 2), (reps, across, tps),
    ]
    buffers = [
        ((2, 3, width), f32), ((reps, ext, tps * feats), dtype), ((chunks, fs_count, rows, both), dtype), ((reps, ext, width), dtype),
        ((reps, ext, both), dtype), ((reps, main, 2 * width), dtype), ((chunks, fs_count, rows, both), dtype),
        ((2, chunks, fs_count, rows, both), dtype), ((chunks, rows, both), dtype),
        ((tps, parts, tokens, feats), dtype), ((parts, tokens, feats), dtype),
        ((2, 2, tokens, feats), dtype), ((2, tokens, feats), dtype),
        ((8, width), f32), ((deep, 8, width), f32), ((reps, across, tps, 8, width), f32),
    ]
    vmem, hbm = pl.BlockSpec(memory_space=pltpu.VMEM), pl.BlockSpec(memory_space=pl.ANY)
    return pl.pallas_call(
        functools.partial(fused_kernel, (deep, across, width), factor),
        out_shape=(
            jax.ShapeDtypeStruct((tokens, feats), dtype),
            jax.ShapeDtypeStruct((rows, hid), dtype),
            jax.ShapeDtypeStruct((rows, hid), dtype),
            jax.ShapeDtypeStruct(gate_taps.shape, f32),
            jax.ShapeDtypeStruct(value_taps.shape, f32),
        ),
        in_specs=[hbm] * 6,
        out_specs=(vmem,) * 5,
        scratch_shapes=[pltpu.VMEM(*b) for b in buffers] + [sem(s) for s in sems],
        compiler_params=pltpu.CompilerParams(has_side_effects=True, collective_id=0, vmem_limit_bytes=60 * 1024 * 1024),
        name="fused_all",
    )(x_own, gate_w, value_w, gate_taps, value_taps, g_own)


def store_kernel(in_grad, gate, value, gate_taps, value_taps, *refs):
    outs, held, (gate_wide, value_wide, load_sem, sem) = refs[:5], refs[5:10], refs[10:]
    loads = [
        pltpu.make_async_copy(src, dst, load_sem.at[k])
        for k, (src, dst) in enumerate(zip((in_grad, gate, value, gate_taps, value_taps), held))
    ]
    order = (1, 2, 0, 3, 4)
    for k in order:
        loads[k].start()
    copies = []
    for k in order:
        loads[k].wait()
        src = held[k]
        if k in (1, 2):
            src = gate_wide if k == 1 else value_wide
            src[...] = held[k][...].astype(src.dtype)
        copies.append(pltpu.make_async_copy(src, outs[k], sem.at[k]))
        copies[-1].start()
    for copy in copies:
        copy.wait()


def store_all(*arrays):
    hbm = pl.BlockSpec(memory_space=pl.ANY)
    wide = jax.ShapeDtypeStruct(arrays[1].shape, jnp.float32)
    outs = [jax.ShapeDtypeStruct(a.shape, a.dtype) for a in arrays]
    outs[1:3] = wide, wide
    sem = pltpu.SemaphoreType.DMA((5,))
    return pl.pallas_call(
        store_kernel,
        out_shape=tuple(outs),
        in_specs=[hbm] * 5,
        out_specs=(hbm,) * 5,
        scratch_shapes=[pltpu.VMEM(a.shape, a.dtype) for a in arrays] + [pltpu.VMEM(wide.shape, wide.dtype)] * 2 + [sem] * 2,
        compiler_params=pltpu.CompilerParams(vmem_limit_bytes=60 * 1024 * 1024),
        name="store_all",
    )(*arrays)


def fits_plane(across, inputs, gate_proj):
    reps, fs_count, tps = (lax.axis_size(a) for a in ("rep", "fs", "tp"))
    tokens, feats = inputs.shape[1:]
    rows, hid = gate_proj.shape
    parts = reps * across
    width = part_width(hid, parts)
    return (
        reps == across == tps == 2 and fs_count > across and tokens % 16 == 0 and tokens >= 48
        and hid % LANES == 0 and rows % LANES == 0 and feats % rows == 0 and feats % (2 * LANES) == 0
        and 4 * parts * width <= 5 * hid
    )


def shards(across, inputs, gate_proj, value_proj, gate_taps, value_taps, out_grad):
    if fits_plane(across, inputs, gate_proj):
        in_grad, gate_grad, value_grad, gate_terms, value_terms = store_all(
            *fused_all(across, inputs[0], gate_proj, value_proj, gate_taps, value_taps, out_grad[0])
        )
        return in_grad[None], gate_grad, value_grad, gate_terms, value_terms

    contract_cols = (((1,), (1,)), ((), ()))
    contract_rows = (((0,), (0,)), ((), ()))
    reps, fs_count = lax.axis_size("rep"), lax.axis_size("fs")
    rep = lax.axis_index("rep")
    tokens, feats = inputs.shape[1:]
    hid = gate_proj.shape[1]
    width = min(hid, -(-hid // reps // 128) * 128)
    last = hid - width

    def start_of(part):
        return jnp.minimum(part * width, last)

    first = start_of(rep)
    dead = rep * width - first
    live = jnp.arange(width) >= dead

    def part_cols(x, part):
        return lax.dynamic_slice_in_dim(x, start_of(part), width, x.ndim - 1)

    w_own = jnp.concatenate(
        [jnp.where(live, part_cols(w, rep), jnp.zeros((), w.dtype)) for w in (gate_proj, value_proj)], axis=1
    )
    g_parts = jnp.stack([part_cols(out_grad[0], (rep + step) % reps) for step in range(reps)])
    x_all, g_all, w_all = gather_all(inputs[0], g_parts, w_own, across)
    w_all = w_all.reshape(-1, 2 * width)

    ext = tokens + 2 * HALO
    pre = jnp.dot(x_all.reshape(reps * ext, -1), w_all, preferred_element_type=jnp.float32)
    pre = pre.astype(jnp.bfloat16).reshape(reps, ext, 2 * width)
    tap_start = lax.axis_index("tp") * hid + first
    taps = jnp.concatenate(
        [lax.dynamic_slice_in_dim(t, tap_start, width, 1) for t in (gate_taps, value_taps)], axis=1
    )
    factor = float(tokens * fs_count * reps) ** (-0.5)
    pre_cot, tap_terms = mix_all(pre, g_all, taps, tokens, fs_count, factor)
    pre_cot = pre_cot.reshape(reps * tokens, 2 * width)
    tap_terms = tap_terms[:3]

    grads = lax.dot_general(
        x_all[:, :tokens].reshape(reps * tokens, -1), pre_cot, contract_rows, preferred_element_type=jnp.float32
    )
    grads = (grads * factor).astype(jnp.bfloat16).reshape(fs_count, -1, 2 * width)
    partial_value = lax.dot_general(pre_cot, w_all, contract_cols, preferred_element_type=jnp.float32)
    partial_value = partial_value.astype(jnp.bfloat16).reshape(reps, tokens, -1)
    lanes = -(-tap_terms.size // 1024) * 128
    tap_terms = jnp.pad(tap_terms.reshape(-1), (0, 8 * lanes - tap_terms.size)).reshape(8, lanes)
    own, in_grad, tap_all = scatter_all(grads, partial_value, tap_terms, across)

    skips = [max(0, p * width - last) for p in range(reps)]
    proj_grads = [
        jnp.concatenate(
            [own[p, :, branch * width + skips[p] : (branch + 1) * width] for p in range(reps)], axis=1
        ).astype(jnp.float32)
        for branch in range(2)
    ]
    tap_all = tap_all.reshape(reps, -1, 8 * lanes)[:, :, : 6 * width].reshape(reps, -1, 3, 2, width)
    taps_out = jnp.concatenate(
        [tap_all[p, half, :, :, skips[p] :] for half in range(tap_all.shape[1]) for p in range(reps)], axis=2
    )
    return in_grad[None], proj_grads[0], proj_grads[1], taps_out[:, 0], taps_out[:, 1]


def solution(mesh):
    placed = (P("rep", "fs", "tp"), P("fs", "tp"), P("fs", "tp"), P(), P(), P("rep", "fs", "tp"))
    return jax.shard_map(
        functools.partial(shards, row_length(mesh)),
        mesh=mesh,
        in_specs=placed,
        out_specs=(P("rep", "fs", "tp"), P("fs", "tp"), P("fs", "tp"), P(), P()),
        check_vma=False,
    )
```

```python
import functools

import jax
import jax.numpy as jnp
from jax import lax
from jax.experimental import pallas as pl
from jax.experimental.pallas import tpu as pltpu
from jax.sharding import PartitionSpec as P

HALO = 8


def row_length(mesh):
    axis = mesh.axis_names.index("fs")
    devices = mesh.devices.swapaxes(0, axis)
    line = devices.reshape(devices.shape[0], -1)[:, 0]
    places = [tuple(getattr(d, "coords", (i,))) for i, d in enumerate(line)]
    moved = lambda a, b: [i for i in range(len(a)) if a[i] != b[i]]
    length = 1
    while length < len(places) and moved(places[0], places[length]) == moved(places[0], places[1]):
        length += 1
    return length if len(places) % length == 0 else 1


def remote(src, dst, send, recv, **device):
    return pltpu.make_async_remote_copy(
        src_ref=src, dst_ref=dst, send_sem=send, recv_sem=recv, device_id=device, device_id_type=pl.DeviceIdType.MESH
    )


def gather_kernel(
    sizes, x_ref, g_ref, w_ref, x_all, g_all, w_all,
    w_send, w_recv, xr_send, xt_send, x_recv, xh_send, xh_recv, g_send, g_recv, gh_send, gh_recv, own_sem,
):
    reps, fs_count, tps, across = sizes
    deep = fs_count // across
    rep, fs, tp = (lax.axis_index(a) for a in ("rep", "fs", "tp"))
    z, y = fs // across, fs % across
    tokens, feats = x_ref.shape

    def other(axis_index, step, count):
        return (axis_index + step) % count

    def cols(index):
        return pl.ds(pl.multiple_of(index * feats, feats), feats)

    half_width = w_ref.shape[1] // 2

    def half(c):
        return pl.ds(c * half_width, half_width)

    def send_w(block, c, src, way, target):
        return remote(
            src.at[:, half(c)], w_all.at[block, :, half(c)], w_send.at[block, c, way], w_recv.at[block, c], fs=target
        )

    def along(block, c, src, down, up, sink):
        if down:
            @pl.when(z > 0)
            def _():
                sink(send_w(block, c, src, 0, fs - across))
        if up:
            @pl.when(z < deep - 1)
            def _():
                sink(send_w(block, c, src, 1, fs + across))

    def to_row(block, c, src, sink):
        for step in range(1, across):
            sink(send_w(block, c, src, 1 + step, z * across + other(y, step, across)))

    start = lambda c: c.start()
    sent = lambda c: c.wait_send()

    def x_main(slot, src, sem, **device):
        return remote(src, x_all.at[slot, pl.ds(0, tokens), cols(tp)], sem, x_recv.at[slot, tp], **device)

    def halos(sink):
        for side in range(2):
            near = pl.ds(0, HALO) if side == 0 else pl.ds(tokens - HALO, HALO)
            far = pl.ds(tokens + side * HALO, HALO)
            target = fs - 1 if side == 0 else fs + 1

            @pl.when((fs > 0) if side == 0 else (fs < fs_count - 1))
            def _():
                for slot in range(reps):
                    to_rep = other(rep, slot, reps)
                    for step in range(tps):
                        sink(remote(
                            x_ref.at[near], x_all.at[slot, far, cols(tp)], xh_send.at[side, slot, step],
                            xh_recv.at[side, slot, tp], rep=to_rep, fs=target, tp=other(tp, step, tps),
                        ))
                    sink(remote(
                        g_ref.at[slot, near], g_all.at[slot, far], gh_send.at[side, slot],
                        gh_recv.at[side, slot], rep=to_rep, fs=target,
                    ))

    def to_reps(sink):
        for slot in range(1, reps):
            sink(x_main(slot, x_ref, xr_send.at[slot], rep=other(rep, slot, reps)))
        for slot in range(1, reps):
            sink(remote(
                g_ref.at[slot], g_all.at[slot, pl.ds(0, tokens)], g_send.at[slot], g_recv.at[slot],
                rep=other(rep, slot, reps),
            ))

    def to_tps(slot, src, sink):
        for step in range(1, tps):
            sink(x_main(slot, src, xt_send.at[slot, step], tp=other(tp, step, tps)))

    halos(start)
    for c in range(2):
        along(fs, c, w_ref, True, True, start)
        to_row(fs, c, w_ref, start)
    to_reps(start)
    to_tps(0, x_ref, start)
    own = [
        pltpu.make_async_copy(w_ref, w_all.at[fs], own_sem.at[0]),
        pltpu.make_async_copy(x_ref, x_all.at[0, pl.ds(0, tokens), cols(tp)], own_sem.at[1]),
        pltpu.make_async_copy(g_ref.at[0], g_all.at[0, pl.ds(0, tokens)], own_sem.at[2]),
    ]
    for copy in own:
        copy.start()

    def landed(ref, sem):
        pltpu.make_async_copy(ref, ref, sem).wait()

    def hops(dist, arrive, sink):
        for sign in (-1, 1):
            block = fs + sign * dist * across

            @pl.when((z >= dist) if sign < 0 else (z + dist < deep))
            def _():
                for c in range(2):
                    if arrive:
                        landed(w_all.at[block, :, half(c)], w_recv.at[block, c])
                    along(block, c, w_all.at[block], sign > 0, sign < 0, sink)
                    if c == 0:
                        to_row(block, c, w_all.at[block], sink)
                    else:
                        level = z + sign * dist

                        @pl.when((level > 0) & (level < deep - 1))
                        def _():
                            to_row(block, c, w_all.at[block], sink)

    def across_first(dist, arrive, sink):
        for end in ((0, deep - 1) if deep > 1 else (0,)):
            @pl.when(z == end + dist if end == 0 else z == end - dist)
            def _():
                for step in range(1, across):
                    block = end * across + other(y, step, across)
                    if arrive:
                        landed(w_all.at[block, :, half(1)], w_recv.at[block, 1])
                    along(block, 1, w_all.at[block], end > 0, end == 0 and deep > 1, sink)

    def forward_x(arrive, sink):
        for slot in range(1, reps):
            mine = x_all.at[slot, pl.ds(0, tokens), cols(tp)]
            if arrive:
                landed(mine, x_recv.at[slot, tp])
            to_tps(slot, mine, sink)

    for dist in range(1, deep):
        hops(dist, True, start)
        across_first(dist - 1, True, start)
        if dist == 1:
            forward_x(True, start)
    if deep == 1:
        forward_x(True, start)
    across_first(deep - 1, True, start)

    for slot in range(reps):
        for step in range(1, tps):
            source = other(tp, step, tps)
            landed(x_all.at[slot, pl.ds(0, tokens), cols(source)], x_recv.at[slot, source])
        if slot:
            landed(g_all.at[slot, pl.ds(0, tokens)], g_recv.at[slot])
    for side in range(2):
        far = pl.ds(tokens + side * HALO, HALO)

        @pl.when((fs < fs_count - 1) if side == 0 else (fs > 0))
        def _():
            for slot in range(reps):
                for source in range(tps):
                    landed(x_all.at[slot, far, cols(source)], xh_recv.at[side, slot, source])
                landed(g_all.at[slot, far], gh_recv.at[side, slot])
    for level in range(deep):
        for step in range(1, across):
            block = level * across + other(y, step, across)
            landed(w_all.at[block, :, half(0)], w_recv.at[block, 0])
            if 0 < level < deep - 1:
                landed(w_all.at[block, :, half(1)], w_recv.at[block, 1])
    for copy in own:
        copy.wait()
    halos(sent)
    for c in range(2):
        along(fs, c, w_ref, True, True, sent)
        to_row(fs, c, w_ref, sent)
    to_reps(sent)
    to_tps(0, x_ref, sent)
    for dist in range(1, deep):
        hops(dist, False, sent)
    for dist in range(deep):
        across_first(dist, False, sent)
    forward_x(False, sent)


def gather_all(x_own, g_parts, w_own, across):
    reps, fs_count, tps = (lax.axis_size(a) for a in ("rep", "fs", "tp"))
    tokens, feats = x_own.shape
    width = g_parts.shape[2]
    ext = tokens + 2 * HALO
    sems = [
        (fs_count, 2, 1 + across), (fs_count, 2), (reps,), (reps, tps), (reps, tps), (2, reps, tps), (2, reps, tps),
        (reps,), (reps,), (2, reps), (2, reps), (3,),
    ]
    vmem, hbm = pl.BlockSpec(memory_space=pltpu.VMEM), pl.BlockSpec(memory_space=pl.ANY)
    return pl.pallas_call(
        functools.partial(gather_kernel, (reps, fs_count, tps, across)),
        out_shape=(
            jax.ShapeDtypeStruct((reps, ext, feats * tps), x_own.dtype),
            jax.ShapeDtypeStruct((reps, ext, width), g_parts.dtype),
            jax.ShapeDtypeStruct((fs_count,) + w_own.shape, w_own.dtype),
        ),
        in_specs=[vmem] * 3,
        out_specs=(hbm,) * 3,
        scratch_shapes=[pltpu.SemaphoreType.DMA(s) for s in sems],
        compiler_params=pltpu.CompilerParams(has_side_effects=True),
        name="gather_all",
    )(x_own, g_parts, w_own)


def scatter_kernel(
    sizes, grads, pv, taps, own_all, in_grad, taps_all, y_got, z_got, tp_got, rep_got, taps_got,
    y_send, y_recv, z_send, z_recv, tp_send, tp_recv, rep_send, rep_recv, own_send, own_recv,
    taps_send, taps_recv, all_send, all_recv,
):
    reps, fs_count, tps, across = sizes
    deep = fs_count // across
    rep, fs, tp = (lax.axis_index(a) for a in ("rep", "fs", "tp"))
    z, y = fs // across, fs % across
    rows, width = grads.shape[1], grads.shape[2] // 2
    tokens, feats = in_grad.shape

    def other(axis_index, step, count):
        return (axis_index + step) % count

    def part(c):
        return pl.ds(c * width, width)

    def cols(index):
        return pl.ds(pl.multiple_of(index * feats, feats), feats)

    start = lambda c: c.start()
    sent = lambda c: c.wait_send()

    def landed(ref, sem):
        pltpu.make_async_copy(ref, ref, sem).wait()

    def tap_terms(sink):
        for step in range(1, fs_count):
            sink(remote(taps, taps_got.at[step], taps_send.at[step], taps_recv.at[step], fs=other(fs, step, fs_count)))

    def y_block(c, level, sink):
        for step in range(1, across):
            to = other(y, step, across)
            sink(remote(
                grads.at[level * across + to, :, part(c)], y_got.at[step, level, c],
                y_send.at[step, level, c], y_recv.at[step, level, c], fs=z * across + to,
            ))

    def far_first(visit):
        for dist in range(deep - 1, 0, -1):
            for way in range(2):
                @pl.when((z + dist < deep) if way == 0 else (z >= dist))
                def _():
                    visit(z + dist if way == 0 else z - dist, way)

    def y_sends(sink):
        for c in range(2):
            far_first(lambda level, way: y_block(c, level, sink))
            y_block(c, z, sink)

    def to_tps(sink):
        for slot in list(range(1, reps)) + [0]:
            for step in range(1, tps):
                to = other(tp, step, tps)
                sink(remote(
                    pv.at[slot, :, cols(to)], tp_got.at[slot, step], tp_send.at[slot, step], tp_recv.at[slot, step], tp=to
                ))

    def to_reps(sink):
        for slot in range(1, reps):
            sink(remote(
                rep_got.at[0, slot], rep_got.at[1, slot], rep_send.at[slot], rep_recv.at[slot],
                rep=other(rep, reps - slot, reps),
            ))

    def z_hop(c, level, way, sink):
        sink(remote(
            grads.at[level * across + y, :, part(c)], z_got.at[way, level, c],
            z_send.at[way, level, c], z_recv.at[way, level, c], fs=fs + across if way == 0 else fs - across,
        ))

    def own_rep(c, sink):
        mine = own_all.at[rep, :, part(c)]
        for step in range(1, reps):
            sink(remote(mine, mine, own_send.at[step, c], own_recv.at[step, c], rep=other(rep, step, reps)))

    def taps_out(sink):
        mine = taps_all.at[rep, tp]
        for slot in range(reps):
            for step in range(tps):
                if slot or step:
                    sink(remote(
                        mine, mine, all_send.at[slot, step], all_recv.at[slot, step],
                        rep=other(rep, slot, reps), tp=other(tp, step, tps),
                    ))

    tap_terms(start)
    to_tps(start)
    y_sends(start)

    for way in range(2):
        @pl.when((z == 0) if way == 0 else (z == deep - 1))
        def _():
            @pl.loop(0, deep)
            def _(level):
                for c in range(2):
                    @pl.loop(0, rows // 16)
                    def _(i):
                        z_got[way, level, c, pl.ds(pl.multiple_of(i * 16, 16), 16)] = jnp.zeros((16, width), z_got.dtype)

    def own_tps(slot, at):
        total = pv[slot, at, cols(tp)].astype(jnp.float32)
        for step in range(1, tps):
            total += tp_got[slot, step, at].astype(jnp.float32)
        return total

    for slot in range(1, reps):
        for step in range(1, tps):
            landed(tp_got.at[slot, step], tp_recv.at[slot, step])

        @pl.loop(0, tokens // 16)
        def _(i):
            at = pl.ds(pl.multiple_of(i * 16, 16), 16)
            rep_got[0, slot, at] = own_tps(slot, at).astype(rep_got.dtype)
    to_reps(start)

    def add_up(c, level, ways, store):
        for step in range(1, across):
            landed(y_got.at[step, level, c], y_recv.at[step, level, c])
        for way in ways:
            @pl.when((z > 0) if way == 0 else (z < deep - 1))
            def _():
                landed(z_got.at[way, level, c], z_recv.at[way, level, c])

        @pl.loop(0, rows // 16)
        def _(i):
            at = pl.ds(pl.multiple_of(i * 16, 16), 16)
            total = grads[level * across + y, at, part(c)].astype(jnp.float32)
            for step in range(1, across):
                total += y_got[step, level, c, at].astype(jnp.float32)
            for way in ways:
                total += z_got[way, level, c, at].astype(jnp.float32)
            store(at, total.astype(grads.dtype))

    def pass_on(c, level, way):
        def store(at, value):
            grads[level * across + y, at, part(c)] = value

        add_up(c, level, (way,), store)
        z_hop(c, level, way, start)

    for c in range(2):
        far_first(lambda level, way: pass_on(c, level, way))

        def store(at, value):
            own_all[rep, at, part(c)] = value

        add_up(c, z, (0, 1), store)
        own_rep(c, start)
        if c == 0:
            total = taps[...]
            for step in range(1, fs_count):
                landed(taps_got.at[step], taps_recv.at[step])
                total += taps_got[step]
            taps_all[rep, tp] = total
            taps_out(start)
            for step in range(1, tps):
                landed(tp_got.at[0, step], tp_recv.at[0, step])
            for slot in range(1, reps):
                landed(rep_got.at[1, slot], rep_recv.at[slot])

            @pl.loop(0, tokens // 16)
            def _(i):
                at = pl.ds(pl.multiple_of(i * 16, 16), 16)
                total = own_tps(0, at)
                for slot in range(1, reps):
                    total += rep_got[1, slot, at].astype(jnp.float32)
                in_grad[at] = total.astype(in_grad.dtype)

    for slot in range(reps):
        for step in range(tps):
            if slot or step:
                landed(taps_all.at[other(rep, reps - slot, reps), other(tp, tps - step, tps)], all_recv.at[slot, step])
    for step in range(1, reps):
        for c in range(2):
            landed(own_all.at[other(rep, reps - step, reps), :, part(c)], own_recv.at[step, c])
    tap_terms(sent)
    to_tps(sent)
    y_sends(sent)
    to_reps(sent)
    for c in range(2):
        far_first(lambda level, way: z_hop(c, level, way, sent))
        own_rep(c, sent)
    taps_out(sent)


def scatter_all(grads, pv, taps, across):
    reps, fs_count, tps = (lax.axis_size(a) for a in ("rep", "fs", "tp"))
    deep = fs_count // across
    rows, width = grads.shape[1], grads.shape[2] // 2
    tokens, feats = pv.shape[1], pv.shape[2] // tps
    sem = pltpu.SemaphoreType.DMA
    pairs = [
        (across, deep, 2), (2, deep, 2), (reps, tps), (reps,), (reps, 2), (fs_count,), (reps, tps),
    ]
    vmem = pl.BlockSpec(memory_space=pltpu.VMEM)
    return pl.pallas_call(
        functools.partial(scatter_kernel, (reps, fs_count, tps, across)),
        out_shape=(
            jax.ShapeDtypeStruct((reps, rows, 2 * width), grads.dtype),
            jax.ShapeDtypeStruct((tokens, feats), pv.dtype),
            jax.ShapeDtypeStruct((reps, tps) + taps.shape, taps.dtype),
        ),
        in_specs=[vmem] * 3,
        out_specs=(vmem,) * 3,
        scratch_shapes=[
            pltpu.VMEM((across, deep, 2, rows, width), grads.dtype),
            pltpu.VMEM((2, deep, 2, rows, width), grads.dtype),
            pltpu.VMEM((reps, tps, tokens, feats), pv.dtype),
            pltpu.VMEM((2, reps, tokens, feats), pv.dtype),
            pltpu.VMEM((fs_count,) + taps.shape, taps.dtype),
        ] + [sem(p) for p in pairs for _ in range(2)],
        compiler_params=pltpu.CompilerParams(has_side_effects=True, vmem_limit_bytes=58 * 1024 * 1024),
        name="scatter_all",
    )(grads, pv, taps)


def mix_kernel(fs_count, factor, pre, g, taps, pre_cot, terms):
    reps, ext, width = g.shape
    tokens = pre_cot.shape[1]
    fs = lax.axis_index("fs")
    row = lax.broadcasted_iota(jnp.int32, (ext, 128), 0)
    has_next, has_prev = (fs < fs_count - 1).astype(jnp.int32), (fs > 0).astype(jnp.int32)
    inside = (row < tokens) | ((row < tokens + HALO) & (has_next > 0)) | ((row >= tokens + HALO) & (has_prev > 0))

    def before(x):
        return pltpu.roll(x, 1, 0)

    def after(x):
        return pltpu.roll(x, ext - 1, 0)

    terms[...] = jnp.zeros_like(terms)

    @pl.loop(0, width // 128)
    def _(j):
        spots = [pl.ds(pl.multiple_of(branch * width + j * 128, 128), 128) for branch in range(2)]
        weights = [[taps[k : k + 1, at] for k in range(3)] for at in spots]
        for slot in range(reps):
            pres = [jnp.where(inside, pre[slot, :, at].astype(jnp.float32), 0.0) for at in spots]
            around = [(before(p), p, after(p)) for p in pres]
            gate_mix, value_mix = [sum(w * p for w, p in zip(ws, ps)) for ws, ps in zip(weights, around)]
            cot_in = jnp.where(inside, g[slot, :, spots[0]].astype(jnp.float32), 0.0)
            sig = jax.nn.sigmoid(gate_mix)
            cots = (
                cot_in * value_mix * (sig * (1.0 + gate_mix * (1.0 - sig))),
                cot_in * (gate_mix * sig),
            )
            for at, ws, ps, cot in zip(spots, weights, around, cots):
                back = ws[0] * after(cot) + ws[1] * cot + ws[2] * before(cot)
                pre_cot[slot, :, at] = back[:tokens].astype(pre_cot.dtype)
                for k in range(3):
                    total = jnp.sum(ps[k][:tokens] * cot[:tokens], axis=0, keepdims=True)
                    terms[k : k + 1, at] += total * factor


def mix_all(pre, g, taps, tokens, fs_count, factor):
    reps, ext, both = pre.shape
    vmem = pl.BlockSpec(memory_space=pltpu.VMEM)
    return pl.pallas_call(
        functools.partial(mix_kernel, fs_count, factor),
        out_shape=(
            jax.ShapeDtypeStruct((reps, tokens, both), pre.dtype),
            jax.ShapeDtypeStruct((8, both), jnp.float32),
        ),
        in_specs=[vmem] * 3,
        out_specs=(vmem,) * 2,
        compiler_params=pltpu.CompilerParams(vmem_limit_bytes=40000 * 1024),
        name="mix_all",
    )(pre, g, taps)


LANES = 128
EDGE = 16


def part_width(hid, parts):
    return min(hid, -(-hid // parts // LANES) * LANES)


TUNED = (
    ("weights_y", 0), ("weights_y", 1), ("tokens_x", 0), ("own", 2), ("own", 0), ("tokens_y", 1), ("near", 0),
    ("tokens_x", 2), ("relay", 0, 1, False), ("relay", 0, 1, True), ("tokens_y", 0), ("tokens_x", 1), ("near", 1),
    ("weights_y", 2), ("edge_out", 0), ("relay", 0, 2, False), ("edge_out", 1), ("take", 1, 0, 2), ("take", 0, 1, 1),
    ("relay", 0, 2, True), ("relay", 2, 1, False), ("own", 1), ("take", 0, 1, 0), ("edge_share", 0),
    ("edge_share", 1), ("tokens_y", 2), ("relay", 1, 1, False), ("take", 1, 1, 1), ("relay", 1, 1, True), ("near", 2),
    ("last", 0), ("take", 1, 0, 0), ("relay", 1, 2, False), ("cots", 0), ("take", 1, 0, 1), ("edge_pass", 0),
    ("edge_pass", 1), ("tokens_core",), ("take", 1, 1, 2), ("take", 1, 1, 0), ("take", 0, 1, 2), ("take_rest",),
    ("project", 0), ("mix", 0), ("relay", 1, 2, True), ("relay", 2, 1, True), ("cots", 1), ("weight", 0), ("last", 1),
    ("relay", 2, 2, False), ("project", 1), ("pass_on", 0, 2), ("relay", 2, 2, True), ("cots", 2), ("mix", 1),
    ("weight", 1), ("pass_on", 0, 1), ("last", 2), ("project", 2), ("mix", 2), ("input", 0), ("finish", 0),
    ("first", 0), ("input", 2), ("pass_on", 1, 2), ("weight", 2), ("owners", 0), ("first", 2), ("input", 1),
    ("taps",), ("pass_on", 1, 1), ("first", 1), ("second", 1), ("pass_on", 2, 2), ("finish", 1), ("second", 0),
    ("pass_on", 2, 1), ("owners", 1), ("input", 3), ("finish", 2), ("taps_sum",), ("owners", 2),
)


def plan(chunks, deep):
    return TUNED if (chunks, deep) == (3, 4) else general_plan(chunks, deep)


def general_plan(chunks, deep):
    yield "weights_y", 0
    yield "tokens_y", 0
    for c in range(1, chunks):
        yield "weights_y", c
        if c < 3:
            yield "tokens_y", c
    for k in range(min(chunks, 3), 3):
        yield "tokens_y", k
    for k in (2, 0, 1):
        yield "tokens_x", k
    for side in range(2):
        yield "edge_out", side
    yield ("tokens_core",)
    for c in range(chunks):
        yield "own", c
    yield "near", 0
    yield "relay", 0, 1, False
    for side in range(2):
        yield "edge_share", side
    yield "take", 1, 0, 2
    for c in range(1, chunks):
        yield "relay", c, 1, False
    yield "take", 0, 1, 0
    yield "relay", 0, 1, True
    for c in range(1, min(chunks, 2)):
        yield "near", c
    for dist in range(2, deep):
        yield "relay", 0, dist, False
        yield "relay", 0, dist, True
    for side in range(2):
        yield "edge_pass", side
    yield "take", 0, 1, 1
    for c in range(chunks):
        yield "cots", c
    for k in (0, 1):
        yield "take", 1, 0, k
    for c in range(2, chunks):
        yield "near", c
    for c in range(1, min(chunks, 2)):
        yield "relay", c, 1, True
        for dist in range(2, deep):
            yield "relay", c, dist, False
    yield "take", 1, 1, 0
    yield "take", 0, 1, 2
    for k in (1, 2):
        yield "take", 1, 1, k
    yield ("take_rest",)
    yield "last", 0
    yield "project", 0
    for c in range(1, chunks):
        for dist in range(1, deep):
            if c > 1 and dist > 1:
                yield "relay", c, dist, False
            if c > 1 or dist > 1:
                yield "relay", c, dist, True
    for c in range(chunks):
        if c:
            yield "last", c
            yield "project", c
        yield "mix", c
        if c < max(chunks - 1, 1):
            yield "weight", c
        if c == chunks - 2:
            for early in range(chunks - 2):
                for dist in range(deep - 1, 0, -1):
                    yield "pass_on", early, dist
    yield ("taps",)
    yield "input", 0
    yield "input", 1
    yield "first", 0
    yield "input", 2
    yield "first", 1
    yield "input", 3
    yield "first", 2
    if chunks > 1:
        yield "weight", chunks - 1
    for c in range(chunks):
        if c >= chunks - 2:
            for dist in range(deep - 1, 0, -1):
                yield "pass_on", c, dist
        if c == max(chunks - 2, 0):
            for f in range(2):
                yield "second", f
            yield ("taps_sum",)
        yield "finish", c
        yield "owners", c


def fused_kernel(
    sizes, factor, x_own, gate_w, value_w, gate_taps, value_taps, g_own,
    in_grad, gate_out, value_out, gate_taps_out, value_taps_out,
    taps_mine, x_all, w_all, g_all, pre, cot, grads, from_z, fin, pv, from_tp, first_got, second_got, terms, terms_z, terms_all,
    own_sem, wy_send, wy_recv, wz_send, wz_recv, x_send, xf_send, xs_send, x_recv, hz_send, hb_send, hs_send, hx_recv,
    g_send, g_recv, hg_send, hg_recv, sz_send, sz_recv, out_send, out_recv, tp_send, tp_recv,
    s1_send, s1_recv, s2_send, s2_recv, tz_send, tz_recv, ta_send, ta_recv,
):
    deep, across, width = sizes
    rep, fs, tp = (lax.axis_index(a) for a in ("rep", "fs", "tp"))
    z, y = fs // across, fs % across
    nrep, ny, ntp = 1 - rep, 1 - y, 1 - tp
    tokens, feats = x_own.shape
    rows, hid = gate_w.shape
    main = across * tokens
    ext = main + 2 * EDGE
    chunks = width // LANES
    both = 2 * LANES
    blocks = feats // rows
    first_feats = feats * 3 // 8 // LANES * LANES
    spans = ((0, first_feats), (first_feats, feats - first_feats))
    cuts = [tokens * k // 16 // 16 * 16 for k in (0, 6, 12, 16)]
    pieces = tuple((low, high - low) for low, high in zip(cuts, cuts[1:]))
    last = len(pieces) - 1
    weights = (gate_w, value_w)
    outs = (gate_out, value_out)
    others = [(dr, dy) for dr in range(2) for dy in range(2) if dr or dy]

    start = lambda c: c.start()
    sent = lambda c: c.wait_send()

    def landed(ref, sem):
        pltpu.make_async_copy(ref, ref, sem).wait()

    def moved(index, step):
        return (index + step) % 2

    def part_of(r, yy):
        return r * across + yy

    part = part_of(rep, y)

    def first_col(which):
        return jnp.minimum(which * width, hid - width)

    def live(which, c):
        return c * LANES >= which * width - first_col(which)

    def chunk_cols(which, c):
        return pl.ds(pl.multiple_of(first_col(which) + c * LANES, LANES), LANES)

    def all_cols(which):
        return pl.ds(pl.multiple_of(first_col(which), LANES), width)

    def cols(half):
        return pl.ds(pl.multiple_of(half * feats, feats), feats)

    def token_rows(yy):
        return pl.ds(pl.multiple_of(yy * tokens, 16), tokens)

    def lanes(branch):
        return pl.ds(branch * LANES, LANES)

    def near(side):
        return pl.ds(0, EDGE) if side == 0 else pl.ds(tokens - EDGE, EDGE)

    def far(side):
        return pl.ds(main + side * EDGE, EDGE)

    def gives_edge(side):
        return (y == 0) & (z > 0) if side == 0 else (y == across - 1) & (z < deep - 1)

    def has_edge(side):
        return z < deep - 1 if side == 0 else z > 0

    def takes_edge(side):
        return (y == 0) & (z < deep - 1) if side == 0 else (y == across - 1) & (z > 0)

    def greet():
        barrier = pltpu.get_barrier_semaphore()

        def hello(**device):
            pl.semaphore_signal(barrier, 1, device_id=device, device_id_type=pl.DeviceIdType.MESH)

        for dr in range(2):
            for dy in range(2):
                for dt in range(2):
                    if dr or dy or dt:
                        hello(rep=moved(rep, dr), fs=z * across + moved(y, dy), tp=moved(tp, dt))
        for step_z in range(1, deep):
            hello(fs=(z + step_z) % deep * across + y)
        for up in (True, False):
            @pl.when(z < deep - 1 if up else z > 0)
            def _():
                for dr, dy in others:
                    hello(rep=moved(rep, dr), fs=(z + 1 if up else z - 1) * across + moved(y, dy))
        next_levels = (z > 0).astype(jnp.int32) + (z < deep - 1).astype(jnp.int32)
        pl.semaphore_wait(barrier, 6 + deep + len(others) * next_levels)

    def w_across(c, sink):
        for branch, w in enumerate(weights):
            sink(remote(
                w.at[:, chunk_cols(part_of(rep, ny), c)], w_all.at[c, fs, :, lanes(branch)],
                wy_send.at[c, branch], wy_recv.at[c, branch], fs=z * across + ny,
            ))

    def w_along(c, block, up, down, sink):
        ref = w_all.at[c, block]
        if up:
            @pl.when(z < deep - 1)
            def _():
                sink(remote(ref, ref, wz_send.at[c, block, 0], wz_recv.at[c, block], fs=fs + across))
        if down:
            @pl.when(z > 0)
            def _():
                sink(remote(ref, ref, wz_send.at[c, block, 1], wz_recv.at[c, block], fs=fs - across))

    def w_local(c):
        return [
            pltpu.make_async_copy(
                w.at[:, chunk_cols(part, c)], w_all.at[c, fs, :, lanes(branch)], own_sem.at[2 * c + branch]
            ) for branch, w in enumerate(weights)
        ]

    def w_own_along(c, sink):
        w_along(c, fs, True, True, sink)

    def w_near_along(c, arrive, sink):
        block = z * across + ny
        if arrive:
            for branch in range(2):
                landed(w_all.at[c, block, :, lanes(branch)], wy_recv.at[c, branch])
        w_along(c, block, True, True, sink)

    def w_step(c, dist, near_block, forward, visit):
        for sign in (-1, 1):
            here = (z >= dist) if sign < 0 else (z + dist < deep)
            goes_on = (z < deep - 1) if sign < 0 else (z > 0)

            @pl.when(here & (goes_on if forward else jnp.logical_not(goes_on)))
            def _():
                visit((z + sign * dist) * across + (ny if near_block else y), sign)

    def w_relay(c, dist, near_block, sink=start):
        def visit(block, sign):
            if sink is start:
                landed(w_all.at[c, block], wz_recv.at[c, block])
            w_along(c, block, sign < 0, sign > 0, sink)

        w_step(c, dist, near_block, True, visit)

    def w_last(c):
        for dist in range(1, deep):
            for near_block in (False, True):
                w_step(
                    c, dist, near_block, False,
                    lambda block, sign: landed(w_all.at[c, block], wz_recv.at[c, block]),
                )

    def x_at(r, yy, k, half):
        offset, size = pieces[k]
        return x_all.at[r, pl.ds(pl.multiple_of(yy * tokens + offset, 16), size), cols(half)]

    def x_mine(k):
        return x_own.at[pl.ds(*pieces[k])]

    def x_across(k, sink):
        sink(remote(x_mine(k), x_at(rep, y, k, tp), x_send.at[1, k], x_recv.at[rep, y, k, tp], fs=z * across + ny))

    def x_over(k, sink):
        sink(remote(x_mine(k), x_at(rep, y, k, tp), x_send.at[0, k], x_recv.at[rep, y, k, tp], rep=nrep))

    def x_to_sibling(sink):
        for k in range(len(pieces)):
            sink(remote(x_mine(k), x_at(rep, y, k, tp), xs_send.at[rep, y, k], x_recv.at[rep, y, k, tp], tp=ntp))

    def x_forward(k, sink):
        if k < last:
            ref = x_at(rep, ny, k, tp)
            sink(remote(ref, ref, xf_send.at[k], x_recv.at[rep, ny, k, tp], rep=nrep))
        else:
            ref = x_at(nrep, y, k, tp)
            sink(remote(ref, ref, xf_send.at[k], x_recv.at[nrep, y, k, tp], fs=z * across + ny))

    def x_take(r, yy, k, forward):
        x_landed(r, yy, k, tp)
        if forward:
            x_forward(k, start)
        x_share(r, yy, k, start)

    def x_share(r, yy, k, sink):
        ref = x_at(r, yy, k, tp)
        sink(remote(ref, ref, xs_send.at[r, yy, k], x_recv.at[r, yy, k, tp], tp=ntp))

    def x_landed(r, yy, k, half):
        landed(x_at(r, yy, k, half), x_recv.at[r, yy, k, half])

    def edge_out(side, sink):
        target = fs - across if side == 0 else fs + across

        @pl.when(gives_edge(side))
        def _():
            sink(remote(
                x_own.at[near(side)], x_all.at[rep, far(side), cols(tp)], hz_send.at[side],
                hx_recv.at[side, rep, tp], fs=target,
            ))
            level = z - 1 if side == 0 else z + 1
            for dr in range(2):
                for dy in range(2):
                    r, yy = moved(rep, dr), moved(y, dy)
                    sink(remote(
                        g_own.at[near(side), all_cols(part_of(r, yy))], g_all.at[rep, far(side)],
                        hg_send.at[side, dr, dy], hg_recv.at[side, rep], rep=r, fs=level * across + yy,
                    ))

    def edge_at(side, r, half):
        return x_all.at[r, far(side), cols(half)]

    def edge_share(side, sink=start):
        @pl.when(takes_edge(side))
        def _():
            ref = edge_at(side, rep, tp)
            if sink is start:
                landed(ref, hx_recv.at[side, rep, tp])
            for dr, dy in others:
                sink(remote(
                    ref, ref, hb_send.at[side, dr, dy], hx_recv.at[side, rep, tp],
                    rep=moved(rep, dr), fs=z * across + moved(y, dy),
                ))
            sink(remote(ref, ref, hs_send.at[side, rep], hx_recv.at[side, rep, tp], tp=ntp))

    def edge_pass(side, sink=start):
        for r in (rep, nrep):
            @pl.when(has_edge(side) & jnp.logical_not(takes_edge(side) & (r == rep)))
            def _():
                ref = edge_at(side, r, tp)
                if sink is start:
                    landed(ref, hx_recv.at[side, r, tp])
                sink(remote(ref, ref, hs_send.at[side, r], hx_recv.at[side, r, tp], tp=ntp))

    def edge_landed(side):
        @pl.when(has_edge(side))
        def _():
            for r in range(2):
                landed(edge_at(side, r, ntp), hx_recv.at[side, r, ntp])
                landed(g_all.at[r, far(side)], hg_recv.at[side, r])

    def g_direct(c, sink):
        for dr, dy in others:
            r, yy = moved(rep, dr), moved(y, dy)
            sink(remote(
                g_own.at[:, chunk_cols(part_of(r, yy), c)], g_all.at[rep, token_rows(y), pl.ds(c * LANES, LANES)],
                g_send.at[c, dr, dy], g_recv.at[c, rep, y], rep=r, fs=z * across + yy,
            ))

    def g_landed(c):
        for dr, dy in others:
            r, yy = moved(rep, dr), moved(y, dy)
            landed(g_all.at[r, token_rows(yy), pl.ds(c * LANES, LANES)], g_recv.at[c, r, yy])

    x_local = pltpu.make_async_copy(
        x_own, x_all.at[rep, token_rows(y), cols(tp)], own_sem.at[2 * chunks]
    )
    g_local = pltpu.make_async_copy(
        g_own.at[:, all_cols(part)], g_all.at[rep, token_rows(y)], own_sem.at[2 * chunks + 1]
    )

    tap_cols = pl.ds(pl.multiple_of(tp * hid + first_col(part), LANES), width)
    taps_local = [
        pltpu.make_async_copy(ref.at[:, tap_cols], taps_mine.at[b], own_sem.at[2 * chunks + 2 + b])
        for b, ref in enumerate((gate_taps, value_taps))
    ]

    def chunk_lanes(c):
        return pl.ds(c * both, both)

    def project(c):
        @pl.loop(0, 2)
        def _(slot):
            total = jnp.dot(
                x_all[slot], w_all[c].reshape(-1, both), preferred_element_type=jnp.float32
            )
            pre[slot] = total.astype(pre.dtype)

    def mix(c):
        row = lax.broadcasted_iota(jnp.int32, (ext, LANES), 0)
        has_next, has_prev = (z < deep - 1).astype(jnp.int32), (z > 0).astype(jnp.int32)
        inside = (row < main) | ((row < main + EDGE) & (has_next > 0)) | ((row >= main + EDGE) & (has_prev > 0))
        counted = inside & (live(part, c).astype(jnp.int32) > 0)
        taps = [[taps_mine[b, k : k + 1, pl.ds(c * LANES, LANES)] for k in range(3)] for b in range(2)]
        terms[:, pl.ds(c * LANES, LANES)] = jnp.zeros((8, LANES), jnp.float32)

        def before(v):
            return pltpu.roll(v, 1, 0)

        def after(v):
            return pltpu.roll(v, ext - 1, 0)

        @pl.loop(0, 2)
        def _(slot):
            pres = [jnp.where(inside, pre[slot, :, lanes(b)].astype(jnp.float32), 0.0) for b in range(2)]
            around = [(before(p), p, after(p)) for p in pres]
            gate_mix, value_mix = [sum(w * p for w, p in zip(ws, ps)) for ws, ps in zip(taps, around)]
            cot_in = jnp.where(counted, g_all[slot, :, pl.ds(c * LANES, LANES)].astype(jnp.float32), 0.0)
            sig = jax.nn.sigmoid(gate_mix)
            cots = (
                cot_in * value_mix * (sig * (1.0 + gate_mix * (1.0 - sig))),
                cot_in * (gate_mix * sig),
            )
            for b in range(2):
                ws, ps, one = taps[b], around[b], cots[b]
                back = ws[0] * after(one) + ws[1] * one + ws[2] * before(one)
                cot[slot, :, pl.ds(c * both + b * LANES, LANES)] = back[:main].astype(cot.dtype)
                for k in range(3):
                    total = jnp.sum(ps[k][:main] * one[:main], axis=0, keepdims=True)
                    terms[2 * k + b : 2 * k + b + 1, pl.ds(c * LANES, LANES)] += total * factor

    def far_first(visit):
        @pl.loop(0, 2 * deep - 1)
        def _(i):
            dist = deep - 1 - i // 2
            level = jnp.where(i % 2 == 0, z + dist, z - dist)

            @pl.when((level >= 0) & (level < deep))
            def _():
                visit(level)

    def sum_hop(c, block, up, sink):
        way = 0 if up else 1
        sink(remote(
            grads.at[c, block], from_z.at[way, c, block], sz_send.at[c, block], sz_recv.at[way, c, block],
            fs=fs + across if up else fs - across,
        ))

    def weight_terms(c):
        def visit(level):
            for yy in (ny, y):
                block = level * across + yy
                at = pl.ds(pl.multiple_of(block * rows, rows), rows)
                total = sum(
                    lax.dot_general(
                        x_all[slot, :main, at], cot[slot, :, chunk_lanes(c)], (((0,), (0,)), ((), ())),
                        preferred_element_type=jnp.float32,
                    ) for slot in range(2)
                )
                grads[c, block] = (total * factor).astype(grads.dtype)
            for up in (True, False):
                @pl.when((level > z) & (z == 0) if up else (level < z) & (z == deep - 1))
                def _():
                    for yy in (ny, y):
                        sum_hop(c, level * across + yy, up, start)

        far_first(visit)

    def pass_on(c, dist):
        for up in (True, False):
            level = z + dist if up else z - dist

            @pl.when((z > 0) & (z < deep - 1) & ((level < deep) if up else (level >= 0)))
            def _():
                way = 0 if up else 1
                for yy in (ny, y):
                    block = level * across + yy
                    landed(from_z.at[way, c, block], sz_recv.at[way, c, block])
                    total = grads[c, block].astype(jnp.float32) + from_z[way, c, block].astype(jnp.float32)
                    grads[c, block] = total.astype(grads.dtype)
                    sum_hop(c, block, up, start)

    def sums_sent(c):
        def visit(level):
            for up in (True, False):
                @pl.when((level > z) if up else (level < z))
                def _():
                    for yy in range(across):
                        sum_hop(c, level * across + yy, up, sent)

        far_first(visit)

    def to_owners(c, same, sink):
        here = chunk_cols(part, c)
        for branch, out in enumerate(outs):
            sems = out_send.at[c, branch, 0 if same else 1], out_recv.at[c, branch, rep, y]
            if same:
                sink(remote(out.at[:, here], out.at[:, here], *sems, rep=nrep))
            else:
                sink(remote(fin.at[c, :, lanes(branch)], out.at[:, here], *sems, fs=z * across + ny))

    def owners_pass(c, sink=start):
        source = part_of(rep, ny)

        @pl.when(live(source, c))
        def _():
            for branch, out in enumerate(outs):
                ref, sem = out.at[:, chunk_cols(source, c)], out_recv.at[c, branch, rep, ny]
                if sink is start:
                    landed(ref, sem)
                sink(remote(ref, ref, out_send.at[c, branch, 2], sem, rep=nrep))

    def owners_last(c):
        for yy in (y, ny):
            source = part_of(nrep, yy)

            @pl.when(live(source, c))
            def _():
                for branch, out in enumerate(outs):
                    landed(out.at[:, chunk_cols(source, c)], out_recv.at[c, branch, nrep, yy])

    def finish(c):
        for same in (False, True):
            block = z * across + (y if same else ny)
            for way in range(2):
                @pl.when(z > 0 if way == 0 else z < deep - 1)
                def _():
                    landed(from_z.at[way, c, block], sz_recv.at[way, c, block])
            total = grads[c, block].astype(jnp.float32)
            for way in range(2):
                total += from_z[way, c, block].astype(jnp.float32)
            total = total.astype(grads.dtype)

            @pl.when(live(part, c))
            def _():
                if same:
                    for branch, out in enumerate(outs):
                        out[:, chunk_cols(part, c)] = total[:, branch * LANES : (branch + 1) * LANES]
                else:
                    fin[c] = total
                to_owners(c, same, start)

    def input_terms(dr, dy):
        r, yy = moved(rep, dr), moved(y, dy)
        q = part_of(r, yy)

        def terms_of(half):
            @pl.loop(0, blocks)
            def _(j):
                total = sum(
                    lax.dot_general(
                        cot[r, token_rows(yy), chunk_lanes(c)], w_all[c, half * blocks + j],
                        (((1,), (1,)), ((), ())), preferred_element_type=jnp.float32,
                    ) for c in range(chunks)
                )
                pv[half, q, :, pl.ds(pl.multiple_of(j * rows, rows), rows)] = total.astype(pv.dtype)

        terms_of(ntp)
        tp_hop(q, start)
        terms_of(tp)

    def tp_hop(q, sink):
        sink(remote(pv.at[ntp, q], from_tp.at[q], tp_send.at[q], tp_recv.at[q], tp=ntp))

    def f_cols(f):
        return pl.ds(*spans[f])

    def first_hop(f, k, sink):
        q = part_of(nrep, ny) if k else part_of(nrep, y) if f == 0 else part_of(rep, ny)
        target = dict(rep=nrep) if f == 0 else dict(fs=z * across + ny)
        sink(remote(pv.at[tp, q, :, f_cols(f)], first_got.at[f, k, :, pl.ds(0, spans[f][1])], s1_send.at[f, k], s1_recv.at[f, k], **target))

    def second_hop(f, sink):
        q = part_of(rep, ny) if f == 0 else part_of(nrep, y)
        target = dict(fs=z * across + ny) if f == 0 else dict(rep=nrep)
        sink(remote(pv.at[tp, q, :, f_cols(f)], second_got.at[f, :, pl.ds(0, spans[f][1])], s2_send.at[f], s2_recv.at[f], **target))

    def row_tiles(body):
        @pl.loop(0, tokens // 16)
        def _(i):
            body(pl.ds(pl.multiple_of(i * 16, 16), 16))

    def add_sibling(q):
        landed(from_tp.at[q], tp_recv.at[q])

        def body(at):
            total = pv[tp, q, at].astype(jnp.float32) + from_tp[q, at].astype(jnp.float32)
            pv[tp, q, at] = total.astype(pv.dtype)

        row_tiles(body)

    def input_first(dr, dy):
        add_sibling(part_of(moved(rep, dr), moved(y, dy)))
        if dr:
            first_hop(0, dy, start)
        if dy:
            first_hop(1, dr, start)

    def input_second(f):
        q = part_of(rep, ny) if f == 0 else part_of(nrep, y)
        landed(first_got.at[f, 1, :, pl.ds(0, spans[f][1])], s1_recv.at[f, 1])

        def body(at):
            total = pv[tp, q, at, f_cols(f)].astype(jnp.float32)
            total += first_got[f, 1, at, : spans[f][1]].astype(jnp.float32)
            pv[tp, q, at, f_cols(f)] = total.astype(pv.dtype)

        row_tiles(body)
        second_hop(f, start)

    def input_last():
        landed(from_tp.at[part], tp_recv.at[part])
        for f in range(2):
            landed(first_got.at[f, 0, :, pl.ds(0, spans[f][1])], s1_recv.at[f, 0])
            landed(second_got.at[f, :, pl.ds(0, spans[f][1])], s2_recv.at[f])

        def body(at):
            for f in range(2):
                total = pv[tp, part, at, f_cols(f)].astype(jnp.float32) + from_tp[part, at, f_cols(f)].astype(jnp.float32)
                total += first_got[f, 0, at, : spans[f][1]].astype(jnp.float32) + second_got[f, at, : spans[f][1]].astype(jnp.float32)
                in_grad[at, f_cols(f)] = total.astype(in_grad.dtype)

        row_tiles(body)

    def taps_along(sink):
        for step in range(1, deep):
            to = (z + step) % deep
            sink(remote(
                terms_z.at[z], terms_z.at[z], tz_send.at[step], tz_recv.at[z], fs=to * across + y
            ))

    def taps_start():
        terms_z[z] = terms[...]
        taps_along(start)

    def taps_out(sink):
        ref = terms_all.at[rep, y, tp]
        for dr in range(2):
            for dy in range(2):
                for dt in range(2):
                    if dr or dy or dt:
                        sink(remote(
                            ref, ref, ta_send.at[dr, dy, dt], ta_recv.at[rep, y, tp],
                            rep=moved(rep, dr), fs=z * across + moved(y, dy), tp=moved(tp, dt),
                        ))

    def taps_sum():
        for step in range(1, deep):
            source = (z + step) % deep
            landed(terms_z.at[source], tz_recv.at[source])
        terms_all[rep, y, tp] = sum(terms_z[level] for level in range(deep))
        taps_out(start)

    def taps_last():
        for dr in range(2):
            for dy in range(2):
                for dt in range(2):
                    if dr or dy or dt:
                        at = (moved(rep, dr), moved(y, dy), moved(tp, dt))
                        landed(terms_all.at[at], ta_recv.at[at])
        for r in range(2):
            for yy in range(across):
                which = r * across + yy
                first = min(which * width, hid - width)
                skip = which * width - first
                for half in range(2):
                    for branch, out in enumerate((gate_taps_out, value_taps_out)):
                        for k in range(3):
                            if skip < width:
                                begin = half * hid + first + skip
                                out[k : k + 1, begin : begin + width - skip] = terms_all[
                                    r, yy, half, 2 * k + branch : 2 * k + branch + 1, skip:
                                ]

    for c in range(chunks):
        for copy in w_local(c):
            copy.start()
    x_local.start()
    g_local.start()
    for copy in taps_local:
        copy.start()
    for way in range(2):
        @pl.when((z == 0) if way == 0 else (z == deep - 1))
        def _():
            for c in range(chunks):
                for yy in range(across):
                    from_z[way, c, z * across + yy] = jnp.zeros((rows, both), from_z.dtype)
    greet()

    def w_own(c):
        for copy in w_local(c):
            copy.wait()
        w_own_along(c, start)

    def take(dr, dy, k):
        x_take(moved(rep, dr), moved(y, dy), k, (not dr) if k < last else (not dy))

    def take_rest():
        x_local.wait()
        g_local.wait()
        for copy in taps_local:
            copy.wait()
        for r in range(2):
            for yy in range(across):
                for k in range(len(pieces)):
                    x_landed(r, yy, k, ntp)
        for side in range(2):
            edge_landed(side)

    def mix_chunk(c):
        g_landed(c)
        mix(c)

    offsets = ((1, 1), (0, 1), (1, 0), (0, 0))
    actions = dict(
        weights_y=lambda c: w_across(c, start),
        tokens_y=lambda k: x_across(k, start),
        tokens_x=lambda k: x_over(k, start),
        tokens_core=lambda: x_to_sibling(start),
        edge_out=lambda side: edge_out(side, start),
        own=w_own,
        near=lambda c: w_near_along(c, True, start),
        relay=w_relay,
        edge_share=edge_share,
        edge_pass=edge_pass,
        take=take,
        cots=lambda c: g_direct(c, start),
        take_rest=take_rest,
        last=w_last,
        project=project,
        mix=mix_chunk,
        weight=weight_terms,
        pass_on=pass_on,
        finish=finish,
        owners=owners_pass,
        taps=taps_start,
        taps_sum=taps_sum,
        input=lambda i: input_terms(*offsets[i]),
        first=lambda i: input_first(*offsets[i]),
        second=input_second,
    )
    for name, *args in plan(chunks, deep):
        actions[name](*args)
    input_last()
    taps_last()
    for c in range(chunks):
        owners_last(c)
    for side in range(2):
        edge_out(side, sent)
        edge_share(side, sent)
        edge_pass(side, sent)
    x_to_sibling(sent)
    for k in range(len(pieces)):
        x_across(k, sent)
        x_over(k, sent)
        x_forward(k, sent)
        for dr, dy in others:
            x_share(moved(rep, dr), moved(y, dy), k, sent)
    for c in range(chunks):
        w_across(c, sent)
        w_own_along(c, sent)
        w_near_along(c, False, sent)
        for dist in range(1, deep):
            for near_block in (False, True):
                w_relay(c, dist, near_block, sent)
        g_direct(c, sent)
        sums_sent(c)

        @pl.when(live(part, c))
        def _():
            for same in (False, True):
                to_owners(c, same, sent)

        owners_pass(c, sent)
    for dr in range(2):
        for dy in range(2):
            tp_hop(part_of(moved(rep, dr), moved(y, dy)), sent)
    for f in range(2):
        for k in range(2):
            first_hop(f, k, sent)
        second_hop(f, sent)
    taps_along(sent)
    taps_out(sent)


def fused_all(across, x_own, gate_w, value_w, gate_taps, value_taps, g_own):
    reps, fs_count, tps = (lax.axis_size(a) for a in ("rep", "fs", "tp"))
    deep = fs_count // across
    tokens, feats = x_own.shape
    rows, hid = gate_w.shape
    width = part_width(hid, reps * across)
    chunks = width // LANES
    both = 2 * LANES
    main = across * tokens
    ext = main + 2 * EDGE
    parts = reps * across
    factor = float(tokens * fs_count * reps) ** (-0.5)
    dtype = x_own.dtype
    f32 = jnp.float32
    sem = pltpu.SemaphoreType.DMA
    sems = [
        (2 * chunks + 4,), (chunks, 2), (chunks, 2), (chunks, fs_count, 2), (chunks, fs_count), (2, 3), (3,),
        (reps, across, 3), (reps, across, 3, tps), (2,), (2, 2, 2), (2, reps), (2, reps, tps),
        (chunks, 2, 2), (chunks, reps, across), (2, 2, 2), (2, reps), (chunks, fs_count), (2, chunks, fs_count),
        (chunks, 2, 3), (chunks, 2, reps, across), (parts,), (parts,),
        (2, 2), (2, 2), (2,), (2,), (deep,), (deep,), (2, 2, 2), (reps, across, tps),
    ]
    buffers = [
        ((2, 3, width), f32), ((reps, ext, tps * feats), dtype), ((chunks, fs_count, rows, both), dtype), ((reps, ext, width), dtype),
        ((reps, ext, both), dtype), ((reps, main, 2 * width), dtype), ((chunks, fs_count, rows, both), dtype),
        ((2, chunks, fs_count, rows, both), dtype), ((chunks, rows, both), dtype),
        ((tps, parts, tokens, feats), dtype), ((parts, tokens, feats), dtype),
        ((2, 2, tokens, feats), dtype), ((2, tokens, feats), dtype),
        ((8, width), f32), ((deep, 8, width), f32), ((reps, across, tps, 8, width), f32),
    ]
    vmem, hbm = pl.BlockSpec(memory_space=pltpu.VMEM), pl.BlockSpec(memory_space=pl.ANY)
    return pl.pallas_call(
        functools.partial(fused_kernel, (deep, across, width), factor),
        out_shape=(
            jax.ShapeDtypeStruct((tokens, feats), dtype),
            jax.ShapeDtypeStruct((rows, hid), dtype),
            jax.ShapeDtypeStruct((rows, hid), dtype),
            jax.ShapeDtypeStruct(gate_taps.shape, f32),
            jax.ShapeDtypeStruct(value_taps.shape, f32),
        ),
        in_specs=[hbm] * 6,
        out_specs=(vmem,) * 5,
        scratch_shapes=[pltpu.VMEM(*b) for b in buffers] + [sem(s) for s in sems],
        compiler_params=pltpu.CompilerParams(has_side_effects=True, collective_id=0, vmem_limit_bytes=60 * 1024 * 1024),
        name="fused_all",
    )(x_own, gate_w, value_w, gate_taps, value_taps, g_own)


def store_kernel(in_grad, gate, value, gate_taps, value_taps, *refs):
    outs, held, (gate_wide, value_wide, load_sem, sem) = refs[:5], refs[5:10], refs[10:]
    sources = (in_grad, gate, value, gate_taps, value_taps)
    count = load_sem.shape[1]

    def split(k):
        rows = sources[k].shape[0]
        size = rows // count
        return [pl.ds(p * size, size) for p in range(count)] if size % 16 == 0 and size * count == rows else [pl.ds(0, rows)]

    tasks = [(k, p, at) for k in (1, 2, 0, 3, 4) for p, at in enumerate(split(k))]
    loads = [pltpu.make_async_copy(sources[k].at[at], held[k].at[at], load_sem.at[k, p]) for k, p, at in tasks]
    for load in loads:
        load.start()
    stores = []
    for (k, p, at), load in zip(tasks, loads):
        load.wait()
        src = {1: gate_wide, 2: value_wide}.get(k, held[k])
        if k in (1, 2):
            src[at] = held[k][at].astype(src.dtype)
        stores.append(pltpu.make_async_copy(src.at[at], outs[k].at[at], sem.at[k, p]))
        stores[-1].start()
    for store in stores:
        store.wait()


def store_all(*arrays):
    hbm = pl.BlockSpec(memory_space=pl.ANY)
    wide = jax.ShapeDtypeStruct(arrays[1].shape, jnp.float32)
    outs = [jax.ShapeDtypeStruct(a.shape, a.dtype) for a in arrays]
    outs[1:3] = wide, wide
    sem = pltpu.SemaphoreType.DMA((5, 4))
    return pl.pallas_call(
        store_kernel,
        out_shape=tuple(outs),
        in_specs=[hbm] * 5,
        out_specs=(hbm,) * 5,
        scratch_shapes=[pltpu.VMEM(a.shape, a.dtype) for a in arrays] + [pltpu.VMEM(wide.shape, wide.dtype)] * 2 + [sem] * 2,
        compiler_params=pltpu.CompilerParams(vmem_limit_bytes=60 * 1024 * 1024),
        name="store_all",
    )(*arrays)


def fits_plane(across, inputs, gate_proj):
    reps, fs_count, tps = (lax.axis_size(a) for a in ("rep", "fs", "tp"))
    tokens, feats = inputs.shape[1:]
    rows, hid = gate_proj.shape
    parts = reps * across
    width = part_width(hid, parts)
    return (
        reps == across == tps == 2 and fs_count > across and tokens % 16 == 0 and tokens >= 48
        and hid % LANES == 0 and rows % LANES == 0 and feats % rows == 0 and feats % (2 * LANES) == 0
        and 4 * parts * width <= 5 * hid
    )


def shards(across, inputs, gate_proj, value_proj, gate_taps, value_taps, out_grad):
    if fits_plane(across, inputs, gate_proj):
        in_grad, gate_grad, value_grad, gate_terms, value_terms = store_all(
            *fused_all(across, inputs[0], gate_proj, value_proj, gate_taps, value_taps, out_grad[0])
        )
        return in_grad[None], gate_grad, value_grad, gate_terms, value_terms

    contract_cols = (((1,), (1,)), ((), ()))
    contract_rows = (((0,), (0,)), ((), ()))
    reps, fs_count = lax.axis_size("rep"), lax.axis_size("fs")
    rep = lax.axis_index("rep")
    tokens, feats = inputs.shape[1:]
    hid = gate_proj.shape[1]
    width = min(hid, -(-hid // reps // 128) * 128)
    last = hid - width

    def start_of(part):
        return jnp.minimum(part * width, last)

    first = start_of(rep)
    dead = rep * width - first
    live = jnp.arange(width) >= dead

    def part_cols(x, part):
        return lax.dynamic_slice_in_dim(x, start_of(part), width, x.ndim - 1)

    w_own = jnp.concatenate(
        [jnp.where(live, part_cols(w, rep), jnp.zeros((), w.dtype)) for w in (gate_proj, value_proj)], axis=1
    )
    g_parts = jnp.stack([part_cols(out_grad[0], (rep + step) % reps) for step in range(reps)])
    x_all, g_all, w_all = gather_all(inputs[0], g_parts, w_own, across)
    w_all = w_all.reshape(-1, 2 * width)

    ext = tokens + 2 * HALO
    pre = jnp.dot(x_all.reshape(reps * ext, -1), w_all, preferred_element_type=jnp.float32)
    pre = pre.astype(jnp.bfloat16).reshape(reps, ext, 2 * width)
    tap_start = lax.axis_index("tp") * hid + first
    taps = jnp.concatenate(
        [lax.dynamic_slice_in_dim(t, tap_start, width, 1) for t in (gate_taps, value_taps)], axis=1
    )
    factor = float(tokens * fs_count * reps) ** (-0.5)
    pre_cot, tap_terms = mix_all(pre, g_all, taps, tokens, fs_count, factor)
    pre_cot = pre_cot.reshape(reps * tokens, 2 * width)
    tap_terms = tap_terms[:3]

    grads = lax.dot_general(
        x_all[:, :tokens].reshape(reps * tokens, -1), pre_cot, contract_rows, preferred_element_type=jnp.float32
    )
    grads = (grads * factor).astype(jnp.bfloat16).reshape(fs_count, -1, 2 * width)
    partial_value = lax.dot_general(pre_cot, w_all, contract_cols, preferred_element_type=jnp.float32)
    partial_value = partial_value.astype(jnp.bfloat16).reshape(reps, tokens, -1)
    lanes = -(-tap_terms.size // 1024) * 128
    tap_terms = jnp.pad(tap_terms.reshape(-1), (0, 8 * lanes - tap_terms.size)).reshape(8, lanes)
    own, in_grad, tap_all = scatter_all(grads, partial_value, tap_terms, across)

    skips = [max(0, p * width - last) for p in range(reps)]
    proj_grads = [
        jnp.concatenate(
            [own[p, :, branch * width + skips[p] : (branch + 1) * width] for p in range(reps)], axis=1
        ).astype(jnp.float32)
        for branch in range(2)
    ]
    tap_all = tap_all.reshape(reps, -1, 8 * lanes)[:, :, : 6 * width].reshape(reps, -1, 3, 2, width)
    taps_out = jnp.concatenate(
        [tap_all[p, half, :, :, skips[p] :] for half in range(tap_all.shape[1]) for p in range(reps)], axis=2
    )
    return in_grad[None], proj_grads[0], proj_grads[1], taps_out[:, 0], taps_out[:, 1]


def solution(mesh):
    placed = (P("rep", "fs", "tp"), P("fs", "tp"), P("fs", "tp"), P(), P(), P("rep", "fs", "tp"))
    return jax.shard_map(
        functools.partial(shards, row_length(mesh)),
        mesh=mesh,
        in_specs=placed,
        out_specs=(P("rep", "fs", "tp"), P("fs", "tp"), P("fs", "tp"), P(), P()),
        check_vma=False,
    )
```

```python
import functools

import jax
import jax.numpy as jnp
from jax import lax
from jax.experimental import pallas as pl
from jax.experimental.pallas import tpu as pltpu
from jax.sharding import PartitionSpec as P

HALO = 8


def row_length(mesh):
    axis = mesh.axis_names.index("fs")
    devices = mesh.devices.swapaxes(0, axis)
    line = devices.reshape(devices.shape[0], -1)[:, 0]
    places = [tuple(getattr(d, "coords", (i,))) for i, d in enumerate(line)]
    moved = lambda a, b: [i for i in range(len(a)) if a[i] != b[i]]
    length = 1
    while length < len(places) and moved(places[0], places[length]) == moved(places[0], places[1]):
        length += 1
    return length if len(places) % length == 0 else 1


def remote(src, dst, send, recv, **device):
    return pltpu.make_async_remote_copy(
        src_ref=src, dst_ref=dst, send_sem=send, recv_sem=recv, device_id=device, device_id_type=pl.DeviceIdType.MESH
    )


def gather_kernel(
    sizes, x_ref, g_ref, w_ref, x_all, g_all, w_all,
    w_send, w_recv, xr_send, xt_send, x_recv, xh_send, xh_recv, g_send, g_recv, gh_send, gh_recv, own_sem,
):
    reps, fs_count, tps, across = sizes
    deep = fs_count // across
    rep, fs, tp = (lax.axis_index(a) for a in ("rep", "fs", "tp"))
    z, y = fs // across, fs % across
    tokens, feats = x_ref.shape

    def other(axis_index, step, count):
        return (axis_index + step) % count

    def cols(index):
        return pl.ds(pl.multiple_of(index * feats, feats), feats)

    half_width = w_ref.shape[1] // 2

    def half(c):
        return pl.ds(c * half_width, half_width)

    def send_w(block, c, src, way, target):
        return remote(
            src.at[:, half(c)], w_all.at[block, :, half(c)], w_send.at[block, c, way], w_recv.at[block, c], fs=target
        )

    def along(block, c, src, down, up, sink):
        if down:
            @pl.when(z > 0)
            def _():
                sink(send_w(block, c, src, 0, fs - across))
        if up:
            @pl.when(z < deep - 1)
            def _():
                sink(send_w(block, c, src, 1, fs + across))

    def to_row(block, c, src, sink):
        for step in range(1, across):
            sink(send_w(block, c, src, 1 + step, z * across + other(y, step, across)))

    start = lambda c: c.start()
    sent = lambda c: c.wait_send()

    def x_main(slot, src, sem, **device):
        return remote(src, x_all.at[slot, pl.ds(0, tokens), cols(tp)], sem, x_recv.at[slot, tp], **device)

    def halos(sink):
        for side in range(2):
            near = pl.ds(0, HALO) if side == 0 else pl.ds(tokens - HALO, HALO)
            far = pl.ds(tokens + side * HALO, HALO)
            target = fs - 1 if side == 0 else fs + 1

            @pl.when((fs > 0) if side == 0 else (fs < fs_count - 1))
            def _():
                for slot in range(reps):
                    to_rep = other(rep, slot, reps)
                    for step in range(tps):
                        sink(remote(
                            x_ref.at[near], x_all.at[slot, far, cols(tp)], xh_send.at[side, slot, step],
                            xh_recv.at[side, slot, tp], rep=to_rep, fs=target, tp=other(tp, step, tps),
                        ))
                    sink(remote(
                        g_ref.at[slot, near], g_all.at[slot, far], gh_send.at[side, slot],
                        gh_recv.at[side, slot], rep=to_rep, fs=target,
                    ))

    def to_reps(sink):
        for slot in range(1, reps):
            sink(x_main(slot, x_ref, xr_send.at[slot], rep=other(rep, slot, reps)))
        for slot in range(1, reps):
            sink(remote(
                g_ref.at[slot], g_all.at[slot, pl.ds(0, tokens)], g_send.at[slot], g_recv.at[slot],
                rep=other(rep, slot, reps),
            ))

    def to_tps(slot, src, sink):
        for step in range(1, tps):
            sink(x_main(slot, src, xt_send.at[slot, step], tp=other(tp, step, tps)))

    halos(start)
    for c in range(2):
        along(fs, c, w_ref, True, True, start)
        to_row(fs, c, w_ref, start)
    to_reps(start)
    to_tps(0, x_ref, start)
    own = [
        pltpu.make_async_copy(w_ref, w_all.at[fs], own_sem.at[0]),
        pltpu.make_async_copy(x_ref, x_all.at[0, pl.ds(0, tokens), cols(tp)], own_sem.at[1]),
        pltpu.make_async_copy(g_ref.at[0], g_all.at[0, pl.ds(0, tokens)], own_sem.at[2]),
    ]
    for copy in own:
        copy.start()

    def landed(ref, sem):
        pltpu.make_async_copy(ref, ref, sem).wait()

    def hops(dist, arrive, sink):
        for sign in (-1, 1):
            block = fs + sign * dist * across

            @pl.when((z >= dist) if sign < 0 else (z + dist < deep))
            def _():
                for c in range(2):
                    if arrive:
                        landed(w_all.at[block, :, half(c)], w_recv.at[block, c])
                    along(block, c, w_all.at[block], sign > 0, sign < 0, sink)
                    if c == 0:
                        to_row(block, c, w_all.at[block], sink)
                    else:
                        level = z + sign * dist

                        @pl.when((level > 0) & (level < deep - 1))
                        def _():
                            to_row(block, c, w_all.at[block], sink)

    def across_first(dist, arrive, sink):
        for end in ((0, deep - 1) if deep > 1 else (0,)):
            @pl.when(z == end + dist if end == 0 else z == end - dist)
            def _():
                for step in range(1, across):
                    block = end * across + other(y, step, across)
                    if arrive:
                        landed(w_all.at[block, :, half(1)], w_recv.at[block, 1])
                    along(block, 1, w_all.at[block], end > 0, end == 0 and deep > 1, sink)

    def forward_x(arrive, sink):
        for slot in range(1, reps):
            mine = x_all.at[slot, pl.ds(0, tokens), cols(tp)]
            if arrive:
                landed(mine, x_recv.at[slot, tp])
            to_tps(slot, mine, sink)

    for dist in range(1, deep):
        hops(dist, True, start)
        across_first(dist - 1, True, start)
        if dist == 1:
            forward_x(True, start)
    if deep == 1:
        forward_x(True, start)
    across_first(deep - 1, True, start)

    for slot in range(reps):
        for step in range(1, tps):
            source = other(tp, step, tps)
            landed(x_all.at[slot, pl.ds(0, tokens), cols(source)], x_recv.at[slot, source])
        if slot:
            landed(g_all.at[slot, pl.ds(0, tokens)], g_recv.at[slot])
    for side in range(2):
        far = pl.ds(tokens + side * HALO, HALO)

        @pl.when((fs < fs_count - 1) if side == 0 else (fs > 0))
        def _():
            for slot in range(reps):
                for source in range(tps):
                    landed(x_all.at[slot, far, cols(source)], xh_recv.at[side, slot, source])
                landed(g_all.at[slot, far], gh_recv.at[side, slot])
    for level in range(deep):
        for step in range(1, across):
            block = level * across + other(y, step, across)
            landed(w_all.at[block, :, half(0)], w_recv.at[block, 0])
            if 0 < level < deep - 1:
                landed(w_all.at[block, :, half(1)], w_recv.at[block, 1])
    for copy in own:
        copy.wait()
    halos(sent)
    for c in range(2):
        along(fs, c, w_ref, True, True, sent)
        to_row(fs, c, w_ref, sent)
    to_reps(sent)
    to_tps(0, x_ref, sent)
    for dist in range(1, deep):
        hops(dist, False, sent)
    for dist in range(deep):
        across_first(dist, False, sent)
    forward_x(False, sent)


def gather_all(x_own, g_parts, w_own, across):
    reps, fs_count, tps = (lax.axis_size(a) for a in ("rep", "fs", "tp"))
    tokens, feats = x_own.shape
    width = g_parts.shape[2]
    ext = tokens + 2 * HALO
    sems = [
        (fs_count, 2, 1 + across), (fs_count, 2), (reps,), (reps, tps), (reps, tps), (2, reps, tps), (2, reps, tps),
        (reps,), (reps,), (2, reps), (2, reps), (3,),
    ]
    vmem, hbm = pl.BlockSpec(memory_space=pltpu.VMEM), pl.BlockSpec(memory_space=pl.ANY)
    return pl.pallas_call(
        functools.partial(gather_kernel, (reps, fs_count, tps, across)),
        out_shape=(
            jax.ShapeDtypeStruct((reps, ext, feats * tps), x_own.dtype),
            jax.ShapeDtypeStruct((reps, ext, width), g_parts.dtype),
            jax.ShapeDtypeStruct((fs_count,) + w_own.shape, w_own.dtype),
        ),
        in_specs=[vmem] * 3,
        out_specs=(hbm,) * 3,
        scratch_shapes=[pltpu.SemaphoreType.DMA(s) for s in sems],
        compiler_params=pltpu.CompilerParams(has_side_effects=True),
        name="gather_all",
    )(x_own, g_parts, w_own)


def scatter_kernel(
    sizes, grads, pv, taps, own_all, in_grad, taps_all, y_got, z_got, tp_got, rep_got, taps_got,
    y_send, y_recv, z_send, z_recv, tp_send, tp_recv, rep_send, rep_recv, own_send, own_recv,
    taps_send, taps_recv, all_send, all_recv,
):
    reps, fs_count, tps, across = sizes
    deep = fs_count // across
    rep, fs, tp = (lax.axis_index(a) for a in ("rep", "fs", "tp"))
    z, y = fs // across, fs % across
    rows, width = grads.shape[1], grads.shape[2] // 2
    tokens, feats = in_grad.shape

    def other(axis_index, step, count):
        return (axis_index + step) % count

    def part(c):
        return pl.ds(c * width, width)

    def cols(index):
        return pl.ds(pl.multiple_of(index * feats, feats), feats)

    start = lambda c: c.start()
    sent = lambda c: c.wait_send()

    def landed(ref, sem):
        pltpu.make_async_copy(ref, ref, sem).wait()

    def tap_terms(sink):
        for step in range(1, fs_count):
            sink(remote(taps, taps_got.at[step], taps_send.at[step], taps_recv.at[step], fs=other(fs, step, fs_count)))

    def y_block(c, level, sink):
        for step in range(1, across):
            to = other(y, step, across)
            sink(remote(
                grads.at[level * across + to, :, part(c)], y_got.at[step, level, c],
                y_send.at[step, level, c], y_recv.at[step, level, c], fs=z * across + to,
            ))

    def far_first(visit):
        for dist in range(deep - 1, 0, -1):
            for way in range(2):
                @pl.when((z + dist < deep) if way == 0 else (z >= dist))
                def _():
                    visit(z + dist if way == 0 else z - dist, way)

    def y_sends(sink):
        for c in range(2):
            far_first(lambda level, way: y_block(c, level, sink))
            y_block(c, z, sink)

    def to_tps(sink):
        for slot in list(range(1, reps)) + [0]:
            for step in range(1, tps):
                to = other(tp, step, tps)
                sink(remote(
                    pv.at[slot, :, cols(to)], tp_got.at[slot, step], tp_send.at[slot, step], tp_recv.at[slot, step], tp=to
                ))

    def to_reps(sink):
        for slot in range(1, reps):
            sink(remote(
                rep_got.at[0, slot], rep_got.at[1, slot], rep_send.at[slot], rep_recv.at[slot],
                rep=other(rep, reps - slot, reps),
            ))

    def z_hop(c, level, way, sink):
        sink(remote(
            grads.at[level * across + y, :, part(c)], z_got.at[way, level, c],
            z_send.at[way, level, c], z_recv.at[way, level, c], fs=fs + across if way == 0 else fs - across,
        ))

    def own_rep(c, sink):
        mine = own_all.at[rep, :, part(c)]
        for step in range(1, reps):
            sink(remote(mine, mine, own_send.at[step, c], own_recv.at[step, c], rep=other(rep, step, reps)))

    def taps_out(sink):
        mine = taps_all.at[rep, tp]
        for slot in range(reps):
            for step in range(tps):
                if slot or step:
                    sink(remote(
                        mine, mine, all_send.at[slot, step], all_recv.at[slot, step],
                        rep=other(rep, slot, reps), tp=other(tp, step, tps),
                    ))

    tap_terms(start)
    to_tps(start)
    y_sends(start)

    for way in range(2):
        @pl.when((z == 0) if way == 0 else (z == deep - 1))
        def _():
            @pl.loop(0, deep)
            def _(level):
                for c in range(2):
                    @pl.loop(0, rows // 16)
                    def _(i):
                        z_got[way, level, c, pl.ds(pl.multiple_of(i * 16, 16), 16)] = jnp.zeros((16, width), z_got.dtype)

    def own_tps(slot, at):
        total = pv[slot, at, cols(tp)].astype(jnp.float32)
        for step in range(1, tps):
            total += tp_got[slot, step, at].astype(jnp.float32)
        return total

    for slot in range(1, reps):
        for step in range(1, tps):
            landed(tp_got.at[slot, step], tp_recv.at[slot, step])

        @pl.loop(0, tokens // 16)
        def _(i):
            at = pl.ds(pl.multiple_of(i * 16, 16), 16)
            rep_got[0, slot, at] = own_tps(slot, at).astype(rep_got.dtype)
    to_reps(start)

    def add_up(c, level, ways, store):
        for step in range(1, across):
            landed(y_got.at[step, level, c], y_recv.at[step, level, c])
        for way in ways:
            @pl.when((z > 0) if way == 0 else (z < deep - 1))
            def _():
                landed(z_got.at[way, level, c], z_recv.at[way, level, c])

        @pl.loop(0, rows // 16)
        def _(i):
            at = pl.ds(pl.multiple_of(i * 16, 16), 16)
            total = grads[level * across + y, at, part(c)].astype(jnp.float32)
            for step in range(1, across):
                total += y_got[step, level, c, at].astype(jnp.float32)
            for way in ways:
                total += z_got[way, level, c, at].astype(jnp.float32)
            store(at, total.astype(grads.dtype))

    def pass_on(c, level, way):
        def store(at, value):
            grads[level * across + y, at, part(c)] = value

        add_up(c, level, (way,), store)
        z_hop(c, level, way, start)

    for c in range(2):
        far_first(lambda level, way: pass_on(c, level, way))

        def store(at, value):
            own_all[rep, at, part(c)] = value

        add_up(c, z, (0, 1), store)
        own_rep(c, start)
        if c == 0:
            total = taps[...]
            for step in range(1, fs_count):
                landed(taps_got.at[step], taps_recv.at[step])
                total += taps_got[step]
            taps_all[rep, tp] = total
            taps_out(start)
            for step in range(1, tps):
                landed(tp_got.at[0, step], tp_recv.at[0, step])
            for slot in range(1, reps):
                landed(rep_got.at[1, slot], rep_recv.at[slot])

            @pl.loop(0, tokens // 16)
            def _(i):
                at = pl.ds(pl.multiple_of(i * 16, 16), 16)
                total = own_tps(0, at)
                for slot in range(1, reps):
                    total += rep_got[1, slot, at].astype(jnp.float32)
                in_grad[at] = total.astype(in_grad.dtype)

    for slot in range(reps):
        for step in range(tps):
            if slot or step:
                landed(taps_all.at[other(rep, reps - slot, reps), other(tp, tps - step, tps)], all_recv.at[slot, step])
    for step in range(1, reps):
        for c in range(2):
            landed(own_all.at[other(rep, reps - step, reps), :, part(c)], own_recv.at[step, c])
    tap_terms(sent)
    to_tps(sent)
    y_sends(sent)
    to_reps(sent)
    for c in range(2):
        far_first(lambda level, way: z_hop(c, level, way, sent))
        own_rep(c, sent)
    taps_out(sent)


def scatter_all(grads, pv, taps, across):
    reps, fs_count, tps = (lax.axis_size(a) for a in ("rep", "fs", "tp"))
    deep = fs_count // across
    rows, width = grads.shape[1], grads.shape[2] // 2
    tokens, feats = pv.shape[1], pv.shape[2] // tps
    sem = pltpu.SemaphoreType.DMA
    pairs = [
        (across, deep, 2), (2, deep, 2), (reps, tps), (reps,), (reps, 2), (fs_count,), (reps, tps),
    ]
    vmem = pl.BlockSpec(memory_space=pltpu.VMEM)
    return pl.pallas_call(
        functools.partial(scatter_kernel, (reps, fs_count, tps, across)),
        out_shape=(
            jax.ShapeDtypeStruct((reps, rows, 2 * width), grads.dtype),
            jax.ShapeDtypeStruct((tokens, feats), pv.dtype),
            jax.ShapeDtypeStruct((reps, tps) + taps.shape, taps.dtype),
        ),
        in_specs=[vmem] * 3,
        out_specs=(vmem,) * 3,
        scratch_shapes=[
            pltpu.VMEM((across, deep, 2, rows, width), grads.dtype),
            pltpu.VMEM((2, deep, 2, rows, width), grads.dtype),
            pltpu.VMEM((reps, tps, tokens, feats), pv.dtype),
            pltpu.VMEM((2, reps, tokens, feats), pv.dtype),
            pltpu.VMEM((fs_count,) + taps.shape, taps.dtype),
        ] + [sem(p) for p in pairs for _ in range(2)],
        compiler_params=pltpu.CompilerParams(has_side_effects=True, vmem_limit_bytes=58 * 1024 * 1024),
        name="scatter_all",
    )(grads, pv, taps)


def mix_kernel(fs_count, factor, pre, g, taps, pre_cot, terms):
    reps, ext, width = g.shape
    tokens = pre_cot.shape[1]
    fs = lax.axis_index("fs")
    row = lax.broadcasted_iota(jnp.int32, (ext, 128), 0)
    has_next, has_prev = (fs < fs_count - 1).astype(jnp.int32), (fs > 0).astype(jnp.int32)
    inside = (row < tokens) | ((row < tokens + HALO) & (has_next > 0)) | ((row >= tokens + HALO) & (has_prev > 0))

    def before(x):
        return pltpu.roll(x, 1, 0)

    def after(x):
        return pltpu.roll(x, ext - 1, 0)

    terms[...] = jnp.zeros_like(terms)

    @pl.loop(0, width // 128)
    def _(j):
        spots = [pl.ds(pl.multiple_of(branch * width + j * 128, 128), 128) for branch in range(2)]
        weights = [[taps[k : k + 1, at] for k in range(3)] for at in spots]
        for slot in range(reps):
            pres = [jnp.where(inside, pre[slot, :, at].astype(jnp.float32), 0.0) for at in spots]
            around = [(before(p), p, after(p)) for p in pres]
            gate_mix, value_mix = [sum(w * p for w, p in zip(ws, ps)) for ws, ps in zip(weights, around)]
            cot_in = jnp.where(inside, g[slot, :, spots[0]].astype(jnp.float32), 0.0)
            sig = jax.nn.sigmoid(gate_mix)
            cots = (
                cot_in * value_mix * (sig * (1.0 + gate_mix * (1.0 - sig))),
                cot_in * (gate_mix * sig),
            )
            for at, ws, ps, cot in zip(spots, weights, around, cots):
                back = ws[0] * after(cot) + ws[1] * cot + ws[2] * before(cot)
                pre_cot[slot, :, at] = back[:tokens].astype(pre_cot.dtype)
                for k in range(3):
                    total = jnp.sum(ps[k][:tokens] * cot[:tokens], axis=0, keepdims=True)
                    terms[k : k + 1, at] += total * factor


def mix_all(pre, g, taps, tokens, fs_count, factor):
    reps, ext, both = pre.shape
    vmem = pl.BlockSpec(memory_space=pltpu.VMEM)
    return pl.pallas_call(
        functools.partial(mix_kernel, fs_count, factor),
        out_shape=(
            jax.ShapeDtypeStruct((reps, tokens, both), pre.dtype),
            jax.ShapeDtypeStruct((8, both), jnp.float32),
        ),
        in_specs=[vmem] * 3,
        out_specs=(vmem,) * 2,
        compiler_params=pltpu.CompilerParams(vmem_limit_bytes=40000 * 1024),
        name="mix_all",
    )(pre, g, taps)


LANES = 128
EDGE = 16


def part_width(hid, parts):
    return min(hid, -(-hid // parts // LANES) * LANES)


TUNED = (
    ("weights_y", 0), ("weights_y", 1), ("tokens_x", 0), ("own", 2), ("own", 0), ("tokens_y", 1), ("near", 0),
    ("tokens_x", 2), ("relay", 0, 1, False), ("relay", 0, 1, True), ("tokens_y", 0), ("tokens_x", 1), ("near", 1),
    ("weights_y", 2), ("edge_out", 0), ("relay", 0, 2, False), ("edge_out", 1), ("take", 1, 0, 2), ("take", 0, 1, 1),
    ("relay", 0, 2, True), ("relay", 2, 1, False), ("own", 1), ("take", 0, 1, 0), ("edge_share", 0),
    ("edge_share", 1), ("tokens_y", 2), ("relay", 1, 1, False), ("take", 1, 1, 1), ("relay", 1, 1, True), ("near", 2),
    ("last", 0), ("take", 1, 0, 0), ("relay", 1, 2, False), ("cots", 0), ("take", 1, 0, 1), ("edge_pass", 0),
    ("edge_pass", 1), ("tokens_core",), ("take", 1, 1, 2), ("take", 1, 1, 0), ("take", 0, 1, 2), ("take_rest",),
    ("project", 0), ("mix", 0), ("relay", 1, 2, True), ("relay", 2, 1, True), ("cots", 1), ("weight", 0), ("last", 1),
    ("relay", 2, 2, False), ("project", 1), ("pass_on", 0, 2), ("relay", 2, 2, True), ("cots", 2), ("mix", 1),
    ("weight", 1), ("pass_on", 0, 1), ("last", 2), ("project", 2), ("mix", 2), ("input", 0), ("finish", 0),
    ("first", 0), ("input", 2), ("pass_on", 1, 2), ("weight", 2), ("owners", 0), ("first", 2), ("input", 1),
    ("taps",), ("pass_on", 1, 1), ("first", 1), ("second", 1), ("pass_on", 2, 2), ("finish", 1), ("second", 0),
    ("pass_on", 2, 1), ("owners", 1), ("input", 3), ("finish", 2), ("taps_sum",), ("owners", 2),
)


def plan(chunks, deep):
    return TUNED if (chunks, deep) == (3, 4) else general_plan(chunks, deep)


def general_plan(chunks, deep):
    yield "weights_y", 0
    yield "tokens_y", 0
    for c in range(1, chunks):
        yield "weights_y", c
        if c < 3:
            yield "tokens_y", c
    for k in range(min(chunks, 3), 3):
        yield "tokens_y", k
    for k in (2, 0, 1):
        yield "tokens_x", k
    for side in range(2):
        yield "edge_out", side
    yield ("tokens_core",)
    for c in range(chunks):
        yield "own", c
    yield "near", 0
    yield "relay", 0, 1, False
    for side in range(2):
        yield "edge_share", side
    yield "take", 1, 0, 2
    for c in range(1, chunks):
        yield "relay", c, 1, False
    yield "take", 0, 1, 0
    yield "relay", 0, 1, True
    for c in range(1, min(chunks, 2)):
        yield "near", c
    for dist in range(2, deep):
        yield "relay", 0, dist, False
        yield "relay", 0, dist, True
    for side in range(2):
        yield "edge_pass", side
    yield "take", 0, 1, 1
    for c in range(chunks):
        yield "cots", c
    for k in (0, 1):
        yield "take", 1, 0, k
    for c in range(2, chunks):
        yield "near", c
    for c in range(1, min(chunks, 2)):
        yield "relay", c, 1, True
        for dist in range(2, deep):
            yield "relay", c, dist, False
    yield "take", 1, 1, 0
    yield "take", 0, 1, 2
    for k in (1, 2):
        yield "take", 1, 1, k
    yield ("take_rest",)
    yield "last", 0
    yield "project", 0
    for c in range(1, chunks):
        for dist in range(1, deep):
            if c > 1 and dist > 1:
                yield "relay", c, dist, False
            if c > 1 or dist > 1:
                yield "relay", c, dist, True
    for c in range(chunks):
        if c:
            yield "last", c
            yield "project", c
        yield "mix", c
        if c < max(chunks - 1, 1):
            yield "weight", c
        if c == chunks - 2:
            for early in range(chunks - 2):
                for dist in range(deep - 1, 0, -1):
                    yield "pass_on", early, dist
    yield ("taps",)
    yield "input", 0
    yield "input", 1
    yield "first", 0
    yield "input", 2
    yield "first", 1
    yield "input", 3
    yield "first", 2
    if chunks > 1:
        yield "weight", chunks - 1
    for c in range(chunks):
        if c >= chunks - 2:
            for dist in range(deep - 1, 0, -1):
                yield "pass_on", c, dist
        if c == max(chunks - 2, 0):
            for f in range(2):
                yield "second", f
            yield ("taps_sum",)
        yield "finish", c
        yield "owners", c


def fused_kernel(
    sizes, factor, x_own, gate_w, value_w, gate_taps, value_taps, g_own,
    in_grad, gate_out, value_out, gate_taps_out, value_taps_out,
    taps_mine, x_all, w_all, g_all, pre, cot, grads, from_z, fin, pv, from_tp, first_got, second_got, terms, terms_z, terms_all,
    own_sem, wy_send, wy_recv, wz_send, wz_recv, x_send, xf_send, xs_send, x_recv, hz_send, hb_send, hs_send, hx_recv,
    g_send, g_recv, hg_send, hg_recv, sz_send, sz_recv, out_send, out_recv, tp_send, tp_recv,
    s1_send, s1_recv, s2_send, s2_recv, tz_send, tz_recv, ta_send, ta_recv,
):
    deep, across, width = sizes
    rep, fs, tp = (lax.axis_index(a) for a in ("rep", "fs", "tp"))
    z, y = fs // across, fs % across
    nrep, ny, ntp = 1 - rep, 1 - y, 1 - tp
    tokens, feats = x_own.shape
    rows, hid = gate_w.shape
    main = across * tokens
    ext = main + 2 * EDGE
    chunks = width // LANES
    both = 2 * LANES
    blocks = feats // rows
    first_feats = feats * 3 // 8 // LANES * LANES
    spans = ((0, first_feats), (first_feats, feats - first_feats))
    cuts = [tokens * k // 16 // 16 * 16 for k in (0, 6, 12, 16)]
    pieces = tuple((low, high - low) for low, high in zip(cuts, cuts[1:]))
    last = len(pieces) - 1
    weights = (gate_w, value_w)
    outs = (gate_out, value_out)
    others = [(dr, dy) for dr in range(2) for dy in range(2) if dr or dy]

    start = lambda c: c.start()
    sent = lambda c: c.wait_send()

    def landed(ref, sem):
        pltpu.make_async_copy(ref, ref, sem).wait()

    def moved(index, step):
        return (index + step) % 2

    def part_of(r, yy):
        return r * across + yy

    part = part_of(rep, y)

    def first_col(which):
        return jnp.minimum(which * width, hid - width)

    def live(which, c):
        return c * LANES >= which * width - first_col(which)

    def chunk_cols(which, c):
        return pl.ds(pl.multiple_of(first_col(which) + c * LANES, LANES), LANES)

    def all_cols(which):
        return pl.ds(pl.multiple_of(first_col(which), LANES), width)

    def cols(half):
        return pl.ds(pl.multiple_of(half * feats, feats), feats)

    def token_rows(yy):
        return pl.ds(pl.multiple_of(yy * tokens, 16), tokens)

    def lanes(branch):
        return pl.ds(branch * LANES, LANES)

    def near(side):
        return pl.ds(0, EDGE) if side == 0 else pl.ds(tokens - EDGE, EDGE)

    def far(side):
        return pl.ds(main + side * EDGE, EDGE)

    def gives_edge(side):
        return (y == 0) & (z > 0) if side == 0 else (y == across - 1) & (z < deep - 1)

    def has_edge(side):
        return z < deep - 1 if side == 0 else z > 0

    def takes_edge(side):
        return (y == 0) & (z < deep - 1) if side == 0 else (y == across - 1) & (z > 0)

    def greet():
        barrier = pltpu.get_barrier_semaphore()

        def hello(**device):
            pl.semaphore_signal(barrier, 1, device_id=device, device_id_type=pl.DeviceIdType.MESH)

        for dr in range(2):
            for dy in range(2):
                for dt in range(2):
                    if dr or dy or dt:
                        hello(rep=moved(rep, dr), fs=z * across + moved(y, dy), tp=moved(tp, dt))
        for step_z in range(1, deep):
            hello(fs=(z + step_z) % deep * across + y)
        for up in (True, False):
            @pl.when(z < deep - 1 if up else z > 0)
            def _():
                for dr, dy in others:
                    hello(rep=moved(rep, dr), fs=(z + 1 if up else z - 1) * across + moved(y, dy))
        next_levels = (z > 0).astype(jnp.int32) + (z < deep - 1).astype(jnp.int32)
        pl.semaphore_wait(barrier, 6 + deep + len(others) * next_levels)

    def w_across(c, sink):
        for branch, w in enumerate(weights):
            sink(remote(
                w.at[:, chunk_cols(part_of(rep, ny), c)], w_all.at[c, fs, :, lanes(branch)],
                wy_send.at[c, branch], wy_recv.at[c, branch], fs=z * across + ny,
            ))

    def w_along(c, block, up, down, sink):
        ref = w_all.at[c, block]
        if up:
            @pl.when(z < deep - 1)
            def _():
                sink(remote(ref, ref, wz_send.at[c, block, 0], wz_recv.at[c, block], fs=fs + across))
        if down:
            @pl.when(z > 0)
            def _():
                sink(remote(ref, ref, wz_send.at[c, block, 1], wz_recv.at[c, block], fs=fs - across))

    def w_local(c):
        return [
            pltpu.make_async_copy(
                w.at[:, chunk_cols(part, c)], w_all.at[c, fs, :, lanes(branch)], own_sem.at[2 * c + branch]
            ) for branch, w in enumerate(weights)
        ]

    def w_own_along(c, sink):
        w_along(c, fs, True, True, sink)

    def w_near_along(c, arrive, sink):
        block = z * across + ny
        if arrive:
            for branch in range(2):
                landed(w_all.at[c, block, :, lanes(branch)], wy_recv.at[c, branch])
        w_along(c, block, True, True, sink)

    def w_step(c, dist, near_block, forward, visit):
        for sign in (-1, 1):
            here = (z >= dist) if sign < 0 else (z + dist < deep)
            goes_on = (z < deep - 1) if sign < 0 else (z > 0)

            @pl.when(here & (goes_on if forward else jnp.logical_not(goes_on)))
            def _():
                visit((z + sign * dist) * across + (ny if near_block else y), sign)

    def w_relay(c, dist, near_block, sink=start):
        def visit(block, sign):
            if sink is start:
                landed(w_all.at[c, block], wz_recv.at[c, block])
            w_along(c, block, sign < 0, sign > 0, sink)

        w_step(c, dist, near_block, True, visit)

    def w_last(c):
        for dist in range(1, deep):
            for near_block in (False, True):
                w_step(
                    c, dist, near_block, False,
                    lambda block, sign: landed(w_all.at[c, block], wz_recv.at[c, block]),
                )

    def x_at(r, yy, k, half):
        offset, size = pieces[k]
        return x_all.at[r, pl.ds(pl.multiple_of(yy * tokens + offset, 16), size), cols(half)]

    def x_mine(k):
        return x_own.at[pl.ds(*pieces[k])]

    def x_across(k, sink):
        sink(remote(x_mine(k), x_at(rep, y, k, tp), x_send.at[1, k], x_recv.at[rep, y, k, tp], fs=z * across + ny))

    def x_over(k, sink):
        sink(remote(x_mine(k), x_at(rep, y, k, tp), x_send.at[0, k], x_recv.at[rep, y, k, tp], rep=nrep))

    def x_to_sibling(sink):
        for k in range(len(pieces)):
            sink(remote(x_mine(k), x_at(rep, y, k, tp), xs_send.at[rep, y, k], x_recv.at[rep, y, k, tp], tp=ntp))

    def x_forward(k, sink):
        if k < last:
            ref = x_at(rep, ny, k, tp)
            sink(remote(ref, ref, xf_send.at[k], x_recv.at[rep, ny, k, tp], rep=nrep))
        else:
            ref = x_at(nrep, y, k, tp)
            sink(remote(ref, ref, xf_send.at[k], x_recv.at[nrep, y, k, tp], fs=z * across + ny))

    def x_take(r, yy, k, forward):
        x_landed(r, yy, k, tp)
        if forward:
            x_forward(k, start)
        x_share(r, yy, k, start)

    def x_share(r, yy, k, sink):
        ref = x_at(r, yy, k, tp)
        sink(remote(ref, ref, xs_send.at[r, yy, k], x_recv.at[r, yy, k, tp], tp=ntp))

    def x_landed(r, yy, k, half):
        landed(x_at(r, yy, k, half), x_recv.at[r, yy, k, half])

    def edge_out(side, sink):
        target = fs - across if side == 0 else fs + across

        @pl.when(gives_edge(side))
        def _():
            sink(remote(
                x_own.at[near(side)], x_all.at[rep, far(side), cols(tp)], hz_send.at[side],
                hx_recv.at[side, rep, tp], fs=target,
            ))
            level = z - 1 if side == 0 else z + 1
            for dr in range(2):
                for dy in range(2):
                    r, yy = moved(rep, dr), moved(y, dy)
                    sink(remote(
                        g_own.at[near(side), all_cols(part_of(r, yy))], g_all.at[rep, far(side)],
                        hg_send.at[side, dr, dy], hg_recv.at[side, rep], rep=r, fs=level * across + yy,
                    ))

    def edge_at(side, r, half):
        return x_all.at[r, far(side), cols(half)]

    def edge_share(side, sink=start):
        @pl.when(takes_edge(side))
        def _():
            ref = edge_at(side, rep, tp)
            if sink is start:
                landed(ref, hx_recv.at[side, rep, tp])
            for dr, dy in others:
                sink(remote(
                    ref, ref, hb_send.at[side, dr, dy], hx_recv.at[side, rep, tp],
                    rep=moved(rep, dr), fs=z * across + moved(y, dy),
                ))
            sink(remote(ref, ref, hs_send.at[side, rep], hx_recv.at[side, rep, tp], tp=ntp))

    def edge_pass(side, sink=start):
        for r in (rep, nrep):
            @pl.when(has_edge(side) & jnp.logical_not(takes_edge(side) & (r == rep)))
            def _():
                ref = edge_at(side, r, tp)
                if sink is start:
                    landed(ref, hx_recv.at[side, r, tp])
                sink(remote(ref, ref, hs_send.at[side, r], hx_recv.at[side, r, tp], tp=ntp))

    def edge_landed(side):
        @pl.when(has_edge(side))
        def _():
            for r in range(2):
                landed(edge_at(side, r, ntp), hx_recv.at[side, r, ntp])
                landed(g_all.at[r, far(side)], hg_recv.at[side, r])

    def g_direct(c, sink):
        for dr, dy in others:
            r, yy = moved(rep, dr), moved(y, dy)
            sink(remote(
                g_own.at[:, chunk_cols(part_of(r, yy), c)], g_all.at[rep, token_rows(y), pl.ds(c * LANES, LANES)],
                g_send.at[c, dr, dy], g_recv.at[c, rep, y], rep=r, fs=z * across + yy,
            ))

    def g_landed(c):
        for dr, dy in others:
            r, yy = moved(rep, dr), moved(y, dy)
            landed(g_all.at[r, token_rows(yy), pl.ds(c * LANES, LANES)], g_recv.at[c, r, yy])

    x_local = pltpu.make_async_copy(
        x_own, x_all.at[rep, token_rows(y), cols(tp)], own_sem.at[2 * chunks]
    )
    g_local = pltpu.make_async_copy(
        g_own.at[:, all_cols(part)], g_all.at[rep, token_rows(y)], own_sem.at[2 * chunks + 1]
    )

    tap_cols = pl.ds(pl.multiple_of(tp * hid + first_col(part), LANES), width)
    taps_local = [
        pltpu.make_async_copy(ref.at[:, tap_cols], taps_mine.at[b], own_sem.at[2 * chunks + 2 + b])
        for b, ref in enumerate((gate_taps, value_taps))
    ]

    def chunk_lanes(c):
        return pl.ds(c * both, both)

    def project(c):
        @pl.loop(0, 2)
        def _(slot):
            total = jnp.dot(
                x_all[slot], w_all[c].reshape(-1, both), preferred_element_type=jnp.float32
            )
            pre[slot] = total.astype(pre.dtype)

    def mix(c):
        row = lax.broadcasted_iota(jnp.int32, (ext, LANES), 0)
        has_next, has_prev = (z < deep - 1).astype(jnp.int32), (z > 0).astype(jnp.int32)
        inside = (row < main) | ((row < main + EDGE) & (has_next > 0)) | ((row >= main + EDGE) & (has_prev > 0))
        counted = inside & (live(part, c).astype(jnp.int32) > 0)
        taps = [[taps_mine[b, k : k + 1, pl.ds(c * LANES, LANES)] for k in range(3)] for b in range(2)]
        terms[:, pl.ds(c * LANES, LANES)] = jnp.zeros((8, LANES), jnp.float32)

        def before(v):
            return pltpu.roll(v, 1, 0)

        def after(v):
            return pltpu.roll(v, ext - 1, 0)

        @pl.loop(0, 2)
        def _(slot):
            pres = [jnp.where(inside, pre[slot, :, lanes(b)].astype(jnp.float32), 0.0) for b in range(2)]
            around = [(before(p), p, after(p)) for p in pres]
            gate_mix, value_mix = [sum(w * p for w, p in zip(ws, ps)) for ws, ps in zip(taps, around)]
            cot_in = jnp.where(counted, g_all[slot, :, pl.ds(c * LANES, LANES)].astype(jnp.float32), 0.0)
            sig = jax.nn.sigmoid(gate_mix)
            cots = (
                cot_in * value_mix * (sig * (1.0 + gate_mix * (1.0 - sig))),
                cot_in * (gate_mix * sig),
            )
            for b in range(2):
                ws, ps, one = taps[b], around[b], cots[b]
                back = ws[0] * after(one) + ws[1] * one + ws[2] * before(one)
                cot[slot, :, pl.ds(c * both + b * LANES, LANES)] = back[:main].astype(cot.dtype)
                for k in range(3):
                    total = jnp.sum(ps[k][:main] * one[:main], axis=0, keepdims=True)
                    terms[2 * k + b : 2 * k + b + 1, pl.ds(c * LANES, LANES)] += total * factor

    def far_first(visit):
        @pl.loop(0, 2 * deep - 1)
        def _(i):
            dist = deep - 1 - i // 2
            level = jnp.where(i % 2 == 0, z + dist, z - dist)

            @pl.when((level >= 0) & (level < deep))
            def _():
                visit(level)

    def sum_hop(c, block, up, sink):
        way = 0 if up else 1
        sink(remote(
            grads.at[c, block], from_z.at[way, c, block], sz_send.at[c, block], sz_recv.at[way, c, block],
            fs=fs + across if up else fs - across,
        ))

    def weight_terms(c):
        def visit(level):
            for yy in (ny, y):
                block = level * across + yy
                at = pl.ds(pl.multiple_of(block * rows, rows), rows)
                total = sum(
                    lax.dot_general(
                        x_all[slot, :main, at], cot[slot, :, chunk_lanes(c)], (((0,), (0,)), ((), ())),
                        preferred_element_type=jnp.float32,
                    ) for slot in range(2)
                )
                grads[c, block] = (total * factor).astype(grads.dtype)
            for up in (True, False):
                @pl.when((level > z) & (z == 0) if up else (level < z) & (z == deep - 1))
                def _():
                    for yy in (ny, y):
                        sum_hop(c, level * across + yy, up, start)

        far_first(visit)

    def pass_on(c, dist):
        for up in (True, False):
            level = z + dist if up else z - dist

            @pl.when((z > 0) & (z < deep - 1) & ((level < deep) if up else (level >= 0)))
            def _():
                way = 0 if up else 1
                for yy in (ny, y):
                    block = level * across + yy
                    landed(from_z.at[way, c, block], sz_recv.at[way, c, block])
                    total = grads[c, block].astype(jnp.float32) + from_z[way, c, block].astype(jnp.float32)
                    grads[c, block] = total.astype(grads.dtype)
                    sum_hop(c, block, up, start)

    def sums_sent(c):
        def visit(level):
            for up in (True, False):
                @pl.when((level > z) if up else (level < z))
                def _():
                    for yy in range(across):
                        sum_hop(c, level * across + yy, up, sent)

        far_first(visit)

    def to_owners(c, same, sink):
        here = chunk_cols(part, c)
        for branch, out in enumerate(outs):
            sems = out_send.at[c, branch, 0 if same else 1], out_recv.at[c, branch, rep, y]
            if same:
                sink(remote(out.at[:, here], out.at[:, here], *sems, rep=nrep))
            else:
                sink(remote(fin.at[c, :, lanes(branch)], out.at[:, here], *sems, fs=z * across + ny))

    def owners_pass(c, sink=start):
        source = part_of(rep, ny)

        @pl.when(live(source, c))
        def _():
            for branch, out in enumerate(outs):
                ref, sem = out.at[:, chunk_cols(source, c)], out_recv.at[c, branch, rep, ny]
                if sink is start:
                    landed(ref, sem)
                sink(remote(ref, ref, out_send.at[c, branch, 2], sem, rep=nrep))

    def owners_last(c):
        for yy in (y, ny):
            source = part_of(nrep, yy)

            @pl.when(live(source, c))
            def _():
                for branch, out in enumerate(outs):
                    landed(out.at[:, chunk_cols(source, c)], out_recv.at[c, branch, nrep, yy])

    def finish(c):
        for same in (False, True):
            block = z * across + (y if same else ny)
            for way in range(2):
                @pl.when(z > 0 if way == 0 else z < deep - 1)
                def _():
                    landed(from_z.at[way, c, block], sz_recv.at[way, c, block])
            total = grads[c, block].astype(jnp.float32)
            for way in range(2):
                total += from_z[way, c, block].astype(jnp.float32)
            total = total.astype(grads.dtype)

            @pl.when(live(part, c))
            def _():
                if same:
                    for branch, out in enumerate(outs):
                        out[:, chunk_cols(part, c)] = total[:, branch * LANES : (branch + 1) * LANES]
                else:
                    fin[c] = total
                to_owners(c, same, start)

    def input_terms(dr, dy):
        r, yy = moved(rep, dr), moved(y, dy)
        q = part_of(r, yy)

        def terms_of(half):
            @pl.loop(0, blocks)
            def _(j):
                total = sum(
                    lax.dot_general(
                        cot[r, token_rows(yy), chunk_lanes(c)], w_all[c, half * blocks + j],
                        (((1,), (1,)), ((), ())), preferred_element_type=jnp.float32,
                    ) for c in range(chunks)
                )
                pv[half, q, :, pl.ds(pl.multiple_of(j * rows, rows), rows)] = total.astype(pv.dtype)

        terms_of(ntp)
        tp_hop(q, start)
        terms_of(tp)

    def tp_hop(q, sink):
        sink(remote(pv.at[ntp, q], from_tp.at[q], tp_send.at[q], tp_recv.at[q], tp=ntp))

    def f_cols(f):
        return pl.ds(*spans[f])

    def first_hop(f, k, sink):
        q = part_of(nrep, ny) if k else part_of(nrep, y) if f == 0 else part_of(rep, ny)
        target = dict(rep=nrep) if f == 0 else dict(fs=z * across + ny)
        sink(remote(pv.at[tp, q, :, f_cols(f)], first_got.at[f, k, :, pl.ds(0, spans[f][1])], s1_send.at[f, k], s1_recv.at[f, k], **target))

    def second_hop(f, sink):
        q = part_of(rep, ny) if f == 0 else part_of(nrep, y)
        target = dict(fs=z * across + ny) if f == 0 else dict(rep=nrep)
        sink(remote(pv.at[tp, q, :, f_cols(f)], second_got.at[f, :, pl.ds(0, spans[f][1])], s2_send.at[f], s2_recv.at[f], **target))

    def row_tiles(body):
        @pl.loop(0, tokens // 16)
        def _(i):
            body(pl.ds(pl.multiple_of(i * 16, 16), 16))

    def add_sibling(q):
        landed(from_tp.at[q], tp_recv.at[q])

        def body(at):
            total = pv[tp, q, at].astype(jnp.float32) + from_tp[q, at].astype(jnp.float32)
            pv[tp, q, at] = total.astype(pv.dtype)

        row_tiles(body)

    def input_first(dr, dy):
        add_sibling(part_of(moved(rep, dr), moved(y, dy)))
        if dr:
            first_hop(0, dy, start)
        if dy:
            first_hop(1, dr, start)

    def input_second(f):
        q = part_of(rep, ny) if f == 0 else part_of(nrep, y)
        landed(first_got.at[f, 1, :, pl.ds(0, spans[f][1])], s1_recv.at[f, 1])

        def body(at):
            total = pv[tp, q, at, f_cols(f)].astype(jnp.float32)
            total += first_got[f, 1, at, : spans[f][1]].astype(jnp.float32)
            pv[tp, q, at, f_cols(f)] = total.astype(pv.dtype)

        row_tiles(body)
        second_hop(f, start)

    def input_last():
        landed(from_tp.at[part], tp_recv.at[part])
        for f in range(2):
            landed(first_got.at[f, 0, :, pl.ds(0, spans[f][1])], s1_recv.at[f, 0])
            landed(second_got.at[f, :, pl.ds(0, spans[f][1])], s2_recv.at[f])

        def body(at):
            for f in range(2):
                total = pv[tp, part, at, f_cols(f)].astype(jnp.float32) + from_tp[part, at, f_cols(f)].astype(jnp.float32)
                total += first_got[f, 0, at, : spans[f][1]].astype(jnp.float32) + second_got[f, at, : spans[f][1]].astype(jnp.float32)
                in_grad[at, f_cols(f)] = total.astype(in_grad.dtype)

        row_tiles(body)

    def taps_along(sink):
        for step in range(1, deep):
            to = (z + step) % deep
            sink(remote(
                terms_z.at[z], terms_z.at[z], tz_send.at[step], tz_recv.at[z], fs=to * across + y
            ))

    def taps_start():
        terms_z[z] = terms[...]
        taps_along(start)

    def taps_out(sink):
        ref = terms_all.at[rep, y, tp]
        for dr in range(2):
            for dy in range(2):
                for dt in range(2):
                    if dr or dy or dt:
                        sink(remote(
                            ref, ref, ta_send.at[dr, dy, dt], ta_recv.at[rep, y, tp],
                            rep=moved(rep, dr), fs=z * across + moved(y, dy), tp=moved(tp, dt),
                        ))

    def taps_sum():
        for step in range(1, deep):
            source = (z + step) % deep
            landed(terms_z.at[source], tz_recv.at[source])
        terms_all[rep, y, tp] = sum(terms_z[level] for level in range(deep))
        taps_out(start)

    def taps_last():
        for dr in range(2):
            for dy in range(2):
                for dt in range(2):
                    if dr or dy or dt:
                        at = (moved(rep, dr), moved(y, dy), moved(tp, dt))
                        landed(terms_all.at[at], ta_recv.at[at])
        for r in range(2):
            for yy in range(across):
                which = r * across + yy
                first = min(which * width, hid - width)
                skip = which * width - first
                for half in range(2):
                    for branch, out in enumerate((gate_taps_out, value_taps_out)):
                        for k in range(3):
                            if skip < width:
                                begin = half * hid + first + skip
                                out[k : k + 1, begin : begin + width - skip] = terms_all[
                                    r, yy, half, 2 * k + branch : 2 * k + branch + 1, skip:
                                ]

    for c in range(chunks):
        for copy in w_local(c):
            copy.start()
    x_local.start()
    g_local.start()
    for copy in taps_local:
        copy.start()
    for way in range(2):
        @pl.when((z == 0) if way == 0 else (z == deep - 1))
        def _():
            for c in range(chunks):
                for yy in range(across):
                    from_z[way, c, z * across + yy] = jnp.zeros((rows, both), from_z.dtype)
    greet()

    def w_own(c):
        for copy in w_local(c):
            copy.wait()
        w_own_along(c, start)

    def take(dr, dy, k):
        x_take(moved(rep, dr), moved(y, dy), k, (not dr) if k < last else (not dy))

    def take_rest():
        x_local.wait()
        g_local.wait()
        for copy in taps_local:
            copy.wait()
        for r in range(2):
            for yy in range(across):
                for k in range(len(pieces)):
                    x_landed(r, yy, k, ntp)
        for side in range(2):
            edge_landed(side)

    def mix_chunk(c):
        g_landed(c)
        mix(c)

    offsets = ((1, 1), (0, 1), (1, 0), (0, 0))
    actions = dict(
        weights_y=lambda c: w_across(c, start),
        tokens_y=lambda k: x_across(k, start),
        tokens_x=lambda k: x_over(k, start),
        tokens_core=lambda: x_to_sibling(start),
        edge_out=lambda side: edge_out(side, start),
        own=w_own,
        near=lambda c: w_near_along(c, True, start),
        relay=w_relay,
        edge_share=edge_share,
        edge_pass=edge_pass,
        take=take,
        cots=lambda c: g_direct(c, start),
        take_rest=take_rest,
        last=w_last,
        project=project,
        mix=mix_chunk,
        weight=weight_terms,
        pass_on=pass_on,
        finish=finish,
        owners=owners_pass,
        taps=taps_start,
        taps_sum=taps_sum,
        input=lambda i: input_terms(*offsets[i]),
        first=lambda i: input_first(*offsets[i]),
        second=input_second,
    )
    for name, *args in plan(chunks, deep):
        actions[name](*args)
    for side in range(2):
        edge_out(side, sent)
        edge_share(side, sent)
        edge_pass(side, sent)
    x_to_sibling(sent)
    for k in range(len(pieces)):
        x_across(k, sent)
        x_over(k, sent)
        x_forward(k, sent)
        for dr, dy in others:
            x_share(moved(rep, dr), moved(y, dy), k, sent)
    for c in range(chunks):
        w_across(c, sent)
        w_own_along(c, sent)
        w_near_along(c, False, sent)
        for dist in range(1, deep):
            for near_block in (False, True):
                w_relay(c, dist, near_block, sent)
        g_direct(c, sent)
    input_last()
    taps_last()
    for c in range(chunks):
        owners_last(c)
    for c in range(chunks):
        sums_sent(c)

        @pl.when(live(part, c))
        def _():
            for same in (False, True):
                to_owners(c, same, sent)

        owners_pass(c, sent)
    for dr in range(2):
        for dy in range(2):
            tp_hop(part_of(moved(rep, dr), moved(y, dy)), sent)
    for f in range(2):
        for k in range(2):
            first_hop(f, k, sent)
        second_hop(f, sent)
    taps_along(sent)
    taps_out(sent)


def fused_all(across, x_own, gate_w, value_w, gate_taps, value_taps, g_own):
    reps, fs_count, tps = (lax.axis_size(a) for a in ("rep", "fs", "tp"))
    deep = fs_count // across
    tokens, feats = x_own.shape
    rows, hid = gate_w.shape
    width = part_width(hid, reps * across)
    chunks = width // LANES
    both = 2 * LANES
    main = across * tokens
    ext = main + 2 * EDGE
    parts = reps * across
    factor = float(tokens * fs_count * reps) ** (-0.5)
    dtype = x_own.dtype
    f32 = jnp.float32
    sem = pltpu.SemaphoreType.DMA
    sems = [
        (2 * chunks + 4,), (chunks, 2), (chunks, 2), (chunks, fs_count, 2), (chunks, fs_count), (2, 3), (3,),
        (reps, across, 3), (reps, across, 3, tps), (2,), (2, 2, 2), (2, reps), (2, reps, tps),
        (chunks, 2, 2), (chunks, reps, across), (2, 2, 2), (2, reps), (chunks, fs_count), (2, chunks, fs_count),
        (chunks, 2, 3), (chunks, 2, reps, across), (parts,), (parts,),
        (2, 2), (2, 2), (2,), (2,), (deep,), (deep,), (2, 2, 2), (reps, across, tps),
    ]
    buffers = [
        ((2, 3, width), f32), ((reps, ext, tps * feats), dtype), ((chunks, fs_count, rows, both), dtype), ((reps, ext, width), dtype),
        ((reps, ext, both), dtype), ((reps, main, 2 * width), dtype), ((chunks, fs_count, rows, both), dtype),
        ((2, chunks, fs_count, rows, both), dtype), ((chunks, rows, both), dtype),
        ((tps, parts, tokens, feats), dtype), ((parts, tokens, feats), dtype),
        ((2, 2, tokens, feats), dtype), ((2, tokens, feats), dtype),
        ((8, width), f32), ((deep, 8, width), f32), ((reps, across, tps, 8, width), f32),
    ]
    vmem, hbm = pl.BlockSpec(memory_space=pltpu.VMEM), pl.BlockSpec(memory_space=pl.ANY)
    return pl.pallas_call(
        functools.partial(fused_kernel, (deep, across, width), factor),
        out_shape=(
            jax.ShapeDtypeStruct((tokens, feats), dtype),
            jax.ShapeDtypeStruct((rows, hid), dtype),
            jax.ShapeDtypeStruct((rows, hid), dtype),
            jax.ShapeDtypeStruct(gate_taps.shape, f32),
            jax.ShapeDtypeStruct(value_taps.shape, f32),
        ),
        in_specs=[hbm] * 6,
        out_specs=(vmem,) * 5,
        scratch_shapes=[pltpu.VMEM(*b) for b in buffers] + [sem(s) for s in sems],
        compiler_params=pltpu.CompilerParams(has_side_effects=True, collective_id=0, vmem_limit_bytes=60 * 1024 * 1024),
        name="fused_all",
    )(x_own, gate_w, value_w, gate_taps, value_taps, g_own)


def store_kernel(in_grad, gate, value, gate_taps, value_taps, *refs):
    outs, held, (gate_wide, value_wide, load_sem, sem) = refs[:5], refs[5:10], refs[10:]
    sources = (in_grad, gate, value, gate_taps, value_taps)
    count = load_sem.shape[1]

    def split(k):
        rows = sources[k].shape[0]
        size = rows // count
        return [pl.ds(p * size, size) for p in range(count)] if size % 16 == 0 and size * count == rows else [pl.ds(0, rows)]

    tasks = [(k, p, at) for k in (1, 2, 0, 3, 4) for p, at in enumerate(split(k))]
    loads = [pltpu.make_async_copy(sources[k].at[at], held[k].at[at], load_sem.at[k, p]) for k, p, at in tasks]
    for load in loads:
        load.start()
    stores = []
    for (k, p, at), load in zip(tasks, loads):
        load.wait()
        src = {1: gate_wide, 2: value_wide}.get(k, held[k])
        if k in (1, 2):
            src[at] = held[k][at].astype(src.dtype)
        stores.append(pltpu.make_async_copy(src.at[at], outs[k].at[at], sem.at[k, p]))
        stores[-1].start()
    for store in stores:
        store.wait()


def store_all(*arrays):
    hbm = pl.BlockSpec(memory_space=pl.ANY)
    wide = jax.ShapeDtypeStruct(arrays[1].shape, jnp.float32)
    outs = [jax.ShapeDtypeStruct(a.shape, a.dtype) for a in arrays]
    outs[1:3] = wide, wide
    sem = pltpu.SemaphoreType.DMA((5, 4))
    return pl.pallas_call(
        store_kernel,
        out_shape=tuple(outs),
        in_specs=[hbm] * 5,
        out_specs=(hbm,) * 5,
        scratch_shapes=[pltpu.VMEM(a.shape, a.dtype) for a in arrays] + [pltpu.VMEM(wide.shape, wide.dtype)] * 2 + [sem] * 2,
        compiler_params=pltpu.CompilerParams(vmem_limit_bytes=60 * 1024 * 1024),
        name="store_all",
    )(*arrays)


def fits_plane(across, inputs, gate_proj):
    reps, fs_count, tps = (lax.axis_size(a) for a in ("rep", "fs", "tp"))
    tokens, feats = inputs.shape[1:]
    rows, hid = gate_proj.shape
    parts = reps * across
    width = part_width(hid, parts)
    return (
        reps == across == tps == 2 and fs_count > across and tokens % 16 == 0 and tokens >= 48
        and hid % LANES == 0 and rows % LANES == 0 and feats % rows == 0 and feats % (2 * LANES) == 0
        and 4 * parts * width <= 5 * hid
    )


def shards(across, inputs, gate_proj, value_proj, gate_taps, value_taps, out_grad):
    if fits_plane(across, inputs, gate_proj):
        in_grad, gate_grad, value_grad, gate_terms, value_terms = store_all(
            *fused_all(across, inputs[0], gate_proj, value_proj, gate_taps, value_taps, out_grad[0])
        )
        return in_grad[None], gate_grad, value_grad, gate_terms, value_terms

    contract_cols = (((1,), (1,)), ((), ()))
    contract_rows = (((0,), (0,)), ((), ()))
    reps, fs_count = lax.axis_size("rep"), lax.axis_size("fs")
    rep = lax.axis_index("rep")
    tokens, feats = inputs.shape[1:]
    hid = gate_proj.shape[1]
    width = min(hid, -(-hid // reps // 128) * 128)
    last = hid - width

    def start_of(part):
        return jnp.minimum(part * width, last)

    first = start_of(rep)
    dead = rep * width - first
    live = jnp.arange(width) >= dead

    def part_cols(x, part):
        return lax.dynamic_slice_in_dim(x, start_of(part), width, x.ndim - 1)

    w_own = jnp.concatenate(
        [jnp.where(live, part_cols(w, rep), jnp.zeros((), w.dtype)) for w in (gate_proj, value_proj)], axis=1
    )
    g_parts = jnp.stack([part_cols(out_grad[0], (rep + step) % reps) for step in range(reps)])
    x_all, g_all, w_all = gather_all(inputs[0], g_parts, w_own, across)
    w_all = w_all.reshape(-1, 2 * width)

    ext = tokens + 2 * HALO
    pre = jnp.dot(x_all.reshape(reps * ext, -1), w_all, preferred_element_type=jnp.float32)
    pre = pre.astype(jnp.bfloat16).reshape(reps, ext, 2 * width)
    tap_start = lax.axis_index("tp") * hid + first
    taps = jnp.concatenate(
        [lax.dynamic_slice_in_dim(t, tap_start, width, 1) for t in (gate_taps, value_taps)], axis=1
    )
    factor = float(tokens * fs_count * reps) ** (-0.5)
    pre_cot, tap_terms = mix_all(pre, g_all, taps, tokens, fs_count, factor)
    pre_cot = pre_cot.reshape(reps * tokens, 2 * width)
    tap_terms = tap_terms[:3]

    grads = lax.dot_general(
        x_all[:, :tokens].reshape(reps * tokens, -1), pre_cot, contract_rows, preferred_element_type=jnp.float32
    )
    grads = (grads * factor).astype(jnp.bfloat16).reshape(fs_count, -1, 2 * width)
    partial_value = lax.dot_general(pre_cot, w_all, contract_cols, preferred_element_type=jnp.float32)
    partial_value = partial_value.astype(jnp.bfloat16).reshape(reps, tokens, -1)
    lanes = -(-tap_terms.size // 1024) * 128
    tap_terms = jnp.pad(tap_terms.reshape(-1), (0, 8 * lanes - tap_terms.size)).reshape(8, lanes)
    own, in_grad, tap_all = scatter_all(grads, partial_value, tap_terms, across)

    skips = [max(0, p * width - last) for p in range(reps)]
    proj_grads = [
        jnp.concatenate(
            [own[p, :, branch * width + skips[p] : (branch + 1) * width] for p in range(reps)], axis=1
        ).astype(jnp.float32)
        for branch in range(2)
    ]
    tap_all = tap_all.reshape(reps, -1, 8 * lanes)[:, :, : 6 * width].reshape(reps, -1, 3, 2, width)
    taps_out = jnp.concatenate(
        [tap_all[p, half, :, :, skips[p] :] for half in range(tap_all.shape[1]) for p in range(reps)], axis=2
    )
    return in_grad[None], proj_grads[0], proj_grads[1], taps_out[:, 0], taps_out[:, 1]


def solution(mesh):
    placed = (P("rep", "fs", "tp"), P("fs", "tp"), P("fs", "tp"), P(), P(), P("rep", "fs", "tp"))
    return jax.shard_map(
        functools.partial(shards, row_length(mesh)),
        mesh=mesh,
        in_specs=placed,
        out_specs=(P("rep", "fs", "tp"), P("fs", "tp"), P("fs", "tp"), P(), P()),
        check_vma=False,
    )
```
